512 devices in a mesh: grp: 2 (over y), sp: 32 (over z), tp: 8 (over x, core).
Axes of the slice: x: 4, y: 2, z: 32, core: 2. Of those that a mesh axis runs over, the one named last changes fastest.
The devices are a block of a 4x8x32 slice.
Arguments:
- tokens: bfloat16 [32768, 2048], P(('grp', 'sp')), parts along dimension 0, may hold values from -6 to 6
- fresh_token_input: bfloat16 [4096], P('grp'), parts along dimension 0, may hold values from -6 to 6
- value_matrix: bfloat16 [2048, 2048], P(None, 'tp'), may hold values from -0.125 to 0.125
- write_matrix: bfloat16 [2048, 1024], P(None, 'tp'), may hold values from -0.125 to 0.125
- read_matrix: bfloat16 [2048, 1024], P(None, 'tp'), may hold values from -0.125 to 0.125
- gate_matrix: bfloat16 [2048, 2048], P(None, 'tp'), may hold values from -0.125 to 0.125
- step_matrix: bfloat16 [2048, 32], replicated, may hold values from -0.125 to 0.125
- value_filter_taps: bfloat16 [4, 2048], replicated, may hold values from -3 to 3
- write_filter_taps: bfloat16 [4, 1024], replicated, may hold values from -3 to 3
- read_filter_taps: bfloat16 [4, 1024], replicated, may hold values from -3 to 3
- head_log_decay: float32 [32], replicated
- step_offset_bias: float32 [32], replicated, may hold values from -3.5 to -2.5
- decay_spike: float32 [32768, 32], P(('grp', 'sp'), 'tp'), parts along dimension 0, may hold values from -3 to 0, as said below
- bypass_scale: float32 [32], replicated, may hold values from 0.5 to 2
- group_norm_scale: float32 [2048], replicated, may hold values from 0.1 to 1.9
Outputs:
- prompt_out: bfloat16 [32768, 2048], P(('grp', 'sp'), 'tp'), parts along dimension 0
- state_cache: bfloat16 [256, 2048], P(('grp', 'sp'), 'tp'), parts along dimension 0
- step_out: bfloat16 [128, 32], P(('grp', 'tp'), 'sp'), parts along dimension 0
The draws below stay inside these ranges and needn't reach their ends.
There are 2 independent parts, one for each index of `grp`. The reference program is written for one: setup_inputs(seed, part) draws one part's arguments, and reference() takes and returns one part's arrays. A program takes and returns all parts, laid end to end along the dimension named above; an argument that names none is the same for every part. Nothing has to cross between parts.
Inputs may be any that keep to these rules, and one draw needn't show every extreme that they name: `decay_spike`: never positive.
All inputs are finite; a program needn't handle non-finite values.
Results may differ from the reference program's by a relative error of at most 0.023.
Values may be sent and summed in bfloat16 or wider, within the bound.
No kernel may reach another device: no remote copies, remote signals or barrier semaphores. Data moves between devices by JAX's collectives and lax.ppermute only.
A program may use at most 64 MiB of HBM per device.

```python
import jax
import jax.numpy as jnp
from jax import lax

D = 2048
HEADS = 32
HEAD = 64
GROUPS = 8
STATE = 128
CONV = 4
BLOCK = 128
TOK_DEV = 512
INNER = 2048
TOKENS = 16384
N_SP = 32


def draw_head_log_decay(key, part):
    key_pick, key_fast, key_slow = jax.random.split(jax.random.fold_in(key, 11), 3)
    chance = 0.5
    fast_pick = jax.random.uniform(key_pick, (HEADS,), jnp.float32) < chance
    fast_rate = jax.random.uniform(key_fast, (HEADS,), jnp.float32, 0.3, 1.0)
    slow_rate = jnp.exp(jax.random.uniform(key_slow, (HEADS,), jnp.float32, jnp.log(5.0 / TOKENS), jnp.log(12.0 / TOKENS)))
    return jnp.log(jnp.where(fast_pick, fast_rate, slow_rate)).astype(jnp.float32)


def draw_decay_spike(key, part):
    key_span, key_place, key_drop = jax.random.split(jax.random.fold_in(key, 23), 3)
    span_count = TOKENS // TOK_DEV
    span_scale = jnp.exp(jax.random.uniform(key_span, (span_count, HEADS), jnp.float32, jnp.log(0.5), jnp.log(2.0)))
    baseline_tier = -0.3 / TOKENS * jnp.repeat(span_scale, TOK_DEV, axis=0)
    places = jax.random.randint(key_place, (3,), 0, TOKENS)
    omitted_occasions = jnp.log(jax.random.uniform(key_drop, (3, HEADS), jnp.float32, 0.5, 0.8))
    agreeing_tally = (jnp.arange(TOKENS)[:, None] == places[None, :]).astype(jnp.float32)
    sudden_surges = jnp.sum(agreeing_tally[:, :, None] * omitted_occasions[None], axis=1)
    return (baseline_tier + sudden_surges).astype(jnp.float32)


def level_of(stream_key, shape, shards, low, largest):
    loudness, own = 1.0, jax.random.fold_in(stream_key, 6)
    for dim, shards_of in shards:
        heights = jnp.exp(jax.random.uniform(jax.random.fold_in(own, dim), (shards_of,), jnp.float32, low / len(shards), largest / len(shards)))
        loudness = loudness * jnp.repeat(heights, shape[dim] // shards_of).reshape([-1 if axis == dim else 1 for axis in range(len(shape))])
    return loudness


def bell_draw(key, dims, scale, most, cuts=(), held_as=jnp.bfloat16):
    level = level_of(key, dims, cuts, -0.22, 0.18) if cuts else 1.0
    values = jax.random.normal(key, dims, jnp.float32) * scale * level
    return jnp.minimum(jnp.maximum(values, -most), most).astype(held_as)


def setup_inputs(seed: int = 0, part: int = 0) -> dict:
    arg_keys = jax.random.split(jax.random.key(seed), 16)
    part_splits = jax.random.split(jax.random.fold_in(arg_keys[15], part), 16)
    tokens = bell_draw(part_splits[0], (TOKENS, D), 1.0, 6.0, ((0, 32),))
    fresh_token_input = bell_draw(part_splits[1], (D,), 1.0, 6.0)
    value_matrix = bell_draw(arg_keys[2], (D, INNER), D ** -0.5, 0.125, ((1, 8),))
    write_matrix = bell_draw(arg_keys[3], (D, GROUPS * STATE), D ** -0.5, 0.125, ((1, 8),))
    read_matrix = bell_draw(arg_keys[4], (D, GROUPS * STATE), D ** -0.5, 0.125, ((1, 8),))
    gate_matrix = bell_draw(arg_keys[5], (D, INNER), D ** -0.5, 0.125, ((1, 8),))
    step_matrix = bell_draw(arg_keys[6], (D, HEADS), D ** -0.5, 0.125)
    value_filter_taps = bell_draw(arg_keys[7], (CONV, INNER), CONV ** -0.5, 3.0)
    write_filter_taps = bell_draw(arg_keys[8], (CONV, GROUPS * STATE), CONV ** -0.5, 3.0)
    read_filter_taps = bell_draw(arg_keys[9], (CONV, GROUPS * STATE), CONV ** -0.5, 3.0)
    head_log_decay = draw_head_log_decay(jax.random.fold_in(arg_keys[15], 71), part)
    step_offset_bias = jnp.clip(jax.random.uniform(arg_keys[11], (HEADS,), jnp.float32, -3.5, -2.5), -3.5, -2.5)
    decay_spike = draw_decay_spike(jax.random.fold_in(jax.random.fold_in(arg_keys[15], part), 71), part)
    bypass_scale = jnp.clip(jax.random.uniform(arg_keys[13], (HEADS,), jnp.float32, 0.5, 2.0), 0.5, 2.0)
    group_norm_scale = jnp.clip(1.0 + 0.18 * jax.random.normal(arg_keys[14], (INNER,), jnp.float32), 0.1, 1.9)
    return {"tokens": tokens, "fresh_token_input": fresh_token_input, "value_matrix": value_matrix, "write_matrix": write_matrix, "read_matrix": read_matrix, "gate_matrix": gate_matrix, "step_matrix": step_matrix, "value_filter_taps": value_filter_taps, "write_filter_taps": write_filter_taps, "read_filter_taps": read_filter_taps, "head_log_decay": head_log_decay, "step_offset_bias": step_offset_bias, "decay_spike": decay_spike, "bypass_scale": bypass_scale, "group_norm_scale": group_norm_scale}


epsilon = 1e-06

def project(operand, weights):
    return jnp.dot(operand, weights, preferred_element_type=jnp.float32).astype(jnp.bfloat16)

def apply_taps(previous, current, tap_weights):
    joined = jnp.concatenate([previous, current], axis=0).astype(jnp.float32)
    length = current.shape[0]
    summed = jnp.zeros(current.shape, jnp.float32)
    for offset in range(CONV):
        summed = summed + tap_weights[offset].astype(jnp.float32) * joined[offset:offset + length]
    return summed

def group_norm(gated_rows, groups):
    shaped = gated_rows.reshape(gated_rows.shape[:-1] + (groups, -1))
    normed = shaped * lax.rsqrt(lax.optimization_barrier(jnp.mean(shaped * shaped, axis=-1, keepdims=True)) + epsilon)
    return normed.reshape(gated_rows.shape)

def reference(tokens, fresh_token_input, value_matrix, write_matrix, read_matrix, gate_matrix, step_matrix, value_filter_taps, write_filter_taps, read_filter_taps, head_log_decay, step_offset_bias, decay_spike, bypass_scale, group_norm_scale):
    per_group = HEADS // GROUPS
    value_rows = project(tokens, value_matrix)
    write_rows = project(tokens, write_matrix)
    read_rows = project(tokens, read_matrix)
    gate_rows = project(tokens, gate_matrix)
    step_raw = jnp.dot(tokens, step_matrix, preferred_element_type=jnp.float32)
    zero_wide = jnp.zeros((CONV - 1, INNER), jnp.bfloat16)
    zero_maps = jnp.zeros((CONV - 1, GROUPS * STATE), jnp.bfloat16)
    values = jax.nn.silu(apply_taps(zero_wide, value_rows, value_filter_taps)).astype(jnp.bfloat16)
    writes = jax.nn.silu(apply_taps(zero_maps, write_rows, write_filter_taps)).astype(jnp.bfloat16)
    reads = jax.nn.silu(apply_taps(zero_maps, read_rows, read_filter_taps)).astype(jnp.bfloat16)
    step_length = jax.nn.softplus(step_raw + step_offset_bias)
    head_decay_rates = jnp.exp(head_log_decay)
    log_decay_value = decay_spike - step_length * head_decay_rates
    blocks = TOKENS // BLOCK
    block_values = values.reshape(blocks, BLOCK, GROUPS, per_group, HEAD)
    block_writes = writes.reshape(blocks, BLOCK, GROUPS, STATE)
    block_reads = reads.reshape(blocks, BLOCK, GROUPS, STATE)
    block_steps = step_length.reshape(blocks, BLOCK, GROUPS, per_group)
    segment_fading = log_decay_value.reshape(blocks, BLOCK, GROUPS, per_group)
    causal = jnp.tril(jnp.ones((BLOCK, BLOCK), bool))

    def block_step(entering, inputs):
        val_in, wri_in, rea_in, stp_in, dec_in = inputs
        cumulative = jnp.cumsum(dec_in, axis=0)
        scores = jnp.einsum('lgn,sgn->gls', rea_in.astype(jnp.float32), wri_in.astype(jnp.float32))
        cum_heads = jnp.transpose(cumulative, (1, 2, 0))
        decay_gaps = cum_heads[:, :, :, None] - cum_heads[:, :, None, :]
        step_heads = jnp.transpose(stp_in, (1, 2, 0))
        mixing = (scores[:, None] * jnp.exp(jnp.where(causal, decay_gaps, -jnp.inf)) * step_heads[:, :, None, :]).astype(jnp.bfloat16)
        inner_part = jnp.einsum('gels,sgep->lgep', mixing.astype(jnp.float32), val_in.astype(jnp.float32))
        block_end = cumulative[-1]
        scaled = ((jnp.exp(block_end[None] - cumulative) * stp_in)[..., None] * val_in.astype(jnp.float32)).astype(jnp.bfloat16)
        block_state = jnp.einsum('sgn,sgep->ngep', wri_in.astype(jnp.float32), scaled.astype(jnp.float32))
        carried = jnp.exp(cumulative)[..., None] * jnp.einsum('lgn,ngep->lgep', rea_in.astype(jnp.float32), entering, precision=lax.Precision.HIGHEST)
        leaving = jnp.exp(block_end)[None, :, :, None] * entering + block_state
        return (leaving, inner_part + carried)
    initial = jnp.zeros((STATE, GROUPS, per_group, HEAD), jnp.float32)
    final_state, outputs = lax.scan(block_step, initial, (block_values, block_writes, block_reads, block_steps, segment_fading))
    mixed_rows = outputs.reshape(TOKENS, HEADS, HEAD) + bypass_scale[None, :, None] * values.astype(jnp.float32).reshape(TOKENS, HEADS, HEAD)
    gated_rows = mixed_rows.reshape(TOKENS, INNER) * jax.nn.silu(gate_rows.astype(jnp.float32))
    prompt_out = (group_norm(gated_rows, GROUPS) * group_norm_scale).astype(jnp.bfloat16)
    state_cache = final_state.reshape(STATE, INNER).astype(jnp.bfloat16)
    new_row = fresh_token_input[None]
    new_value = project(new_row, value_matrix)
    new_write = project(new_row, write_matrix)
    new_read = project(new_row, read_matrix)
    new_gate = project(new_row, gate_matrix)
    new_step = jax.nn.softplus(jnp.dot(new_row, step_matrix, preferred_element_type=jnp.float32)[0] + step_offset_bias)
    edge = TOKENS - (CONV - 1)
    new_values = jax.nn.silu(apply_taps(value_rows[edge:], new_value, value_filter_taps)).astype(jnp.bfloat16)
    latest_stores = jax.nn.silu(apply_taps(write_rows[edge:], new_write, write_filter_taps)).astype(jnp.bfloat16)
    new_reads = jax.nn.silu(apply_taps(read_rows[edge:], new_read, read_filter_taps)).astype(jnp.bfloat16)
    value_now = new_values.astype(jnp.float32).reshape(GROUPS, per_group, HEAD)
    write_now = latest_stores.astype(jnp.float32).reshape(GROUPS, STATE)
    read_now = new_reads.astype(jnp.float32).reshape(GROUPS, STATE)
    new_decay = jnp.exp(-new_step * head_decay_rates).reshape(GROUPS, per_group)
    step_now = new_step.reshape(GROUPS, per_group)
    cached = state_cache.astype(jnp.float32).reshape(STATE, GROUPS, per_group, HEAD)
    updated = new_decay[None, :, :, None] * cached + step_now[None, :, :, None] * write_now.T[:, :, None, None] * value_now[None]
    reading = jnp.einsum('gn,ngep->gep', read_now, updated, precision=lax.Precision.HIGHEST)
    new_mixed = reading + bypass_scale.reshape(GROUPS, per_group)[:, :, None] * value_now
    new_gated = new_mixed.reshape(1, INNER) * jax.nn.silu(new_gate.astype(jnp.float32))
    step_out = (group_norm(new_gated, GROUPS) * group_norm_scale).astype(jnp.bfloat16)[0]
    step_out = step_out.reshape(INNER // N_SP, N_SP)
    return (prompt_out, state_cache, step_out)
```

```python
import jax
import jax.numpy as jnp
from jax import lax
from jax.experimental import pallas as pl
from jax.experimental.pallas import tpu as pltpu
from jax.sharding import PartitionSpec as P

HEAD = 64
STATE = 128
CONV = 4
BLOCK = 128
SUB = 8
MISC = 128
HALO = 8

epsilon = 1e-06
f32 = jnp.float32
bf16 = jnp.bfloat16
HIGHEST = lax.Precision.HIGHEST
VMEM_LIMIT = 56 * 1024 * 1024


def dot(a, b, dims=((1,), (0,)), precision=None):
    return lax.dot_general(a, b, (dims, ((), ())), precision=precision, preferred_element_type=f32)


def silu(x):
    return x / (1.0 + jnp.exp(-x))


def softplus(x):
    return jnp.maximum(x, 0.0) + jnp.log1p(jnp.exp(-jnp.abs(x)))


def iota(shape, dim):
    return lax.broadcasted_iota(jnp.int32, shape, dim)


def spread(heads, channels):
    return (iota((heads, channels), 0) == iota((heads, channels), 1) // HEAD).astype(f32)


def own_rows(table, rank, count):
    picked = table[0:count]
    for other in range(1, table.shape[0] // count):
        picked = jnp.where(rank == other, table[other * count : (other + 1) * count], picked)
    return picked


def head_column(ref, first, count, width):
    rows = iota((count, width), 0)
    column = jnp.full((count, width), ref[first], f32)
    for h in range(1, count):
        column = jnp.where(rows == h, ref[first + h], column)
    return column


def project_kernel(
    tok_ref, fresh_ref, wv_ref, ww_ref, wr_ref, ws_ref, rows_ref, step_ref, new_ref, newstep_ref,
    acc, accs, accn, accns,
):
    k = pl.program_id(0)
    last = pl.num_programs(0) - 1
    tok = tok_ref[...]
    fresh = jnp.broadcast_to(fresh_ref[...], (16, fresh_ref.shape[1]))
    weights = jnp.concatenate([wv_ref[...], ww_ref[...], wr_ref[...]], axis=1)
    part = dot(tok, weights)
    parts = dot(ws_ref[...], tok, ((1,), (1,)))
    partn = dot(fresh, weights)
    partns = dot(ws_ref[...], fresh, ((1,), (1,)))

    @pl.when(k == 0)
    def _():
        acc[...] = part
        accs[...] = parts
        accn[...] = partn
        accns[...] = partns

    @pl.when(k > 0)
    def _():
        acc[...] += part
        accs[...] += parts
        accn[...] += partn
        accns[...] += partns

    @pl.when(k == last)
    def _():
        rank = lax.axis_index("tp")
        heads = step_ref.shape[0]
        rows_ref[...] = acc[...].astype(bf16)
        step_ref[...] = own_rows(accs[...], rank, heads)
        new_ref[...] = accn[...][0:8]
        newstep_ref[...] = own_rows(accns[...], rank, heads)


def local_kernel(
    rows_ref, halo_ref, wv_ref, ww_ref, wr_ref, step_ref, new_ref, newstep_ref, spike_ref,
    vtap_ref, wtap_ref, rtap_ref, decay_ref, bias_ref, skip_ref,
    vwr_ref, cum_ref, dt_ref, inside_ref, send_ref, ext,
):
    rank = lax.axis_index("tp")
    length = rows_ref.shape[0]
    heads = step_ref.shape[0]
    channels = wv_ref.shape[1]
    first = rank * heads
    halo = halo_ref[...]
    before = jnp.concatenate(
        [dot(halo, wv_ref[...]), dot(halo, ww_ref[...]), dot(halo, wr_ref[...])], axis=1
    )
    ext[0:HALO] = before.astype(bf16).astype(f32)
    ext[HALO:] = rows_ref[...].astype(f32)
    taps = jnp.concatenate(
        [
            vtap_ref[:, pl.ds(pl.multiple_of(rank * channels, 128), channels)].astype(f32),
            wtap_ref[:, pl.ds(pl.multiple_of(rank * STATE, 128), STATE)].astype(f32),
            rtap_ref[:, pl.ds(pl.multiple_of(rank * STATE, 128), STATE)].astype(f32),
        ],
        axis=1,
    )
    off = HALO - (CONV - 1)
    summed = taps[0:1] * ext[off : off + length]
    for k in range(1, CONV):
        summed = summed + taps[k : k + 1] * ext[off + k : off + k + length]
    vwr = silu(summed).astype(bf16)
    vwr_ref[...] = vwr
    newest = taps[CONV - 1 : CONV] * new_ref[0:1].astype(bf16).astype(f32)
    for k in range(CONV - 1):
        row = length + off + k
        newest = newest + taps[k : k + 1] * ext[row : row + 1]
    newest = silu(newest).astype(bf16).astype(f32)
    new_value = newest[:, 0:channels]
    new_write = newest[:, channels : channels + STATE]
    new_read = newest[:, channels + STATE :]
    bias = head_column(bias_ref, first, heads, 128)
    rate = jnp.exp(head_column(decay_ref, first, heads, 128))
    upper = (iota((BLOCK, BLOCK), 0) <= iota((BLOCK, BLOCK), 1)).astype(f32)
    expand = spread(heads, channels)
    running = jnp.zeros((STATE, channels), f32)
    total = jnp.zeros((heads, 128), f32)
    for b in range(length // BLOCK):
        at = slice(b * BLOCK, (b + 1) * BLOCK)
        dt = softplus(step_ref[:, at] + bias)
        log_decay = spike_ref[:, at] - dt * rate
        cum = dot(log_decay, upper, precision=HIGHEST)
        dt_ref[:, at] = dt
        cum_ref[:, at] = cum
        end = jnp.broadcast_to(cum[:, BLOCK - 1 :], (heads, BLOCK))
        factor = dot(jnp.exp(end - cum) * dt, expand, ((0,), (0,)), HIGHEST)
        scaled = (factor * vwr[at, 0:channels].astype(f32)).astype(bf16)
        states = dot(vwr[at, channels : channels + STATE], scaled, ((0,), (0,)))
        fade = dot(jnp.exp(end), expand, ((0,), (0,)), HIGHEST)
        inside_ref[b] = running.astype(bf16)
        running = fade * running + states
        total = total + end
    fade = jnp.exp(total)
    high = fade.astype(bf16).astype(f32)
    low = fade - high
    shape = (STATE, MISC)
    lanes = iota(shape, 1)
    rows = iota(shape, 0)
    misc = jnp.zeros(shape, f32)
    for h in range(heads):
        misc = jnp.where(lanes == h, high[h : h + 1, 0:1], misc)
        misc = jnp.where(lanes == heads + h, low[h : h + 1, 0:1], misc)
    own = STATE // lax.axis_size("sp")
    stretch = SUB * own
    diagonal = jnp.where(rows == lanes, jnp.broadcast_to(new_read, shape), 0.0)
    read_column = jnp.sum(diagonal, axis=1, keepdims=True)
    new_dt = softplus(newstep_ref[...][:, 0:1] + bias[:, 0:1])
    skip = head_column(skip_ref, first, heads, 128)[:, 0:1]
    weight = new_dt * jnp.sum(new_read * new_write, axis=1, keepdims=True) + skip
    direct = jnp.sum(expand * weight, axis=0, keepdims=True) * new_value
    placed = jnp.where(iota((8, channels), 0) == iota((8, channels), 1) // HEAD, direct, 0.0)
    shift = (iota((channels, MISC), 0) % HEAD + (MISC - HEAD) == iota((channels, MISC), 1)).astype(f32)
    direct_rows = dot(placed, shift, precision=HIGHEST)[0:own]
    for g in range(STATE // stretch):
        at = slice(g * stretch, (g + 1) * stretch)
        piece = running[at].reshape(SUB, own, channels).astype(bf16)
        for copy in range(STATE // stretch):
            send_ref[copy * SUB : (copy + 1) * SUB, :, g * channels : (g + 1) * channels] = piece
    note = misc[0:stretch]
    for g in range(STATE // stretch):
        at = slice(g * stretch, (g + 1) * stretch)
        note = jnp.where(lanes[0:stretch] == 2 * heads + g, read_column[at], note)
    note = note.reshape(SUB, own, MISC)
    note = jnp.where(iota(note.shape, 2) >= MISC - HEAD, direct_rows[None], note).astype(bf16)
    wide = STATE // stretch * channels
    for copy in range(STATE // stretch):
        send_ref[copy * SUB : (copy + 1) * SUB, :, wide:] = note


def inner_kernel(
    tok_ref, wg_ref, fresh_ref, vwr_ref, cum_ref, dt_ref, inside_ref, skip_ref,
    base_ref, lift_ref, newgate_ref, before,
):
    b = pl.program_id(0)
    rank = lax.axis_index("tp")
    heads = cum_ref.shape[0]
    channels = wg_ref.shape[1]

    @pl.when(b == 0)
    def _():
        before[...] = jnp.zeros_like(before)
        fresh = jnp.broadcast_to(fresh_ref[...], (16, fresh_ref.shape[1]))
        gate = dot(fresh, wg_ref[...])[0:8].astype(bf16).astype(f32)
        newgate_ref[...] = silu(gate)

    expand = spread(heads, channels)
    skip = jnp.sum(
        expand * head_column(skip_ref, rank * heads, heads, channels), axis=0, keepdims=True
    )
    cum = cum_ref[...]
    dt = dt_ref[...]
    values = vwr_ref[:, 0:channels]
    writes = vwr_ref[:, channels : channels + STATE]
    reads = vwr_ref[:, channels + STATE :]
    gate = silu(dot(tok_ref[...], wg_ref[...]).astype(bf16).astype(f32))
    scores = dot(reads, writes, ((1,), (1,)))
    causal = iota((BLOCK, BLOCK), 0) >= iota((BLOCK, BLOCK), 1)
    columns = jnp.transpose(jnp.concatenate([cum, cum], axis=0))
    parts = []
    for h in range(heads):
        gap = columns[:, h : h + 1] - cum[h : h + 1]
        mixing = scores * jnp.exp(jnp.where(causal, gap, -jnp.inf)) * dt[h : h + 1]
        parts.append(dot(mixing.astype(bf16), values[:, h * HEAD : (h + 1) * HEAD]))
    inner = jnp.concatenate(parts, axis=1)
    fade = dot(jnp.exp(cum), expand, ((0,), (0,)), HIGHEST)
    carried = fade * dot(reads, inside_ref[0])
    base_ref[...] = (inner + carried + skip * values.astype(f32)) * gate
    far = jnp.exp(cum + before[...])
    lift_ref[...] = dot(far, expand, ((0,), (0,)), HIGHEST) * gate
    before[...] += jnp.broadcast_to(cum[:, BLOCK - 1 :], before.shape)


def prefix_kernel(recv_ref, newstep_ref, decay_ref, bias_ref, send_ref, cache_ref, direct_ref, states):
    rank = lax.axis_index("tp")
    place = lax.axis_index("sp")
    count = recv_ref.shape[0]
    own = recv_ref.shape[1]
    wide = recv_ref.shape[2] - MISC
    pieces = count // SUB
    channels = wide // pieces
    heads = channels // HEAD
    group = place // SUB
    notes = recv_ref[:, 0:1, wide:].astype(f32).reshape(count, MISC)
    lane = iota((MISC, channels), 0)
    owner = iota((MISC, channels), 1) // HEAD
    pick = jnp.where((lane == owner) | (lane == owner + heads), 1.0, 0.0)
    fades = dot(jnp.where(iota(notes.shape, 1) < 2 * heads, notes, 0.0), pick, precision=HIGHEST)
    state = jnp.zeros((own, wide), f32)
    for k in range(count):
        states[k] = state
        fade = jnp.concatenate([fades[k : k + 1]] * pieces, axis=1)
        state = fade * state + recv_ref[k, :, 0:wide].astype(f32)
    kept = state.astype(bf16)
    mine = kept[:, 0:channels]
    for g in range(1, pieces):
        mine = jnp.where(group == g, kept[:, g * channels : (g + 1) * channels], mine)
    cache_ref[...] = mine
    note = recv_ref[count - 1, :, wide:].astype(f32)
    reading = jnp.zeros((own, channels), f32)
    for g in range(pieces):
        column = note[:, 2 * heads + g : 2 * heads + g + 1]
        reading = reading + column * kept[:, g * channels : (g + 1) * channels].astype(f32)
    first = rank * heads
    bias = head_column(bias_ref, first, heads, 1)
    rate = jnp.exp(head_column(decay_ref, first, heads, 1))
    decay = jnp.exp(-softplus(newstep_ref[...][:, 0:1] + bias) * rate)
    decay = jnp.sum(spread(heads, channels) * decay, axis=0, keepdims=True)
    partial = jnp.sum(reading, axis=0, keepdims=True) * decay
    high = partial.astype(bf16).astype(f32)
    low = partial - high
    rows = iota((own, channels), 0)
    share = jnp.where(rows == 0, high, jnp.where(rows == 1, low, 0.0)).astype(bf16)
    chosen = states[pl.ds(group * SUB, SUB)]
    send_ref[:, :, 0:wide] = chosen.astype(bf16)
    send_ref[:, :, wide:] = jnp.broadcast_to(share[None], (SUB, own, channels))
    unshift = (iota((MISC, channels), 0) == iota((MISC, channels), 1) % HEAD + (MISC - HEAD)).astype(f32)
    laid = dot(note, unshift, precision=HIGHEST)
    direct_ref[...] = jnp.sum(jnp.where(rows == iota(rows.shape, 1) // HEAD, laid, 0.0), axis=0, keepdims=True)


def finish_kernel(recv_ref, base_ref, lift_ref, reads_ref, gain_ref, direct_ref, newgate_ref, out_ref, step_ref):
    rank = lax.axis_index("tp")
    place = lax.axis_index("sp")
    channels = base_ref.shape[1]
    wide = recv_ref.shape[2] - channels
    pieces = wide // channels
    own = recv_ref.shape[1]
    earlier = jnp.concatenate(
        [
            recv_ref[:, :, g * channels : (g + 1) * channels].astype(f32).reshape(SUB * own, channels)
            for g in range(pieces)
        ],
        axis=0,
    ).astype(bf16)
    gain = gain_ref[:, pl.ds(pl.multiple_of(rank * channels, 128), channels)]
    gated = base_ref[...] + dot(reads_ref[...], earlier) * lift_ref[...]
    scale = lax.rsqrt(jnp.mean(gated * gated, axis=1, keepdims=True) + epsilon)
    out_ref[...] = (gated * scale * gain).astype(bf16)
    partial = jnp.sum(jnp.sum(recv_ref[:, :, wide:].astype(f32), axis=0), axis=0, keepdims=True)
    new = (partial + direct_ref[...]) * newgate_ref[0:1]
    scale = lax.rsqrt(jnp.mean(new * new, axis=1, keepdims=True) + epsilon)
    step = (new * scale * gain).astype(bf16)
    columns = lax.axis_size("sp")
    channel = iota((channels, 128), 0)
    take = (channel // columns == iota((channels, 128), 1)) & (channel % columns == place)
    picked = dot(jnp.broadcast_to(step, (16, channels)), take.astype(bf16))
    step_ref[...] = picked[0:1, 0 : channels // columns].astype(bf16)


def call(kernel, out_shape, grid=None, in_specs=None, out_specs=None, scratch=(), flops=0, name=None):
    return pl.pallas_call(
        kernel,
        out_shape=out_shape,
        grid_spec=pltpu.PrefetchScalarGridSpec(
            num_scalar_prefetch=0,
            grid=grid or (),
            in_specs=in_specs,
            out_specs=out_specs,
            scratch_shapes=scratch,
        ),
        compiler_params=pltpu.CompilerParams(
            vmem_limit_bytes=VMEM_LIMIT,
            dimension_semantics=("arbitrary",) * len(grid or ()),
        ),
        cost_estimate=pl.CostEstimate(flops=flops, transcendentals=0, bytes_accessed=1 << 20),
        name=name,
    )


def shaped(*shape, dtype=f32):
    return jax.ShapeDtypeStruct(shape, dtype)


def on_device(
    tokens,
    fresh_token_input,
    value_matrix,
    write_matrix,
    read_matrix,
    gate_matrix,
    step_matrix,
    value_filter_taps,
    write_filter_taps,
    read_filter_taps,
    head_log_decay,
    step_offset_bias,
    decay_spike,
    bypass_scale,
    group_norm_scale,
):
    sequence_count = lax.axis_size("sp")
    length, depth = tokens.shape
    channels = value_matrix.shape[1]
    heads = channels // HEAD
    all_heads = step_matrix.shape[1]
    own = STATE // sequence_count
    pieces = sequence_count // SUB
    blocks = length // BLOCK
    width = channels + 2 * STATE
    vm = pl.BlockSpec(memory_space=pltpu.VMEM)
    sm = pl.BlockSpec(memory_space=pltpu.SMEM)

    halo = lax.ppermute(
        tokens[length - HALO :], "sp", [(i, i + 1) for i in range(sequence_count - 1)]
    )
    fresh = fresh_token_input[None]
    spike = decay_spike.T
    chunk = depth // 4
    rows, step_raw, new_rows, new_step = call(
        project_kernel,
        (
            shaped(length, width, dtype=bf16),
            shaped(heads, length),
            shaped(8, width),
            shaped(heads, 16),
        ),
        grid=(depth // chunk,),
        in_specs=[
            pl.BlockSpec((length, chunk), lambda k: (0, k)),
            pl.BlockSpec((1, chunk), lambda k: (0, k)),
            pl.BlockSpec((chunk, channels), lambda k: (k, 0)),
            pl.BlockSpec((chunk, STATE), lambda k: (k, 0)),
            pl.BlockSpec((chunk, STATE), lambda k: (k, 0)),
            pl.BlockSpec((all_heads, chunk), lambda k: (0, k)),
        ],
        out_specs=[
            pl.BlockSpec((length, width), lambda k: (0, 0)),
            pl.BlockSpec((heads, length), lambda k: (0, 0)),
            pl.BlockSpec((8, width), lambda k: (0, 0)),
            pl.BlockSpec((heads, 16), lambda k: (0, 0)),
        ],
        scratch=[
            pltpu.VMEM((length, width), f32),
            pltpu.VMEM((all_heads, length), f32),
            pltpu.VMEM((16, width), f32),
            pltpu.VMEM((all_heads, 16), f32),
        ],
        flops=2 * length * depth * width,
        name="project",
    )(tokens, fresh, value_matrix, write_matrix, read_matrix, step_matrix.T)

    wide = pieces * channels
    vwr, cum, dt, inside, send = call(
        local_kernel,
        (
            shaped(length, width, dtype=bf16),
            shaped(heads, length),
            shaped(heads, length),
            shaped(blocks, STATE, channels, dtype=bf16),
            shaped(sequence_count, own, wide + MISC, dtype=bf16),
        ),
        in_specs=[vm] * 12 + [sm] * 3,
        out_specs=[vm] * 5,
        scratch=[pltpu.VMEM((length + HALO, width), f32)],
        flops=2 * length * STATE * channels,
        name="local",
    )(
        rows, halo, value_matrix, write_matrix, read_matrix, step_raw, new_rows, new_step, spike,
        value_filter_taps, write_filter_taps, read_filter_taps,
        head_log_decay, step_offset_bias, bypass_scale,
    )

    received = lax.all_to_all(send, "sp", 0, 0, tiled=True)

    base, lift, new_gate = call(
        inner_kernel,
        (shaped(length, channels), shaped(length, channels), shaped(8, channels)),
        grid=(blocks,),
        in_specs=[
            pl.BlockSpec((BLOCK, depth), lambda b: (b, 0)),
            pl.BlockSpec((depth, channels), lambda b: (0, 0)),
            pl.BlockSpec((1, depth), lambda b: (0, 0)),
            pl.BlockSpec((BLOCK, width), lambda b: (b, 0)),
            pl.BlockSpec((heads, BLOCK), lambda b: (0, b)),
            pl.BlockSpec((heads, BLOCK), lambda b: (0, b)),
            pl.BlockSpec((1, STATE, channels), lambda b: (b, 0, 0)),
            sm,
        ],
        out_specs=[
            pl.BlockSpec((BLOCK, channels), lambda b: (b, 0)),
            pl.BlockSpec((BLOCK, channels), lambda b: (b, 0)),
            pl.BlockSpec((8, channels), lambda b: (0, 0)),
        ],
        scratch=[pltpu.VMEM((heads, BLOCK), f32)],
        flops=2 * length * depth * channels,
        name="inner",
    )(tokens, gate_matrix, fresh, vwr, cum, dt, inside, bypass_scale)

    send_back, cache_rows, direct = call(
        prefix_kernel,
        (
            shaped(SUB, own, wide + channels, dtype=bf16),
            shaped(own, channels, dtype=bf16),
            shaped(1, channels),
        ),
        in_specs=[vm, vm, sm, sm],
        out_specs=[vm] * 3,
        scratch=[pltpu.VMEM((sequence_count, own, wide), f32)],
        name="prefix",
    )(received, new_step, head_log_decay, step_offset_bias)

    teams = [[SUB * t + i for i in range(SUB)] for t in range(pieces)]
    returned = lax.all_to_all(send_back, "sp", 0, 0, tiled=True, axis_index_groups=teams)

    prompt_out, step_row = call(
        finish_kernel,
        (
            shaped(length, channels, dtype=bf16),
            shaped(1, channels // sequence_count, dtype=bf16),
        ),
        grid=(1,),
        in_specs=[
            pl.BlockSpec(returned.shape, lambda i: (0, 0, 0)),
            pl.BlockSpec((length, channels), lambda i: (0, 0)),
            pl.BlockSpec((length, channels), lambda i: (0, 0)),
            pl.BlockSpec((length, STATE), lambda i: (0, (channels + STATE) // STATE)),
            pl.BlockSpec((1, group_norm_scale.shape[0]), lambda i: (0, 0)),
            pl.BlockSpec((1, channels), lambda i: (0, 0)),
            pl.BlockSpec((8, channels), lambda i: (0, 0)),
        ],
        out_specs=[
            pl.BlockSpec((length, channels), lambda i: (0, 0)),
            pl.BlockSpec((1, channels // sequence_count), lambda i: (0, 0)),
        ],
        name="finish",
    )(returned, base, lift, vwr, group_norm_scale[None], direct, new_gate)
    return (prompt_out, cache_rows, step_row.T)


def solution(mesh):
    placed = (
        P(("grp", "sp"), None),
        P("grp"),
        P(None, "tp"),
        P(None, "tp"),
        P(None, "tp"),
        P(None, "tp"),
        P(),
        P(),
        P(),
        P(),
        P(),
        P(),
        P(("grp", "sp"), "tp"),
        P(),
        P(),
    )
    return jax.shard_map(
        on_device,
        mesh=mesh,
        in_specs=placed,
        out_specs=(P(("grp", "sp"), "tp"), P(("grp", "sp"), "tp"), P(("grp", "tp"), "sp")),
        check_vma=False,
    )
```

```python
import jax
import jax.numpy as jnp
from jax import lax
from jax.experimental import pallas as pl
from jax.experimental.pallas import tpu as pltpu
from jax.sharding import PartitionSpec as P

HEAD = 64
STATE = 128
CONV = 4
BLOCK = 128
SUB = 32
MISC = 128
HALO = 8

epsilon = 1e-06
f32 = jnp.float32
bf16 = jnp.bfloat16
HIGHEST = lax.Precision.HIGHEST
VMEM_LIMIT = 56 * 1024 * 1024


def dot(a, b, dims=((1,), (0,)), precision=None):
    return lax.dot_general(a, b, (dims, ((), ())), precision=precision, preferred_element_type=f32)


def silu(x):
    return x / (1.0 + jnp.exp(-x))


def softplus(x):
    return jnp.maximum(x, 0.0) + jnp.log1p(jnp.exp(-jnp.abs(x)))


def iota(shape, dim):
    return lax.broadcasted_iota(jnp.int32, shape, dim)


def spread(heads, channels):
    return (iota((heads, channels), 0) == iota((heads, channels), 1) // HEAD).astype(f32)


def own_rows(table, rank, count):
    picked = table[0:count]
    for other in range(1, table.shape[0] // count):
        picked = jnp.where(rank == other, table[other * count : (other + 1) * count], picked)
    return picked


def head_column(ref, first, count, width):
    rows = iota((count, width), 0)
    column = jnp.full((count, width), ref[first], f32)
    for h in range(1, count):
        column = jnp.where(rows == h, ref[first + h], column)
    return column


def project_kernel(
    tok_ref, fresh_ref, wv_ref, ww_ref, wr_ref, ws_ref, rows_ref, step_ref, new_ref, newstep_ref,
    acc, accs, accn, accns,
):
    k = pl.program_id(0)
    last = pl.num_programs(0) - 1
    tok = tok_ref[...]
    fresh = jnp.broadcast_to(fresh_ref[...], (16, fresh_ref.shape[1]))
    weights = jnp.concatenate([wv_ref[...], ww_ref[...], wr_ref[...]], axis=1)
    part = dot(tok, weights)
    parts = dot(ws_ref[...], tok, ((1,), (1,)))
    partn = dot(fresh, weights)
    partns = dot(ws_ref[...], fresh, ((1,), (1,)))

    @pl.when(k == 0)
    def _():
        acc[...] = part
        accs[...] = parts
        accn[...] = partn
        accns[...] = partns

    @pl.when(k > 0)
    def _():
        acc[...] += part
        accs[...] += parts
        accn[...] += partn
        accns[...] += partns

    @pl.when(k == last)
    def _():
        rank = lax.axis_index("tp")
        heads = step_ref.shape[0]
        rows_ref[...] = acc[...].astype(bf16)
        step_ref[...] = own_rows(accs[...], rank, heads)
        new_ref[...] = accn[...][0:8]
        newstep_ref[...] = own_rows(accns[...], rank, heads)


def local_kernel(
    rows_ref, halo_ref, wv_ref, ww_ref, wr_ref, step_ref, new_ref, newstep_ref, spike_ref,
    vtap_ref, wtap_ref, rtap_ref, decay_ref, bias_ref, skip_ref,
    vwr_ref, cum_ref, dt_ref, inside_ref, send_ref, ext,
):
    rank = lax.axis_index("tp")
    length = rows_ref.shape[0]
    heads = step_ref.shape[0]
    channels = wv_ref.shape[1]
    first = rank * heads
    halo = halo_ref[...]
    before = jnp.concatenate(
        [dot(halo, wv_ref[...]), dot(halo, ww_ref[...]), dot(halo, wr_ref[...])], axis=1
    )
    ext[0:HALO] = before.astype(bf16).astype(f32)
    ext[HALO:] = rows_ref[...].astype(f32)
    taps = jnp.concatenate(
        [
            vtap_ref[:, pl.ds(pl.multiple_of(rank * channels, 128), channels)].astype(f32),
            wtap_ref[:, pl.ds(pl.multiple_of(rank * STATE, 128), STATE)].astype(f32),
            rtap_ref[:, pl.ds(pl.multiple_of(rank * STATE, 128), STATE)].astype(f32),
        ],
        axis=1,
    )
    off = HALO - (CONV - 1)
    summed = taps[0:1] * ext[off : off + length]
    for k in range(1, CONV):
        summed = summed + taps[k : k + 1] * ext[off + k : off + k + length]
    vwr = silu(summed).astype(bf16)
    vwr_ref[...] = vwr
    newest = taps[CONV - 1 : CONV] * new_ref[0:1].astype(bf16).astype(f32)
    for k in range(CONV - 1):
        row = length + off + k
        newest = newest + taps[k : k + 1] * ext[row : row + 1]
    newest = silu(newest).astype(bf16).astype(f32)
    new_value = newest[:, 0:channels]
    new_write = newest[:, channels : channels + STATE]
    new_read = newest[:, channels + STATE :]
    bias = head_column(bias_ref, first, heads, 128)
    rate = jnp.exp(head_column(decay_ref, first, heads, 128))
    upper = (iota((BLOCK, BLOCK), 0) <= iota((BLOCK, BLOCK), 1)).astype(f32)
    expand = spread(heads, channels)
    running = jnp.zeros((STATE, channels), f32)
    total = jnp.zeros((heads, 128), f32)
    for b in range(length // BLOCK):
        at = slice(b * BLOCK, (b + 1) * BLOCK)
        dt = softplus(step_ref[:, at] + bias)
        log_decay = spike_ref[:, at] - dt * rate
        cum = dot(log_decay, upper, precision=HIGHEST)
        dt_ref[:, at] = dt
        cum_ref[:, at] = cum
        end = jnp.broadcast_to(cum[:, BLOCK - 1 :], (heads, BLOCK))
        factor = dot(jnp.exp(end - cum) * dt, expand, ((0,), (0,)), HIGHEST)
        scaled = (factor * vwr[at, 0:channels].astype(f32)).astype(bf16)
        states = dot(vwr[at, channels : channels + STATE], scaled, ((0,), (0,)))
        fade = dot(jnp.exp(end), expand, ((0,), (0,)), HIGHEST)
        inside_ref[b] = running.astype(bf16)
        running = fade * running + states
        total = total + end
    fade = jnp.exp(total)
    high = fade.astype(bf16).astype(f32)
    low = fade - high
    shape = (STATE, MISC)
    lanes = iota(shape, 1)
    rows = iota(shape, 0)
    misc = jnp.zeros(shape, f32)
    for h in range(heads):
        misc = jnp.where(lanes == h, high[h : h + 1, 0:1], misc)
        misc = jnp.where(lanes == heads + h, low[h : h + 1, 0:1], misc)
    own = STATE // lax.axis_size("sp")
    stretch = SUB * own
    diagonal = jnp.where(rows == lanes, jnp.broadcast_to(new_read, shape), 0.0)
    read_column = jnp.sum(diagonal, axis=1, keepdims=True)
    new_dt = softplus(newstep_ref[...][:, 0:1] + bias[:, 0:1])
    skip = head_column(skip_ref, first, heads, 128)[:, 0:1]
    weight = new_dt * jnp.sum(new_read * new_write, axis=1, keepdims=True) + skip
    direct = jnp.sum(expand * weight, axis=0, keepdims=True) * new_value
    placed = jnp.where(iota((8, channels), 0) == iota((8, channels), 1) // HEAD, direct, 0.0)
    shift = (iota((channels, MISC), 0) % HEAD + (MISC - HEAD) == iota((channels, MISC), 1)).astype(f32)
    direct_rows = dot(placed, shift, precision=HIGHEST)[0:own]
    for g in range(STATE // stretch):
        at = slice(g * stretch, (g + 1) * stretch)
        piece = running[at].reshape(SUB, own, channels).astype(bf16)
        for copy in range(STATE // stretch):
            send_ref[copy * SUB : (copy + 1) * SUB, :, g * channels : (g + 1) * channels] = piece
    note = misc[0:stretch]
    for g in range(STATE // stretch):
        at = slice(g * stretch, (g + 1) * stretch)
        note = jnp.where(lanes[0:stretch] == 2 * heads + g, read_column[at], note)
    note = note.reshape(SUB, own, MISC)
    note = jnp.where(iota(note.shape, 2) >= MISC - HEAD, direct_rows[None], note).astype(bf16)
    wide = STATE // stretch * channels
    for copy in range(STATE // stretch):
        send_ref[copy * SUB : (copy + 1) * SUB, :, wide:] = note


def inner_kernel(
    tok_ref, wg_ref, fresh_ref, vwr_ref, cum_ref, dt_ref, inside_ref, skip_ref,
    base_ref, lift_ref, newgate_ref, before,
):
    b = pl.program_id(0)
    rank = lax.axis_index("tp")
    heads = cum_ref.shape[0]
    channels = wg_ref.shape[1]

    @pl.when(b == 0)
    def _():
        before[...] = jnp.zeros_like(before)
        fresh = jnp.broadcast_to(fresh_ref[...], (16, fresh_ref.shape[1]))
        gate = dot(fresh, wg_ref[...])[0:8].astype(bf16).astype(f32)
        newgate_ref[...] = silu(gate)

    expand = spread(heads, channels)
    skip = jnp.sum(
        expand * head_column(skip_ref, rank * heads, heads, channels), axis=0, keepdims=True
    )
    cum = cum_ref[...]
    dt = dt_ref[...]
    values = vwr_ref[:, 0:channels]
    writes = vwr_ref[:, channels : channels + STATE]
    reads = vwr_ref[:, channels + STATE :]
    gate = silu(dot(tok_ref[...], wg_ref[...]).astype(bf16).astype(f32))
    scores = dot(reads, writes, ((1,), (1,)))
    causal = iota((BLOCK, BLOCK), 0) >= iota((BLOCK, BLOCK), 1)
    columns = jnp.transpose(jnp.concatenate([cum, cum], axis=0))
    parts = []
    for h in range(heads):
        gap = columns[:, h : h + 1] - cum[h : h + 1]
        mixing = scores * jnp.exp(jnp.where(causal, gap, -jnp.inf)) * dt[h : h + 1]
        parts.append(dot(mixing.astype(bf16), values[:, h * HEAD : (h + 1) * HEAD]))
    inner = jnp.concatenate(parts, axis=1)
    fade = dot(jnp.exp(cum), expand, ((0,), (0,)), HIGHEST)
    carried = fade * dot(reads, inside_ref[0])
    base_ref[...] = (inner + carried + skip * values.astype(f32)) * gate
    far = jnp.exp(cum + before[...])
    lift_ref[...] = dot(far, expand, ((0,), (0,)), HIGHEST) * gate
    before[...] += jnp.broadcast_to(cum[:, BLOCK - 1 :], before.shape)


def prefix_kernel(recv_ref, newstep_ref, decay_ref, bias_ref, send_ref, cache_ref, direct_ref, states):
    rank = lax.axis_index("tp")
    place = lax.axis_index("sp")
    count = recv_ref.shape[0]
    own = recv_ref.shape[1]
    wide = recv_ref.shape[2] - MISC
    pieces = count // SUB
    channels = wide // pieces
    heads = channels // HEAD
    group = place // SUB
    notes = recv_ref[:, 0:1, wide:].astype(f32).reshape(count, MISC)
    lane = iota((MISC, channels), 0)
    owner = iota((MISC, channels), 1) // HEAD
    pick = jnp.where((lane == owner) | (lane == owner + heads), 1.0, 0.0)
    fades = dot(jnp.where(iota(notes.shape, 1) < 2 * heads, notes, 0.0), pick, precision=HIGHEST)
    state = jnp.zeros((own, wide), f32)
    for k in range(count):
        states[k] = state
        fade = jnp.concatenate([fades[k : k + 1]] * pieces, axis=1)
        state = fade * state + recv_ref[k, :, 0:wide].astype(f32)
    kept = state.astype(bf16)
    mine = kept[:, 0:channels]
    for g in range(1, pieces):
        mine = jnp.where(group == g, kept[:, g * channels : (g + 1) * channels], mine)
    cache_ref[...] = mine
    note = recv_ref[count - 1, :, wide:].astype(f32)
    reading = jnp.zeros((own, channels), f32)
    for g in range(pieces):
        column = note[:, 2 * heads + g : 2 * heads + g + 1]
        reading = reading + column * kept[:, g * channels : (g + 1) * channels].astype(f32)
    first = rank * heads
    bias = head_column(bias_ref, first, heads, 1)
    rate = jnp.exp(head_column(decay_ref, first, heads, 1))
    decay = jnp.exp(-softplus(newstep_ref[...][:, 0:1] + bias) * rate)
    decay = jnp.sum(spread(heads, channels) * decay, axis=0, keepdims=True)
    partial = jnp.sum(reading, axis=0, keepdims=True) * decay
    high = partial.astype(bf16).astype(f32)
    low = partial - high
    rows = iota((own, channels), 0)
    share = jnp.where(rows == 0, high, jnp.where(rows == 1, low, 0.0)).astype(bf16)
    chosen = states[pl.ds(group * SUB, SUB)]
    send_ref[:, :, 0:wide] = chosen.astype(bf16)
    send_ref[:, :, wide:] = jnp.broadcast_to(share[None], (SUB, own, channels))
    unshift = (iota((MISC, channels), 0) == iota((MISC, channels), 1) % HEAD + (MISC - HEAD)).astype(f32)
    laid = dot(note, unshift, precision=HIGHEST)
    direct_ref[...] = jnp.sum(jnp.where(rows == iota(rows.shape, 1) // HEAD, laid, 0.0), axis=0, keepdims=True)


def finish_kernel(recv_ref, base_ref, lift_ref, reads_ref, gain_ref, direct_ref, newgate_ref, out_ref, step_ref):
    rank = lax.axis_index("tp")
    place = lax.axis_index("sp")
    channels = base_ref.shape[1]
    wide = recv_ref.shape[2] - channels
    pieces = wide // channels
    own = recv_ref.shape[1]
    earlier = jnp.concatenate(
        [
            recv_ref[:, :, g * channels : (g + 1) * channels].astype(f32).reshape(SUB * own, channels)
            for g in range(pieces)
        ],
        axis=0,
    ).astype(bf16)
    gain = gain_ref[:, pl.ds(pl.multiple_of(rank * channels, 128), channels)]
    gated = base_ref[...] + dot(reads_ref[...], earlier) * lift_ref[...]
    scale = lax.rsqrt(jnp.mean(gated * gated, axis=1, keepdims=True) + epsilon)
    out_ref[...] = (gated * scale * gain).astype(bf16)
    partial = jnp.sum(jnp.sum(recv_ref[:, :, wide:].astype(f32), axis=0), axis=0, keepdims=True)
    new = (partial + direct_ref[...]) * newgate_ref[0:1]
    scale = lax.rsqrt(jnp.mean(new * new, axis=1, keepdims=True) + epsilon)
    step = (new * scale * gain).astype(bf16)
    columns = lax.axis_size("sp")
    channel = iota((channels, 128), 0)
    take = (channel // columns == iota((channels, 128), 1)) & (channel % columns == place)
    picked = dot(jnp.broadcast_to(step, (16, channels)), take.astype(bf16))
    step_ref[...] = picked[0:1, 0 : channels // columns].astype(bf16)


def call(kernel, out_shape, grid=None, in_specs=None, out_specs=None, scratch=(), flops=0, name=None):
    return pl.pallas_call(
        kernel,
        out_shape=out_shape,
        grid_spec=pltpu.PrefetchScalarGridSpec(
            num_scalar_prefetch=0,
            grid=grid or (),
            in_specs=in_specs,
            out_specs=out_specs,
            scratch_shapes=scratch,
        ),
        compiler_params=pltpu.CompilerParams(
            vmem_limit_bytes=VMEM_LIMIT,
            dimension_semantics=("arbitrary",) * len(grid or ()),
        ),
        cost_estimate=pl.CostEstimate(flops=flops, transcendentals=0, bytes_accessed=1 << 20),
        name=name,
    )


def shaped(*shape, dtype=f32):
    return jax.ShapeDtypeStruct(shape, dtype)


def on_device(
    tokens,
    fresh_token_input,
    value_matrix,
    write_matrix,
    read_matrix,
    gate_matrix,
    step_matrix,
    value_filter_taps,
    write_filter_taps,
    read_filter_taps,
    head_log_decay,
    step_offset_bias,
    decay_spike,
    bypass_scale,
    group_norm_scale,
):
    sequence_count = lax.axis_size("sp")
    length, depth = tokens.shape
    channels = value_matrix.shape[1]
    heads = channels // HEAD
    all_heads = step_matrix.shape[1]
    own = STATE // sequence_count
    pieces = sequence_count // SUB
    blocks = length // BLOCK
    width = channels + 2 * STATE
    vm = pl.BlockSpec(memory_space=pltpu.VMEM)
    sm = pl.BlockSpec(memory_space=pltpu.SMEM)

    halo = lax.ppermute(
        tokens[length - HALO :], "sp", [(i, i + 1) for i in range(sequence_count - 1)]
    )
    fresh = fresh_token_input[None]
    spike = decay_spike.T
    chunk = depth // 4
    rows, step_raw, new_rows, new_step = call(
        project_kernel,
        (
            shaped(length, width, dtype=bf16),
            shaped(heads, length),
            shaped(8, width),
            shaped(heads, 16),
        ),
        grid=(depth // chunk,),
        in_specs=[
            pl.BlockSpec((length, chunk), lambda k: (0, k)),
            pl.BlockSpec((1, chunk), lambda k: (0, k)),
            pl.BlockSpec((chunk, channels), lambda k: (k, 0)),
            pl.BlockSpec((chunk, STATE), lambda k: (k, 0)),
            pl.BlockSpec((chunk, STATE), lambda k: (k, 0)),
            pl.BlockSpec((all_heads, chunk), lambda k: (0, k)),
        ],
        out_specs=[
            pl.BlockSpec((length, width), lambda k: (0, 0)),
            pl.BlockSpec((heads, length), lambda k: (0, 0)),
            pl.BlockSpec((8, width), lambda k: (0, 0)),
            pl.BlockSpec((heads, 16), lambda k: (0, 0)),
        ],
        scratch=[
            pltpu.VMEM((length, width), f32),
            pltpu.VMEM((all_heads, length), f32),
            pltpu.VMEM((16, width), f32),
            pltpu.VMEM((all_heads, 16), f32),
        ],
        flops=2 * length * depth * width,
        name="project",
    )(tokens, fresh, value_matrix, write_matrix, read_matrix, step_matrix.T)

    wide = pieces * channels
    vwr, cum, dt, inside, send = call(
        local_kernel,
        (
            shaped(length, width, dtype=bf16),
            shaped(heads, length),
            shaped(heads, length),
            shaped(blocks, STATE, channels, dtype=bf16),
            shaped(sequence_count, own, wide + MISC, dtype=bf16),
        ),
        in_specs=[vm] * 12 + [sm] * 3,
        out_specs=[vm] * 5,
        scratch=[pltpu.VMEM((length + HALO, width), f32)],
        flops=2 * length * STATE * channels,
        name="local",
    )(
        rows, halo, value_matrix, write_matrix, read_matrix, step_raw, new_rows, new_step, spike,
        value_filter_taps, write_filter_taps, read_filter_taps,
        head_log_decay, step_offset_bias, bypass_scale,
    )

    received = lax.all_to_all(send, "sp", 0, 0, tiled=True)

    base, lift, new_gate = call(
        inner_kernel,
        (shaped(length, channels), shaped(length, channels), shaped(8, channels)),
        grid=(blocks,),
        in_specs=[
            pl.BlockSpec((BLOCK, depth), lambda b: (b, 0)),
            pl.BlockSpec((depth, channels), lambda b: (0, 0)),
            pl.BlockSpec((1, depth), lambda b: (0, 0)),
            pl.BlockSpec((BLOCK, width), lambda b: (b, 0)),
            pl.BlockSpec((heads, BLOCK), lambda b: (0, b)),
            pl.BlockSpec((heads, BLOCK), lambda b: (0, b)),
            pl.BlockSpec((1, STATE, channels), lambda b: (b, 0, 0)),
            sm,
        ],
        out_specs=[
            pl.BlockSpec((BLOCK, channels), lambda b: (b, 0)),
            pl.BlockSpec((BLOCK, channels), lambda b: (b, 0)),
            pl.BlockSpec((8, channels), lambda b: (0, 0)),
        ],
        scratch=[pltpu.VMEM((heads, BLOCK), f32)],
        flops=2 * length * depth * channels,
        name="inner",
    )(tokens, gate_matrix, fresh, vwr, cum, dt, inside, bypass_scale)

    send_back, cache_rows, direct = call(
        prefix_kernel,
        (
            shaped(SUB, own, wide + channels, dtype=bf16),
            shaped(own, channels, dtype=bf16),
            shaped(1, channels),
        ),
        in_specs=[vm, vm, sm, sm],
        out_specs=[vm] * 3,
        scratch=[pltpu.VMEM((sequence_count, own, wide), f32)],
        name="prefix",
    )(received, new_step, head_log_decay, step_offset_bias)

    teams = [[SUB * t + i for i in range(SUB)] for t in range(pieces)]
    teams = teams if pieces > 1 else None
    returned = lax.all_to_all(send_back, "sp", 0, 0, tiled=True, axis_index_groups=teams)

    prompt_out, step_row = call(
        finish_kernel,
        (
            shaped(length, channels, dtype=bf16),
            shaped(1, channels // sequence_count, dtype=bf16),
        ),
        grid=(1,),
        in_specs=[
            pl.BlockSpec(returned.shape, lambda i: (0, 0, 0)),
            pl.BlockSpec((length, channels), lambda i: (0, 0)),
            pl.BlockSpec((length, channels), lambda i: (0, 0)),
            pl.BlockSpec((length, STATE), lambda i: (0, (channels + STATE) // STATE)),
            pl.BlockSpec((1, group_norm_scale.shape[0]), lambda i: (0, 0)),
            pl.BlockSpec((1, channels), lambda i: (0, 0)),
            pl.BlockSpec((8, channels), lambda i: (0, 0)),
        ],
        out_specs=[
            pl.BlockSpec((length, channels), lambda i: (0, 0)),
            pl.BlockSpec((1, channels // sequence_count), lambda i: (0, 0)),
        ],
        name="finish",
    )(returned, base, lift, vwr, group_norm_scale[None], direct, new_gate)
    return (prompt_out, cache_rows, step_row.T)


def solution(mesh):
    placed = (
        P(("grp", "sp"), None),
        P("grp"),
        P(None, "tp"),
        P(None, "tp"),
        P(None, "tp"),
        P(None, "tp"),
        P(),
        P(),
        P(),
        P(),
        P(),
        P(),
        P(("grp", "sp"), "tp"),
        P(),
        P(),
    )
    return jax.shard_map(
        on_device,
        mesh=mesh,
        in_specs=placed,
        out_specs=(P(("grp", "sp"), "tp"), P(("grp", "sp"), "tp"), P(("grp", "tp"), "sp")),
        check_vma=False,
    )
```

```python
import jax
import jax.numpy as jnp
from jax import lax
from jax.experimental import pallas as pl
from jax.experimental.pallas import tpu as pltpu
from jax.sharding import PartitionSpec as P

HEAD = 64
STATE = 128
CONV = 4
BLOCK = 128
TEAM = 8
MISC = 128
HALO = 8

epsilon = 1e-06
f32 = jnp.float32
bf16 = jnp.bfloat16
HIGHEST = lax.Precision.HIGHEST
VMEM_LIMIT = 24 * 1024 * 1024
SPLIT = 4


def dot(a, b, dims=((1,), (0,)), precision=None):
    return lax.dot_general(a, b, (dims, ((), ())), precision=precision, preferred_element_type=f32)


def silu(x):
    return x / (1.0 + jnp.exp(-x))


def softplus(x):
    return jnp.maximum(x, 0.0) + jnp.log1p(jnp.exp(-jnp.abs(x)))


def iota(shape, dim):
    return lax.broadcasted_iota(jnp.int32, shape, dim)


def spread(heads, channels):
    return (iota((heads, channels), 0) == iota((heads, channels), 1) // HEAD).astype(f32)


def own_rows(table, rank, count):
    picked = table[0:count]
    for other in range(1, table.shape[0] // count):
        picked = jnp.where(rank == other, table[other * count : (other + 1) * count], picked)
    return picked


def head_column(ref, first, count, width):
    rows = iota((count, width), 0)
    column = jnp.full((count, width), ref[first], f32)
    for h in range(1, count):
        column = jnp.where(rows == h, ref[first + h], column)
    return column


def project_kernel(
    tok_hbm, fresh_ref, wv_hbm, ww_hbm, wr_hbm, ws_ref,
    rows_ref, weights, step_ref, new_ref, newstep_ref, tok, sems,
):
    depth = tok.shape[1]
    channels = wv_hbm.shape[1]
    state = ww_hbm.shape[1]
    chunk = depth // SPLIT
    copies = []
    for k in range(SPLIT):
        at = pl.ds(k * chunk, chunk)
        moves = [
            (tok_hbm.at[:, at], tok.at[:, at]),
            (wv_hbm.at[at], weights.at[at, 0:channels]),
            (ww_hbm.at[at], weights.at[at, channels : channels + state]),
            (wr_hbm.at[at], weights.at[at, channels + state : channels + 2 * state]),
        ]
        copies.append(
            [pltpu.make_async_copy(a, b, sems.at[k, i]) for i, (a, b) in enumerate(moves)]
        )
        for copy in copies[-1]:
            copy.start()
    rank = lax.axis_index("tp")
    heads = step_ref.shape[0]
    acc = accs = accn = accns = None
    lines = fresh_ref[...].astype(f32)
    for k in range(SPLIT):
        at = slice(k * chunk, (k + 1) * chunk)
        each = chunk // 128
        fresh = jnp.concatenate([lines[k * each + i : k * each + i + 1] for i in range(each)], axis=1)
        fresh = jnp.broadcast_to(fresh, (8, chunk)).astype(bf16)
        for copy in copies[k]:
            copy.wait()
        part = dot(tok[:, at], weights[at])
        parts = dot(ws_ref[:, at], tok[:, at], ((1,), (1,)))
        partn = dot(fresh, weights[at])
        partns = dot(ws_ref[:, at], fresh, ((1,), (1,)))
        acc = part if k == 0 else acc + part
        accs = parts if k == 0 else accs + parts
        accn = partn if k == 0 else accn + partn
        accns = partns if k == 0 else accns + partns
    rows_ref[...] = acc.astype(bf16)
    step_ref[...] = own_rows(accs, rank, heads)
    new_ref[...] = accn
    newstep_ref[...] = own_rows(accns, rank, heads)


def local_kernel(
    rows_ref, halo_ref, weights, step_ref, new_ref, newstep_ref, spike_ref,
    vtap_ref, wtap_ref, rtap_ref, decay_ref, bias_ref, skip_ref,
    vwr_ref, cum_ref, dt_ref, inside_ref, send_ref, ext,
):
    rank = lax.axis_index("tp")
    length = rows_ref.shape[0]
    heads = step_ref.shape[0]
    channels = rows_ref.shape[1] - 2 * STATE
    first = rank * heads
    halo = halo_ref[...]
    before = dot(halo, weights[...])
    ext[0:HALO] = before.astype(bf16).astype(f32)
    ext[HALO:] = rows_ref[...].astype(f32)
    taps = jnp.concatenate(
        [
            vtap_ref[:, pl.ds(pl.multiple_of(rank * channels, 128), channels)].astype(f32),
            wtap_ref[:, pl.ds(pl.multiple_of(rank * STATE, 128), STATE)].astype(f32),
            rtap_ref[:, pl.ds(pl.multiple_of(rank * STATE, 128), STATE)].astype(f32),
        ],
        axis=1,
    )
    off = HALO - (CONV - 1)
    summed = taps[0:1] * ext[off : off + length]
    for k in range(1, CONV):
        summed = summed + taps[k : k + 1] * ext[off + k : off + k + length]
    vwr = silu(summed).astype(bf16)
    vwr_ref[...] = vwr
    newest = taps[CONV - 1 : CONV] * new_ref[0:1].astype(bf16).astype(f32)
    for k in range(CONV - 1):
        row = length + off + k
        newest = newest + taps[k : k + 1] * ext[row : row + 1]
    newest = silu(newest).astype(bf16).astype(f32)
    new_value = newest[:, 0:channels]
    new_write = newest[:, channels : channels + STATE]
    new_read = newest[:, channels + STATE :]
    bias = head_column(bias_ref, first, heads, 128)
    rate = jnp.exp(head_column(decay_ref, first, heads, 128))
    upper = (iota((BLOCK, BLOCK), 0) <= iota((BLOCK, BLOCK), 1)).astype(f32)
    expand = spread(heads, channels)
    running = jnp.zeros((STATE, channels), f32)
    total = jnp.zeros((heads, 128), f32)
    for b in range(length // BLOCK):
        at = slice(b * BLOCK, (b + 1) * BLOCK)
        dt = softplus(step_ref[:, at] + bias)
        log_decay = spike_ref[:, at] - dt * rate
        cum = dot(log_decay, upper, precision=HIGHEST)
        dt_ref[:, at] = dt
        cum_ref[:, at] = cum
        end = jnp.broadcast_to(cum[:, BLOCK - 1 :], (heads, BLOCK))
        factor = dot(jnp.exp(end - cum) * dt, expand, ((0,), (0,)), HIGHEST)
        scaled = (factor * vwr[at, 0:channels].astype(f32)).astype(bf16)
        states = dot(vwr[at, channels : channels + STATE], scaled, ((0,), (0,)))
        fade = dot(jnp.exp(end), expand, ((0,), (0,)), HIGHEST)
        inside_ref[b] = running.astype(bf16)
        running = fade * running + states
        total = total + end
    fade = jnp.exp(total)
    high = fade.astype(bf16).astype(f32)
    low = fade - high
    shape = (STATE, MISC)
    lanes = iota(shape, 1)
    rows = iota(shape, 0)
    misc = jnp.zeros(shape, f32)
    for h in range(heads):
        misc = jnp.where(lanes == h, high[h : h + 1, 0:1], misc)
        misc = jnp.where(lanes == heads + h, low[h : h + 1, 0:1], misc)
    own = STATE // lax.axis_size("sp")
    stretch = TEAM * own
    teams = STATE // stretch
    diagonal = jnp.where(rows == lanes, jnp.broadcast_to(new_read, shape), 0.0)
    read_column = jnp.sum(diagonal, axis=1, keepdims=True)
    new_dt = softplus(newstep_ref[...][:, 0:1] + bias[:, 0:1])
    skip = head_column(skip_ref, first, heads, 128)[:, 0:1]
    weight = new_dt * jnp.sum(new_read * new_write, axis=1, keepdims=True) + skip
    direct = jnp.sum(expand * weight, axis=0, keepdims=True) * new_value
    placed = jnp.where(iota((8, channels), 0) == iota((8, channels), 1) // HEAD, direct, 0.0)
    shift = (iota((channels, MISC), 0) % HEAD + (MISC - HEAD) == iota((channels, MISC), 1)).astype(f32)
    direct_rows = dot(placed, shift, precision=HIGHEST)[0:own]
    for g in range(teams):
        at = slice(g * stretch, (g + 1) * stretch)
        piece = running[at].reshape(TEAM, own, channels).astype(bf16)
        send_ref[:, :, g * channels : (g + 1) * channels] = piece
    note = misc[0:stretch]
    for g in range(teams):
        at = slice(g * stretch, (g + 1) * stretch)
        note = jnp.where(lanes[0:stretch] == 2 * heads + g, read_column[at], note)
    note = note.reshape(TEAM, own, MISC)
    note = jnp.where(iota(note.shape, 2) >= MISC - HEAD, direct_rows[None], note).astype(bf16)
    send_ref[:, :, teams * channels :] = note


def inner_kernel(
    tok_ref, wg_ref, fresh_ref, vwr_ref, cum_ref, dt_ref, inside_ref, skip_ref,
    base_ref, lift_ref, newgate_ref, before,
):
    b = pl.program_id(0)
    rank = lax.axis_index("tp")
    heads = cum_ref.shape[0]
    channels = wg_ref.shape[1]

    @pl.when(b == 0)
    def _():
        before[...] = jnp.zeros_like(before)
        lines = fresh_ref[...].astype(f32)
        fresh = jnp.concatenate([lines[i : i + 1] for i in range(lines.shape[0])], axis=1)
        fresh = jnp.broadcast_to(fresh, (8, fresh.shape[1])).astype(bf16)
        gate = dot(fresh, wg_ref[...]).astype(bf16).astype(f32)
        newgate_ref[...] = silu(gate)

    expand = spread(heads, channels)
    skip = jnp.sum(
        expand * head_column(skip_ref, rank * heads, heads, channels), axis=0, keepdims=True
    )
    cum = cum_ref[...]
    dt = dt_ref[...]
    values = vwr_ref[:, 0:channels]
    writes = vwr_ref[:, channels : channels + STATE]
    reads = vwr_ref[:, channels + STATE :]
    gate = silu(dot(tok_ref[...], wg_ref[...]).astype(bf16).astype(f32))
    scores = dot(reads, writes, ((1,), (1,)))
    causal = iota((BLOCK, BLOCK), 0) >= iota((BLOCK, BLOCK), 1)
    columns = jnp.transpose(jnp.concatenate([cum, cum], axis=0))
    parts = []
    for h in range(heads):
        gap = columns[:, h : h + 1] - cum[h : h + 1]
        mixing = scores * jnp.exp(jnp.where(causal, gap, -jnp.inf)) * dt[h : h + 1]
        parts.append(dot(mixing.astype(bf16), values[:, h * HEAD : (h + 1) * HEAD]))
    inner = jnp.concatenate(parts, axis=1)
    fade = dot(jnp.exp(cum), expand, ((0,), (0,)), HIGHEST)
    carried = fade * dot(reads, inside_ref[0])
    base_ref[...] = (inner + carried + skip * values.astype(f32)) * gate
    far = jnp.exp(cum + before[...])
    lift_ref[...] = dot(far, expand, ((0,), (0,)), HIGHEST) * gate
    before[...] += jnp.broadcast_to(cum[:, BLOCK - 1 :], before.shape)


def fades_of(notes, heads, channels):
    lane = iota((MISC, channels), 0)
    owner = iota((MISC, channels), 1) // HEAD
    pick = jnp.where((lane == owner) | (lane == owner + heads), 1.0, 0.0)
    return dot(jnp.where(iota(notes.shape, 1) < 2 * heads, notes, 0.0), pick, precision=HIGHEST)


def team_kernel(recv_ref, send_ref, local_ref, reach_ref):
    count, own, width = recv_ref.shape
    wide = width - MISC
    teams = send_ref.shape[0]
    channels = wide // teams
    heads = channels // HEAD
    notes = recv_ref[:, 0:1, wide:].astype(f32).reshape(count, MISC)
    fades = fades_of(notes, heads, channels)
    state = jnp.zeros((own, wide), f32)
    reach = jnp.ones((1, channels), f32)
    for k in range(count):
        local_ref[k] = state
        reach_ref[k : k + 1] = reach
        fade = jnp.concatenate([fades[k : k + 1]] * teams, axis=1)
        state = fade * state + recv_ref[k, :, 0:wide].astype(f32)
        reach = reach * fades[k : k + 1]
    total = state.astype(bf16)
    note = recv_ref[count - 1, :, wide:].astype(f32)
    first = (iota((channels, MISC), 0) == iota((channels, MISC), 1) * HEAD).astype(f32)
    high = reach.astype(bf16).astype(f32)
    low = reach - high
    packed = dot(jnp.concatenate([high, low, jnp.zeros((6, channels), f32)], axis=0), first, precision=HIGHEST)
    shifted = (iota((MISC, MISC), 0) + heads == iota((MISC, MISC), 1)).astype(f32)
    moved = dot(packed, shifted, precision=HIGHEST)
    lanes = iota((own, MISC), 1)
    note = jnp.where(lanes < heads, packed[0:1], jnp.where(lanes < 2 * heads, moved[1:2], note)).astype(bf16)
    for t in range(teams):
        send_ref[t, :, 0:wide] = total
        send_ref[t, :, wide:] = note


def prefix_kernel(recv_ref, local_ref, reach_ref, newstep_ref, decay_ref, bias_ref, send_ref, cache_ref, direct_ref):
    rank = lax.axis_index("tp")
    teams, own, width = recv_ref.shape
    wide = width - MISC
    channels = wide // teams
    heads = channels // HEAD
    group = lax.axis_index("sp") // TEAM
    notes = recv_ref[:, 0:1, wide:].astype(f32).reshape(teams, MISC)
    fades = fades_of(notes, heads, channels)
    state = jnp.zeros((own, wide), f32)
    entering = state
    for t in range(teams):
        entering = jnp.where(group == t, state, entering)
        fade = jnp.concatenate([fades[t : t + 1]] * teams, axis=1)
        state = fade * state + recv_ref[t, :, 0:wide].astype(f32)
    for k in range(TEAM):
        reach = jnp.concatenate([reach_ref[k : k + 1]] * teams, axis=1)
        send_ref[k, :, 0:wide] = (local_ref[k] + reach * entering).astype(bf16)
    kept = state.astype(bf16).astype(f32)
    mine = kept[:, 0:channels]
    for g in range(1, teams):
        mine = jnp.where(group == g, kept[:, g * channels : (g + 1) * channels], mine)
    cache_ref[...] = mine.astype(bf16)
    note = recv_ref[teams - 1, :, wide:].astype(f32)
    reading = jnp.zeros((own, channels), f32)
    for g in range(teams):
        column = note[:, 2 * heads + g : 2 * heads + g + 1]
        reading = reading + column * kept[:, g * channels : (g + 1) * channels]
    first = rank * heads
    bias = head_column(bias_ref, first, heads, 1)
    rate = jnp.exp(head_column(decay_ref, first, heads, 1))
    decay = jnp.exp(-softplus(newstep_ref[...][:, 0:1] + bias) * rate)
    decay = jnp.sum(spread(heads, channels) * decay, axis=0, keepdims=True)
    partial = jnp.sum(reading, axis=0, keepdims=True) * decay
    high = partial.astype(bf16).astype(f32)
    low = partial - high
    rows = iota((own, channels), 0)
    share = jnp.where(rows == 0, high, jnp.where(rows == 1, low, 0.0)).astype(bf16)
    send_ref[:, :, wide:] = jnp.broadcast_to(share[None], (TEAM, own, channels))
    unshift = (iota((MISC, channels), 0) == iota((MISC, channels), 1) % HEAD + (MISC - HEAD)).astype(f32)
    laid = dot(note, unshift, precision=HIGHEST)
    direct_ref[...] = jnp.sum(jnp.where(rows == iota(rows.shape, 1) // HEAD, laid, 0.0), axis=0, keepdims=True)


def finish_kernel(recv_ref, base_ref, lift_ref, reads_ref, gain_ref, direct_ref, newgate_ref, out_ref, step_ref):
    rank = lax.axis_index("tp")
    place = lax.axis_index("sp")
    channels = base_ref.shape[1]
    wide = recv_ref.shape[2] - channels
    pieces = wide // channels
    own = recv_ref.shape[1]
    earlier = jnp.concatenate(
        [
            recv_ref[:, :, g * channels : (g + 1) * channels].astype(f32).reshape(TEAM * own, channels)
            for g in range(pieces)
        ],
        axis=0,
    ).astype(bf16)
    gain = gain_ref[:, pl.ds(pl.multiple_of(rank * channels, 128), channels)]
    gated = base_ref[...] + dot(reads_ref[:, channels + STATE :], earlier) * lift_ref[...]
    scale = lax.rsqrt(jnp.mean(gated * gated, axis=1, keepdims=True) + epsilon)
    out_ref[...] = (gated * scale * gain).astype(bf16)
    partial = jnp.sum(jnp.sum(recv_ref[:, :, wide:].astype(f32), axis=0), axis=0, keepdims=True)
    new = (partial + direct_ref[...]) * newgate_ref[0:1]
    scale = lax.rsqrt(jnp.mean(new * new, axis=1, keepdims=True) + epsilon)
    step = (new * scale * gain).astype(bf16)
    columns = lax.axis_size("sp")
    channel = iota((channels, 128), 0)
    take = (channel // columns == iota((channels, 128), 1)) & (channel % columns == place)
    picked = dot(jnp.broadcast_to(step, (16, channels)), take.astype(bf16))
    step_ref[...] = picked[0:1, 0 : channels // columns].astype(bf16)


def call(kernel, out_shape, grid=None, in_specs=None, out_specs=None, scratch=(), flops=0, name=None):
    return pl.pallas_call(
        kernel,
        out_shape=out_shape,
        grid_spec=pltpu.PrefetchScalarGridSpec(
            num_scalar_prefetch=0,
            grid=grid or (),
            in_specs=in_specs,
            out_specs=out_specs,
            scratch_shapes=scratch,
        ),
        compiler_params=pltpu.CompilerParams(
            vmem_limit_bytes=VMEM_LIMIT,
            dimension_semantics=("arbitrary",) * len(grid or ()),
        ),
        cost_estimate=pl.CostEstimate(flops=flops, transcendentals=0, bytes_accessed=1 << 20),
        name=name,
    )


def shaped(*shape, dtype=f32):
    return jax.ShapeDtypeStruct(shape, dtype)


def near(*shape, dtype=f32):
    return pltpu.VMEM(shape, dtype)


def held(array):
    return pltpu.with_memory_space_constraint(array, pltpu.VMEM)


def stored(array):
    return pltpu.with_memory_space_constraint(array, pltpu.HBM)


def on_device(
    tokens,
    fresh_token_input,
    value_matrix,
    write_matrix,
    read_matrix,
    gate_matrix,
    step_matrix,
    value_filter_taps,
    write_filter_taps,
    read_filter_taps,
    head_log_decay,
    step_offset_bias,
    decay_spike,
    bypass_scale,
    group_norm_scale,
):
    sequence_count = lax.axis_size("sp")
    length, depth = tokens.shape
    channels = value_matrix.shape[1]
    heads = channels // HEAD
    own = STATE // sequence_count
    teams = sequence_count // TEAM
    blocks = length // BLOCK
    width = channels + 2 * STATE
    wide = teams * channels
    vm = pl.BlockSpec(memory_space=pltpu.VMEM)
    sm = pl.BlockSpec(memory_space=pltpu.SMEM)
    far = pl.BlockSpec(memory_space=pltpu.HBM)
    inside_team = [[TEAM * t + i for i in range(TEAM)] for t in range(teams)]
    across_teams = [[TEAM * t + i for t in range(teams)] for i in range(TEAM)]

    halo = lax.ppermute(
        tokens[length - HALO :], "sp", [(i, i + 1) for i in range(sequence_count - 1)]
    )
    fresh = fresh_token_input.reshape(depth // 128, 128)
    spike = decay_spike.T
    rows, weights, step_raw, new_rows, new_step = call(
        project_kernel,
        (
            near(length, width, dtype=bf16),
            near(depth, width, dtype=bf16),
            near(heads, length),
            near(8, width),
            near(heads, 8),
        ),
        in_specs=[far, vm, far, far, far, vm],
        out_specs=[vm] * 5,
        scratch=[pltpu.VMEM((length, depth), bf16), pltpu.SemaphoreType.DMA((SPLIT, 4))],
        flops=2 * length * depth * width,
        name="project",
    )(
        stored(tokens), fresh, stored(value_matrix), stored(write_matrix), stored(read_matrix),
        step_matrix.T,
    )

    vwr, cum, dt, inside, send = call(
        local_kernel,
        (
            near(length, width, dtype=bf16),
            near(heads, length),
            near(heads, length),
            near(blocks, STATE, channels, dtype=bf16),
            near(TEAM, own, wide + MISC, dtype=bf16),
        ),
        in_specs=[vm] * 10 + [sm] * 3,
        out_specs=[vm] * 5,
        scratch=[pltpu.VMEM((length + HALO, width), f32)],
        flops=2 * length * STATE * channels,
        name="local",
    )(
        held(rows), held(halo), held(weights), held(step_raw), held(new_rows), held(new_step), spike,
        value_filter_taps, write_filter_taps, read_filter_taps,
        head_log_decay, step_offset_bias, bypass_scale,
    )

    received = lax.all_to_all(held(send), "sp", 0, 0, tiled=True, axis_index_groups=inside_team)

    send, local_states, reach = call(
        team_kernel,
        (
            near(teams, own, wide + MISC, dtype=bf16),
            near(TEAM, own, wide),
            near(TEAM, channels),
        ),
        in_specs=[vm],
        out_specs=[vm] * 3,
        name="team",
    )(held(received))

    received = lax.all_to_all(held(send), "sp", 0, 0, tiled=True, axis_index_groups=across_teams)

    base, lift, new_gate = call(
        inner_kernel,
        (near(length, channels), near(length, channels), near(8, channels)),
        grid=(blocks,),
        in_specs=[
            pl.BlockSpec((BLOCK, depth), lambda b: (b, 0)),
            pl.BlockSpec((depth, channels), lambda b: (0, 0)),
            pl.BlockSpec((depth // 128, 128), lambda b: (0, 0)),
            pl.BlockSpec((BLOCK, width), lambda b: (b, 0)),
            pl.BlockSpec((heads, BLOCK), lambda b: (0, b)),
            pl.BlockSpec((heads, BLOCK), lambda b: (0, b)),
            pl.BlockSpec((1, STATE, channels), lambda b: (b, 0, 0)),
            sm,
        ],
        out_specs=[
            pl.BlockSpec((BLOCK, channels), lambda b: (b, 0)),
            pl.BlockSpec((BLOCK, channels), lambda b: (b, 0)),
            pl.BlockSpec((8, channels), lambda b: (0, 0)),
        ],
        scratch=[pltpu.VMEM((heads, BLOCK), f32)],
        flops=2 * length * depth * channels,
        name="inner",
    )(
        stored(tokens), stored(gate_matrix), fresh, held(vwr), held(cum), held(dt), held(inside),
        bypass_scale,
    )

    send, cache_rows, direct = call(
        prefix_kernel,
        (
            near(TEAM, own, wide + channels, dtype=bf16),
            shaped(own, channels, dtype=bf16),
            near(1, channels),
        ),
        in_specs=[vm] * 4 + [sm] * 2,
        out_specs=[vm] * 3,
        name="prefix",
    )(held(received), held(local_states), held(reach), held(new_step), head_log_decay, step_offset_bias)

    received = lax.all_to_all(held(send), "sp", 0, 0, tiled=True, axis_index_groups=inside_team)

    prompt_out, step_row = call(
        finish_kernel,
        (
            shaped(length, channels, dtype=bf16),
            shaped(1, channels // sequence_count, dtype=bf16),
        ),
        in_specs=[vm] * 7,
        out_specs=[vm] * 2,
        name="finish",
    )(
        held(received), held(base), held(lift), held(vwr), group_norm_scale[None],
        held(direct), held(new_gate),
    )
    return (prompt_out, cache_rows, step_row.T)


def solution(mesh):
    placed = (
        P(("grp", "sp"), None),
        P("grp"),
        P(None, "tp"),
        P(None, "tp"),
        P(None, "tp"),
        P(None, "tp"),
        P(),
        P(),
        P(),
        P(),
        P(),
        P(),
        P(("grp", "sp"), "tp"),
        P(),
        P(),
    )
    return jax.shard_map(
        on_device,
        mesh=mesh,
        in_specs=placed,
        out_specs=(P(("grp", "sp"), "tp"), P(("grp", "sp"), "tp"), P(("grp", "tp"), "sp")),
        check_vma=False,
    )
```

```python
import jax
import jax.numpy as jnp
from jax import lax
from jax.experimental import pallas as pl
from jax.experimental.pallas import tpu as pltpu
from jax.sharding import PartitionSpec as P

HEAD = 64
STATE = 128
CONV = 4
BLOCK = 128
TEAM = 4
MISC = 128
HALO = 8

epsilon = 1e-06
f32 = jnp.float32
bf16 = jnp.bfloat16
HIGHEST = lax.Precision.HIGHEST
VMEM_LIMIT = 24 * 1024 * 1024
SPLIT = 4


def dot(a, b, dims=((1,), (0,)), precision=None):
    return lax.dot_general(a, b, (dims, ((), ())), precision=precision, preferred_element_type=f32)


def silu(x):
    return x / (1.0 + jnp.exp(-x))


def softplus(x):
    return jnp.maximum(x, 0.0) + jnp.log1p(jnp.exp(-jnp.abs(x)))


def iota(shape, dim):
    return lax.broadcasted_iota(jnp.int32, shape, dim)


def spread(heads, channels):
    return (iota((heads, channels), 0) == iota((heads, channels), 1) // HEAD).astype(f32)


def own_rows(table, rank, count):
    picked = table[0:count]
    for other in range(1, table.shape[0] // count):
        picked = jnp.where(rank == other, table[other * count : (other + 1) * count], picked)
    return picked


def head_column(ref, first, count):
    row = ref[...]
    shape = (count, row.shape[1])
    return jnp.sum(jnp.where(iota(shape, 1) == iota(shape, 0) + first, row, 0.0), axis=1, keepdims=True)


def project_kernel(
    tok_hbm, fresh_hbm, wv_hbm, ww_hbm, wr_hbm, ws_hbm,
    rows_ref, weights, step_ref, new_ref, newstep_ref, tok, lines, steps, sems, small,
):
    length, depth = tok_hbm.shape
    channels = wv_hbm.shape[1]
    state = ww_hbm.shape[1]
    chunk = depth // SPLIT
    first = [
        pltpu.make_async_copy(fresh_hbm, lines, small.at[0]),
        pltpu.make_async_copy(ws_hbm, steps, small.at[1]),
    ]
    for copy in first:
        copy.start()
    copies = []
    for k in range(SPLIT):
        at = pl.ds(k * chunk, chunk)
        moves = [
            (tok_hbm.at[:, at], tok.at[pl.ds(0, length), at]),
            (wv_hbm.at[at], weights.at[at, pl.ds(0, channels)]),
            (ww_hbm.at[at], weights.at[at, pl.ds(channels, state)]),
            (wr_hbm.at[at], weights.at[at, pl.ds(channels + state, state)]),
        ]
        copies.append(
            [pltpu.make_async_copy(a, b, sems.at[k, i]) for i, (a, b) in enumerate(moves)]
        )
        for copy in copies[-1]:
            copy.start()
    rank = lax.axis_index("tp")
    heads = step_ref.shape[0]
    extra = tok.shape[0] - length
    for copy in first:
        copy.wait()
    rows = lines[...].astype(f32)
    fresh = jnp.concatenate([rows[i : i + 1] for i in range(depth // 128)], axis=1)
    tok[length:] = jnp.broadcast_to(fresh, (extra, depth)).astype(bf16)
    acc = accs = None
    for k in range(SPLIT):
        at = slice(k * chunk, (k + 1) * chunk)
        for copy in copies[k]:
            copy.wait()
        part = dot(tok[:, at], weights[at])
        parts = dot(steps[:, at], tok[:, at], ((1,), (1,)))
        acc = part if k == 0 else acc + part
        accs = parts if k == 0 else accs + parts
    rows_ref[...] = acc[0:length].astype(bf16)
    new_ref[...] = acc[length : length + 8]
    accs = own_rows(accs, rank, heads)
    step_ref[...] = accs[:, 0:length]
    newstep_ref[...] = accs[:, length : length + 8]


def local_kernel(
    rows_ref, halo_ref, weights, step_ref, new_ref, newstep_ref, spike_ref,
    vtap_ref, wtap_ref, rtap_ref, decay_ref, bias_ref, skip_ref,
    vw_ref, edge_ref, cum_ref, dt_ref, inside_ref, newdecay_ref, send_ref, ext,
):
    rank = lax.axis_index("tp")
    length = rows_ref.shape[0]
    heads = step_ref.shape[0]
    channels = rows_ref.shape[1] - 2 * STATE
    first = rank * heads
    halo = halo_ref[...]
    before = dot(halo, weights[...])
    before = before.astype(bf16).astype(f32)
    used = channels + STATE
    edge_ref[...] = before[:, used:]
    ext[0:HALO] = before[:, 0:used]
    ext[HALO:] = rows_ref[:, 0:used].astype(f32)
    taps = jnp.concatenate(
        [
            vtap_ref[:, pl.ds(pl.multiple_of(rank * channels, 128), channels)].astype(f32),
            wtap_ref[:, pl.ds(pl.multiple_of(rank * STATE, 128), STATE)].astype(f32),
            rtap_ref[:, pl.ds(pl.multiple_of(rank * STATE, 128), STATE)].astype(f32),
        ],
        axis=1,
    )
    off = HALO - (CONV - 1)
    summed = taps[0:1, 0:used] * ext[off : off + length]
    for k in range(1, CONV):
        summed = summed + taps[k : k + 1, 0:used] * ext[off + k : off + k + length]
    vwr = silu(summed).astype(bf16)
    vw_ref[...] = vwr
    newest = taps[CONV - 1 : CONV] * new_ref[0:1].astype(bf16).astype(f32)
    ending = rows_ref[length - 16 :].astype(f32)
    for k in range(CONV - 1):
        row = 16 - (CONV - 1) + k
        newest = newest + taps[k : k + 1] * ending[row : row + 1]
    newest = silu(newest).astype(bf16).astype(f32)
    new_value = newest[:, 0:channels]
    new_write = newest[:, channels : channels + STATE]
    new_read = newest[:, channels + STATE :]
    bias = head_column(bias_ref, first, heads)
    rate = jnp.exp(head_column(decay_ref, first, heads))
    upper = (iota((BLOCK, BLOCK), 0) <= iota((BLOCK, BLOCK), 1)).astype(f32)
    expand = spread(heads, channels)
    running = jnp.zeros((STATE, channels), f32)
    total = jnp.zeros((heads, 128), f32)
    for b in range(length // BLOCK):
        at = slice(b * BLOCK, (b + 1) * BLOCK)
        dt = softplus(step_ref[:, at] + bias)
        log_decay = spike_ref[:, at] - dt * rate
        cum = dot(log_decay, upper, precision=HIGHEST)
        dt_ref[:, at] = dt
        cum_ref[:, at] = cum
        end = jnp.broadcast_to(cum[:, BLOCK - 1 :], (heads, BLOCK))
        factor = dot(jnp.exp(end - cum) * dt, expand, ((0,), (0,)), HIGHEST)
        scaled = (factor * vwr[at, 0:channels].astype(f32)).astype(bf16)
        states = dot(vwr[at, channels : channels + STATE], scaled, ((0,), (0,)))
        fade = dot(jnp.exp(end), expand, ((0,), (0,)), HIGHEST)
        inside_ref[b] = running.astype(bf16)
        running = fade * running + states
        total = total + end
    fade = jnp.exp(total)
    high = fade.astype(bf16).astype(f32)
    low = fade - high
    shape = (STATE, MISC)
    lanes = iota(shape, 1)
    rows = iota(shape, 0)
    misc = jnp.zeros(shape, f32)
    for h in range(heads):
        misc = jnp.where(lanes == h, high[h : h + 1, 0:1], misc)
        misc = jnp.where(lanes == heads + h, low[h : h + 1, 0:1], misc)
    own = STATE // lax.axis_size("sp")
    stretch = TEAM * own
    teams = STATE // stretch
    diagonal = jnp.where(rows == lanes, jnp.broadcast_to(new_read, shape), 0.0)
    read_column = jnp.sum(diagonal, axis=1, keepdims=True)
    new_dt = softplus(newstep_ref[...][:, 0:1] + bias)
    newdecay_ref[...] = jnp.sum(expand * jnp.exp(-new_dt * rate), axis=0, keepdims=True)
    skip = head_column(skip_ref, first, heads)
    weight = new_dt * jnp.sum(new_read * new_write, axis=1, keepdims=True) + skip
    direct = jnp.sum(expand * weight, axis=0, keepdims=True) * new_value
    placed = jnp.where(iota((8, channels), 0) == iota((8, channels), 1) // HEAD, direct, 0.0)
    shift = (iota((channels, MISC), 0) % HEAD + (MISC - HEAD) == iota((channels, MISC), 1)).astype(f32)
    direct_rows = dot(placed, shift, precision=HIGHEST)[0:own]
    for g in range(teams):
        at = slice(g * stretch, (g + 1) * stretch)
        piece = running[at].reshape(TEAM, own, channels).astype(bf16)
        send_ref[:, :, g * channels : (g + 1) * channels] = piece
    note = misc[0:stretch]
    for g in range(teams):
        at = slice(g * stretch, (g + 1) * stretch)
        note = jnp.where(lanes[0:stretch] == 2 * heads + g, read_column[at], note)
    note = note.reshape(TEAM, own, MISC)
    note = jnp.where(iota(note.shape, 2) >= MISC - HEAD, direct_rows[None], note).astype(bf16)
    send_ref[:, :, teams * channels :] = note


def inner_kernel(
    tok_ref, wg_ref, fresh_ref, rows_ref, edge_ref, rtap_ref, vw_ref, cum_ref, dt_ref, inside_ref,
    skip_ref, after_ref, base_ref, lift_ref, newgate_ref, reads_ref, before, ext,
):
    del after_ref
    b = pl.program_id(0)
    rank = lax.axis_index("tp")
    heads = cum_ref.shape[0]
    channels = wg_ref.shape[1]
    length = rows_ref.shape[0]

    @pl.when(b == 0)
    def _():
        before[...] = jnp.zeros_like(before)
        lines = fresh_ref[...].astype(f32)
        fresh = jnp.concatenate([lines[i : i + 1] for i in range(lines.shape[0])], axis=1)
        fresh = jnp.broadcast_to(fresh, (8, fresh.shape[1])).astype(bf16)
        gate = dot(fresh, wg_ref[...]).astype(bf16).astype(f32)
        newgate_ref[...] = silu(gate)
        ext[0:HALO] = edge_ref[...]
        ext[HALO:] = rows_ref[:, channels + STATE :].astype(f32)
        taps = rtap_ref[:, pl.ds(pl.multiple_of(rank * STATE, 128), STATE)].astype(f32)
        off = HALO - (CONV - 1)
        summed = taps[0:1] * ext[off : off + length]
        for k in range(1, CONV):
            summed = summed + taps[k : k + 1] * ext[off + k : off + k + length]
        reads_ref[...] = silu(summed).astype(bf16)

    expand = spread(heads, channels)
    skip = jnp.sum(expand * head_column(skip_ref, rank * heads, heads), axis=0, keepdims=True)
    cum = cum_ref[...]
    dt = dt_ref[...]
    values = vw_ref[:, 0:channels]
    writes = vw_ref[:, channels:]
    reads = reads_ref[pl.ds(pl.multiple_of(b * BLOCK, BLOCK), BLOCK)]
    gate = silu(dot(tok_ref[...], wg_ref[...]).astype(bf16).astype(f32))
    scores = dot(reads, writes, ((1,), (1,)))
    causal = iota((BLOCK, BLOCK), 0) >= iota((BLOCK, BLOCK), 1)
    columns = jnp.transpose(jnp.concatenate([cum, cum], axis=0))
    parts = []
    for h in range(heads):
        gap = columns[:, h : h + 1] - cum[h : h + 1]
        mixing = scores * jnp.exp(jnp.where(causal, gap, -jnp.inf)) * dt[h : h + 1]
        parts.append(dot(mixing.astype(bf16), values[:, h * HEAD : (h + 1) * HEAD]))
    inner = jnp.concatenate(parts, axis=1)
    fade = dot(jnp.exp(cum), expand, ((0,), (0,)), HIGHEST)
    carried = fade * dot(reads, inside_ref[0])
    base_ref[...] = (inner + carried + skip * values.astype(f32)) * gate
    far = jnp.exp(cum + before[...])
    lift_ref[...] = dot(far, expand, ((0,), (0,)), HIGHEST) * gate
    before[...] += jnp.broadcast_to(cum[:, BLOCK - 1 :], before.shape)


def fades_of(notes, heads, channels):
    lane = iota((MISC, channels), 0)
    owner = iota((MISC, channels), 1) // HEAD
    pick = jnp.where((lane == owner) | (lane == owner + heads), 1.0, 0.0)
    return dot(jnp.where(iota(notes.shape, 1) < 2 * heads, notes, 0.0), pick, precision=HIGHEST)


def team_kernel(recv_ref, send_ref, local_ref, reach_ref):
    count, own, width = recv_ref.shape
    wide = width - MISC
    teams = send_ref.shape[0]
    channels = wide // teams
    heads = channels // HEAD
    notes = recv_ref[:, 0:1, wide:].astype(f32).reshape(count, MISC)
    fades = fades_of(notes, heads, channels)
    state = jnp.zeros((own, wide), f32)
    reach = jnp.ones((1, channels), f32)
    for k in range(count):
        local_ref[k] = state
        reach_ref[k : k + 1] = reach
        fade = jnp.concatenate([fades[k : k + 1]] * teams, axis=1)
        state = fade * state + recv_ref[k, :, 0:wide].astype(f32)
        reach = reach * fades[k : k + 1]
    total = state.astype(bf16)
    note = recv_ref[count - 1, :, wide:].astype(f32)
    first = (iota((channels, MISC), 0) == iota((channels, MISC), 1) * HEAD).astype(f32)
    high = reach.astype(bf16).astype(f32)
    low = reach - high
    packed = dot(jnp.concatenate([high, low, jnp.zeros((6, channels), f32)], axis=0), first, precision=HIGHEST)
    shifted = (iota((MISC, MISC), 0) + heads == iota((MISC, MISC), 1)).astype(f32)
    moved = dot(packed, shifted, precision=HIGHEST)
    lanes = iota((own, MISC), 1)
    note = jnp.where(lanes < heads, packed[0:1], jnp.where(lanes < 2 * heads, moved[1:2], note)).astype(bf16)
    for t in range(teams):
        send_ref[t, :, 0:wide] = total
        send_ref[t, :, wide:] = note


def prefix_kernel(recv_ref, local_ref, reach_ref, newdecay_ref, after_ref, send_ref, cache_ref, direct_ref):
    del after_ref
    teams, own, width = recv_ref.shape
    wide = width - MISC
    channels = wide // teams
    heads = channels // HEAD
    group = lax.axis_index("sp") // TEAM
    notes = recv_ref[:, 0:1, wide:].astype(f32).reshape(teams, MISC)
    fades = fades_of(notes, heads, channels)
    state = jnp.zeros((own, wide), f32)
    entering = state
    for t in range(teams):
        entering = jnp.where(group == t, state, entering)
        fade = jnp.concatenate([fades[t : t + 1]] * teams, axis=1)
        state = fade * state + recv_ref[t, :, 0:wide].astype(f32)
    for k in range(TEAM):
        reach = jnp.concatenate([reach_ref[k : k + 1]] * teams, axis=1)
        send_ref[k, :, 0:wide] = (local_ref[k] + reach * entering).astype(bf16)
    kept = state.astype(bf16).astype(f32)
    mine = kept[:, 0:channels]
    for g in range(1, teams):
        mine = jnp.where(group == g, kept[:, g * channels : (g + 1) * channels], mine)
    cache_ref[...] = mine.astype(bf16)
    note = recv_ref[teams - 1, :, wide:].astype(f32)
    reading = jnp.zeros((own, channels), f32)
    for g in range(teams):
        column = note[:, 2 * heads + g : 2 * heads + g + 1]
        reading = reading + column * kept[:, g * channels : (g + 1) * channels]
    partial = jnp.sum(reading, axis=0, keepdims=True) * newdecay_ref[...]
    high = partial.astype(bf16).astype(f32)
    low = partial - high
    rows = iota((own, channels), 0)
    share = jnp.where(rows == 0, high, jnp.where(rows == 1, low, 0.0)).astype(bf16)
    send_ref[:, :, wide:] = jnp.broadcast_to(share[None], (TEAM, own, channels))
    unshift = (iota((MISC, channels), 0) == iota((MISC, channels), 1) % HEAD + (MISC - HEAD)).astype(f32)
    laid = dot(note, unshift, precision=HIGHEST)
    direct_ref[...] = jnp.sum(jnp.where(rows == iota(rows.shape, 1) // HEAD, laid, 0.0), axis=0, keepdims=True)


def finish_kernel(recv_ref, base_ref, lift_ref, reads_ref, gain_ref, direct_ref, newgate_ref, out_ref, step_ref):
    rank = lax.axis_index("tp")
    place = lax.axis_index("sp")
    channels = base_ref.shape[1]
    wide = recv_ref.shape[2] - channels
    pieces = wide // channels
    own = recv_ref.shape[1]
    earlier = jnp.concatenate(
        [
            recv_ref[:, :, g * channels : (g + 1) * channels].astype(f32).reshape(TEAM * own, channels)
            for g in range(pieces)
        ],
        axis=0,
    ).astype(bf16)
    gain = gain_ref[:, pl.ds(pl.multiple_of(rank * channels, 128), channels)]
    gated = base_ref[...] + dot(reads_ref[...], earlier) * lift_ref[...]
    scale = lax.rsqrt(jnp.mean(gated * gated, axis=1, keepdims=True) + epsilon)
    out_ref[...] = (gated * scale * gain).astype(bf16)
    partial = jnp.sum(jnp.sum(recv_ref[:, :, wide:].astype(f32), axis=0), axis=0, keepdims=True)
    new = (partial + direct_ref[...]) * newgate_ref[0:1]
    scale = lax.rsqrt(jnp.mean(new * new, axis=1, keepdims=True) + epsilon)
    step = (new * scale * gain).astype(bf16)
    columns = lax.axis_size("sp")
    channel = iota((channels, 128), 0)
    take = (channel // columns == iota((channels, 128), 1)) & (channel % columns == place)
    picked = dot(jnp.broadcast_to(step, (16, channels)), take.astype(bf16))
    step_ref[...] = picked[0:1, 0 : channels // columns].astype(bf16)


def call(kernel, out_shape, grid=None, in_specs=None, out_specs=None, scratch=(), flops=0, name=None):
    return pl.pallas_call(
        kernel,
        out_shape=out_shape,
        grid_spec=pltpu.PrefetchScalarGridSpec(
            num_scalar_prefetch=0,
            grid=grid or (),
            in_specs=in_specs,
            out_specs=out_specs,
            scratch_shapes=scratch,
        ),
        compiler_params=pltpu.CompilerParams(
            vmem_limit_bytes=VMEM_LIMIT,
            dimension_semantics=("arbitrary",) * len(grid or ()),
        ),
        cost_estimate=pl.CostEstimate(flops=flops, transcendentals=0, bytes_accessed=1 << 20),
        name=name,
    )


def shaped(*shape, dtype=f32):
    return jax.ShapeDtypeStruct(shape, dtype)


def near(*shape, dtype=f32):
    return pltpu.VMEM(shape, dtype)


def held(array):
    return pltpu.with_memory_space_constraint(array, pltpu.VMEM)


def stored(array):
    return pltpu.with_memory_space_constraint(array, pltpu.HBM)


def on_device(
    tokens,
    fresh_token_input,
    value_matrix,
    write_matrix,
    read_matrix,
    gate_matrix,
    step_matrix,
    value_filter_taps,
    write_filter_taps,
    read_filter_taps,
    head_log_decay,
    step_offset_bias,
    decay_spike,
    bypass_scale,
    group_norm_scale,
):
    sequence_count = lax.axis_size("sp")
    length, depth = tokens.shape
    channels = value_matrix.shape[1]
    heads = channels // HEAD
    own = STATE // sequence_count
    teams = sequence_count // TEAM
    blocks = length // BLOCK
    width = channels + 2 * STATE
    wide = teams * channels
    vm = pl.BlockSpec(memory_space=pltpu.VMEM)
    far = pl.BlockSpec(memory_space=pltpu.HBM)
    inside_team = [[TEAM * t + i for i in range(TEAM)] for t in range(teams)]
    across_teams = [[TEAM * t + i for t in range(teams)] for i in range(TEAM)]

    halo = lax.ppermute(
        tokens[length - HALO :], "sp", [(i, i + 1) for i in range(sequence_count - 1)]
    )
    fresh = fresh_token_input.reshape(depth // 128, 128)
    spike = decay_spike.T
    rows, weights, step_raw, new_rows, new_step = call(
        project_kernel,
        (
            near(length, width, dtype=bf16),
            near(depth, width, dtype=bf16),
            near(heads, length),
            near(8, width),
            near(heads, 8),
        ),
        in_specs=[far] * 6,
        out_specs=[vm] * 5,
        scratch=[
            pltpu.VMEM((length + 16, depth), bf16),
            pltpu.VMEM((depth // 128, 128), bf16),
            pltpu.VMEM((step_matrix.shape[1], depth), bf16),
            pltpu.SemaphoreType.DMA((SPLIT, 4)),
            pltpu.SemaphoreType.DMA((2,)),
        ],
        flops=2 * length * depth * width,
        name="project",
    )(
        stored(tokens), stored(fresh), stored(value_matrix), stored(write_matrix),
        stored(read_matrix), stored(step_matrix.T),
    )

    decay_row, bias_row, skip_row = head_log_decay[None], step_offset_bias[None], bypass_scale[None]
    vw, edge, cum, dt, inside, new_decay, send = call(
        local_kernel,
        (
            near(length, channels + STATE, dtype=bf16),
            near(HALO, STATE),
            near(heads, length),
            near(heads, length),
            near(blocks, STATE, channels, dtype=bf16),
            near(1, channels),
            near(TEAM, own, wide + MISC, dtype=bf16),
        ),
        in_specs=[vm] * 13,
        out_specs=[vm] * 7,
        scratch=[pltpu.VMEM((length + HALO, channels + STATE), f32)],
        flops=2 * length * STATE * channels,
        name="local",
    )(
        held(rows), held(halo), held(weights), held(step_raw), held(new_rows), held(new_step), spike,
        value_filter_taps, write_filter_taps, read_filter_taps,
        decay_row, bias_row, skip_row,
    )

    received = lax.all_to_all(held(send), "sp", 0, 0, tiled=True, axis_index_groups=inside_team)

    send, local_states, reach = call(
        team_kernel,
        (
            near(teams, own, wide + MISC, dtype=bf16),
            near(TEAM, own, wide),
            near(TEAM, channels),
        ),
        in_specs=[vm],
        out_specs=[vm] * 3,
        name="team",
    )(held(received))

    received = lax.all_to_all(held(send), "sp", 0, 0, tiled=True, axis_index_groups=across_teams)

    base, lift, new_gate, reads = call(
        inner_kernel,
        (
            near(length, channels),
            near(length, channels),
            near(8, channels),
            near(length, STATE, dtype=bf16),
        ),
        grid=(blocks,),
        in_specs=[
            pl.BlockSpec((BLOCK, depth), lambda b: (b, 0)),
            pl.BlockSpec((depth, channels), lambda b: (0, 0)),
            pl.BlockSpec((depth // 128, 128), lambda b: (0, 0)),
            pl.BlockSpec((length, width), lambda b: (0, 0)),
            pl.BlockSpec((HALO, STATE), lambda b: (0, 0)),
            pl.BlockSpec(read_filter_taps.shape, lambda b: (0, 0)),
            pl.BlockSpec((BLOCK, channels + STATE), lambda b: (b, 0)),
            pl.BlockSpec((heads, BLOCK), lambda b: (0, b)),
            pl.BlockSpec((heads, BLOCK), lambda b: (0, b)),
            pl.BlockSpec((1, STATE, channels), lambda b: (b, 0, 0)),
            pl.BlockSpec(skip_row.shape, lambda b: (0, 0)),
            pl.BlockSpec(reach.shape, lambda b: (0, 0)),
        ],
        out_specs=[
            pl.BlockSpec((BLOCK, channels), lambda b: (b, 0)),
            pl.BlockSpec((BLOCK, channels), lambda b: (b, 0)),
            pl.BlockSpec((8, channels), lambda b: (0, 0)),
            pl.BlockSpec((length, STATE), lambda b: (0, 0)),
        ],
        scratch=[pltpu.VMEM((heads, BLOCK), f32), pltpu.VMEM((length + HALO, STATE), f32)],
        flops=2 * length * depth * channels,
        name="inner",
    )(
        stored(tokens), stored(gate_matrix), fresh, held(rows), held(edge), read_filter_taps,
        held(vw), held(cum), held(dt), held(inside), skip_row, held(reach),
    )

    send, cache_rows, direct = call(
        prefix_kernel,
        (
            near(TEAM, own, wide + channels, dtype=bf16),
            shaped(own, channels, dtype=bf16),
            near(1, channels),
        ),
        in_specs=[vm] * 5,
        out_specs=[vm] * 3,
        name="prefix",
    )(held(received), held(local_states), held(reach), held(new_decay), held(new_gate))

    received = lax.all_to_all(held(send), "sp", 0, 0, tiled=True, axis_index_groups=inside_team)

    prompt_out, step_row = call(
        finish_kernel,
        (
            shaped(length, channels, dtype=bf16),
            shaped(1, channels // sequence_count, dtype=bf16),
        ),
        in_specs=[vm] * 7,
        out_specs=[vm] * 2,
        name="finish",
    )(
        held(received), held(base), held(lift), held(reads), group_norm_scale[None],
        held(direct), held(new_gate),
    )
    return (prompt_out, cache_rows, step_row.T)


def solution(mesh):
    placed = (
        P(("grp", "sp"), None),
        P("grp"),
        P(None, "tp"),
        P(None, "tp"),
        P(None, "tp"),
        P(None, "tp"),
        P(),
        P(),
        P(),
        P(),
        P(),
        P(),
        P(("grp", "sp"), "tp"),
        P(),
        P(),
    )
    return jax.shard_map(
        on_device,
        mesh=mesh,
        in_specs=placed,
        out_specs=(P(("grp", "sp"), "tp"), P(("grp", "sp"), "tp"), P(("grp", "tp"), "sp")),
        check_vma=False,
    )
```

```python
import jax
import jax.numpy as jnp
from jax import lax
from jax.experimental import pallas as pl
from jax.experimental.pallas import tpu as pltpu
from jax.sharding import PartitionSpec as P

HEAD = 64
STATE = 128
CONV = 4
BLOCK = 128
TEAM = 4
MISC = 128
HALO = 8

epsilon = 1e-06
f32 = jnp.float32
bf16 = jnp.bfloat16
HIGHEST = lax.Precision.HIGHEST
VMEM_LIMIT = 24 * 1024 * 1024
SPLIT = 8
AHEAD = 8


def dot(a, b, dims=((1,), (0,)), precision=None):
    return lax.dot_general(a, b, (dims, ((), ())), precision=precision, preferred_element_type=f32)


def silu(x):
    half = 0.5 * x
    return half * jnp.tanh(half) + half


def softplus(x):
    return jnp.maximum(x, 0.0) + jnp.log1p(jnp.exp(-jnp.abs(x)))


def iota(shape, dim):
    return lax.broadcasted_iota(jnp.int32, shape, dim)


def spread(heads, channels):
    return (iota((heads, channels), 0) == iota((heads, channels), 1) // HEAD).astype(f32)


def thirds(x):
    high = x.astype(bf16)
    rest = x - high.astype(f32)
    middle = rest.astype(bf16)
    low = (rest - middle.astype(f32)).astype(bf16)
    return jnp.concatenate([high.astype(f32), middle.astype(f32), low.astype(f32)], axis=0).astype(bf16)


def over_channels(x, channels):
    heads = x.shape[0]
    shape = (3 * heads, channels)
    mask = iota(shape, 0) % heads == iota(shape, 1) // HEAD
    return dot(thirds(x), mask.astype(bf16), ((0,), (0,)))


def summed_up(x, upper):
    heads = x.shape[0]
    parts = dot(thirds(x), upper)
    return parts[0:heads] + parts[heads : 2 * heads] + parts[2 * heads :]


def own_rows(table, rank, count):
    picked = table[0:count]
    for other in range(1, table.shape[0] // count):
        picked = jnp.where(rank == other, table[other * count : (other + 1) * count], picked)
    return picked


def head_column(ref, first, count):
    row = ref[...]
    shape = (count, row.shape[1])
    return jnp.sum(jnp.where(iota(shape, 1) == iota(shape, 0) + first, row, 0.0), axis=1, keepdims=True)


def project_kernel(
    tok_hbm, fresh_hbm, wv_hbm, ww_hbm, wr_hbm, ws_hbm,
    rows_ref, weights, step_ref, fresh_ref, newstep_ref, tok, lines, steps, sems, small,
):
    depth = tok_hbm.shape[1]
    channels = wv_hbm.shape[1]
    state = ww_hbm.shape[1]
    chunk = depth // SPLIT
    first = [
        pltpu.make_async_copy(fresh_hbm, lines, small.at[0]),
        pltpu.make_async_copy(ws_hbm, steps, small.at[1]),
    ]
    for copy in first:
        copy.start()
    copies = []
    for k in range(SPLIT):
        at = pl.ds(k * chunk, chunk)
        moves = [
            (tok_hbm.at[:, at], tok.at[:, at]),
            (wv_hbm.at[at], weights.at[at, pl.ds(0, channels)]),
            (ww_hbm.at[at], weights.at[at, pl.ds(channels, state)]),
            (wr_hbm.at[at], weights.at[at, pl.ds(channels + state, state)]),
        ]
        copies.append(
            [pltpu.make_async_copy(a, b, sems.at[k, i]) for i, (a, b) in enumerate(moves)]
        )
    for k in range(min(AHEAD, SPLIT)):
        for copy in copies[k]:
            copy.start()
    rank = lax.axis_index("tp")
    heads = step_ref.shape[0]
    for copy in first:
        copy.wait()
    rows = lines[...].astype(f32)
    fresh = jnp.concatenate([rows[i : i + 1] for i in range(depth // 128)], axis=1)
    fresh_ref[...] = jnp.broadcast_to(fresh, fresh_ref.shape).astype(bf16)
    newstep = jnp.sum(own_rows(steps[...].astype(f32), rank, heads) * fresh, axis=1, keepdims=True)
    newstep_ref[...] = jnp.broadcast_to(newstep, newstep_ref.shape)
    acc = accs = None
    for k in range(SPLIT):
        at = slice(k * chunk, (k + 1) * chunk)
        for copy in copies[k]:
            copy.wait()
        if k + AHEAD < SPLIT:
            for copy in copies[k + AHEAD]:
                copy.start()
        part = dot(tok[:, at], weights[at])
        parts = dot(steps[:, at], tok[:, at], ((1,), (1,)))
        acc = part if k == 0 else acc + part
        accs = parts if k == 0 else accs + parts
    rows_ref[...] = acc.astype(bf16)
    step_ref[...] = own_rows(accs, rank, heads)


def local_kernel(
    rows_ref, halo_ref, weights, step_ref, fresh_ref, newstep_ref, spike_ref,
    vtap_ref, wtap_ref, rtap_ref, decay_ref, bias_ref, skip_ref,
    vw_ref, edge_ref, cum_ref, dt_ref, inside_ref, newdecay_ref, send_ref, ext,
):
    rank = lax.axis_index("tp")
    length = rows_ref.shape[0]
    heads = step_ref.shape[0]
    channels = rows_ref.shape[1] - 2 * STATE
    first = rank * heads
    few = dot(jnp.concatenate([halo_ref[...], fresh_ref[...]], axis=0), weights[...])
    few = few.astype(bf16).astype(f32)
    before = few[0:HALO]
    used = channels + STATE
    edge_ref[...] = before[:, used:]
    ext[0:HALO] = before[:, 0:used]
    ext[HALO:] = rows_ref[:, 0:used].astype(f32)
    taps = jnp.concatenate(
        [
            vtap_ref[:, pl.ds(pl.multiple_of(rank * channels, 128), channels)].astype(f32),
            wtap_ref[:, pl.ds(pl.multiple_of(rank * STATE, 128), STATE)].astype(f32),
            rtap_ref[:, pl.ds(pl.multiple_of(rank * STATE, 128), STATE)].astype(f32),
        ],
        axis=1,
    )
    off = HALO - (CONV - 1)
    summed = taps[0:1, 0:used] * ext[off : off + length]
    for k in range(1, CONV):
        summed = summed + taps[k : k + 1, 0:used] * ext[off + k : off + k + length]
    vwr = silu(summed).astype(bf16)
    vw_ref[...] = vwr
    newest = taps[CONV - 1 : CONV] * few[HALO : HALO + 1]
    ending = rows_ref[length - 16 :].astype(f32)
    for k in range(CONV - 1):
        row = 16 - (CONV - 1) + k
        newest = newest + taps[k : k + 1] * ending[row : row + 1]
    newest = silu(newest).astype(bf16).astype(f32)
    new_value = newest[:, 0:channels]
    new_write = newest[:, channels : channels + STATE]
    new_read = newest[:, channels + STATE :]
    bias = head_column(bias_ref, first, heads)
    rate = jnp.exp(head_column(decay_ref, first, heads))
    upper = (iota((BLOCK, BLOCK), 0) <= iota((BLOCK, BLOCK), 1)).astype(bf16)
    expand = spread(heads, channels)
    running = jnp.zeros((STATE, channels), f32)
    total = jnp.zeros((heads, 128), f32)
    for b in range(length // BLOCK):
        at = slice(b * BLOCK, (b + 1) * BLOCK)
        dt = softplus(step_ref[:, at] + bias)
        log_decay = spike_ref[:, at] - dt * rate
        cum = summed_up(log_decay, upper)
        dt_ref[:, at] = dt
        cum_ref[:, at] = cum
        end = jnp.broadcast_to(cum[:, BLOCK - 1 :], (heads, BLOCK))
        factor = over_channels(jnp.exp(end - cum) * dt, channels)
        scaled = (factor * vwr[at, 0:channels].astype(f32)).astype(bf16)
        states = dot(vwr[at, channels : channels + STATE], scaled, ((0,), (0,)))
        fade = jnp.sum(expand * jnp.exp(end[:, 0:1]), axis=0, keepdims=True)
        inside_ref[b] = running.astype(bf16)
        running = fade * running + states
        total = total + end
    fade = jnp.exp(total)
    high = fade.astype(bf16).astype(f32)
    low = fade - high
    shape = (STATE, MISC)
    lanes = iota(shape, 1)
    rows = iota(shape, 0)
    misc = jnp.zeros(shape, f32)
    for h in range(heads):
        misc = jnp.where(lanes == h, high[h : h + 1, 0:1], misc)
        misc = jnp.where(lanes == heads + h, low[h : h + 1, 0:1], misc)
    own = STATE // lax.axis_size("sp")
    stretch = TEAM * own
    teams = STATE // stretch
    diagonal = jnp.where(rows == lanes, jnp.broadcast_to(new_read, shape), 0.0)
    read_column = jnp.sum(diagonal, axis=1, keepdims=True)
    new_dt = softplus(newstep_ref[...][:, 0:1] + bias)
    newdecay_ref[...] = jnp.sum(expand * jnp.exp(-new_dt * rate), axis=0, keepdims=True)
    skip = head_column(skip_ref, first, heads)
    weight = new_dt * jnp.sum(new_read * new_write, axis=1, keepdims=True) + skip
    direct = jnp.sum(expand * weight, axis=0, keepdims=True) * new_value
    placed = jnp.where(iota((8, channels), 0) == iota((8, channels), 1) // HEAD, direct, 0.0)
    shift = (iota((channels, MISC), 0) % HEAD + (MISC - HEAD) == iota((channels, MISC), 1)).astype(f32)
    direct_rows = dot(placed, shift, precision=HIGHEST)[0:own]
    for g in range(teams):
        at = slice(g * stretch, (g + 1) * stretch)
        piece = running[at].reshape(TEAM, own, channels).astype(bf16)
        send_ref[:, :, g * channels : (g + 1) * channels] = piece
    note = misc[0:stretch]
    for g in range(teams):
        at = slice(g * stretch, (g + 1) * stretch)
        note = jnp.where(lanes[0:stretch] == 2 * heads + g, read_column[at], note)
    note = note.reshape(TEAM, own, MISC)
    note = jnp.where(iota(note.shape, 2) >= MISC - HEAD, direct_rows[None], note).astype(bf16)
    send_ref[:, :, teams * channels :] = note


def inner_kernel(
    tok_ref, wg_ref, fresh_ref, rows_ref, edge_ref, rtap_ref, vw_ref, cum_ref, dt_ref, inside_ref,
    skip_ref, after_ref, base_ref, lift_ref, newgate_ref, reads_ref, before, ext,
):
    del after_ref
    b = pl.program_id(0)
    rank = lax.axis_index("tp")
    heads = cum_ref.shape[0]
    channels = wg_ref.shape[1]
    length = rows_ref.shape[0]

    @pl.when(b == 0)
    def _():
        before[...] = jnp.zeros_like(before)
        gate = dot(fresh_ref[...], wg_ref[...]).astype(bf16).astype(f32)
        newgate_ref[...] = silu(gate)
        ext[0:HALO] = edge_ref[...]
        ext[HALO:] = rows_ref[:, channels + STATE :].astype(f32)
        taps = rtap_ref[:, pl.ds(pl.multiple_of(rank * STATE, 128), STATE)].astype(f32)
        off = HALO - (CONV - 1)
        summed = taps[0:1] * ext[off : off + length]
        for k in range(1, CONV):
            summed = summed + taps[k : k + 1] * ext[off + k : off + k + length]
        reads_ref[...] = silu(summed).astype(bf16)

    expand = spread(heads, channels)
    skip = jnp.sum(expand * head_column(skip_ref, rank * heads, heads), axis=0, keepdims=True)
    cum = cum_ref[...]
    dt = dt_ref[...]
    values = vw_ref[:, 0:channels]
    writes = vw_ref[:, channels:]
    reads = reads_ref[pl.ds(pl.multiple_of(b * BLOCK, BLOCK), BLOCK)]
    gate = silu(dot(tok_ref[...], wg_ref[...]).astype(bf16).astype(f32))
    scores = dot(reads, writes, ((1,), (1,)))
    causal = iota((BLOCK, BLOCK), 0) >= iota((BLOCK, BLOCK), 1)
    columns = jnp.transpose(jnp.concatenate([cum, cum], axis=0))
    parts = []
    for h in range(heads):
        gap = columns[:, h : h + 1] - cum[h : h + 1]
        mixing = scores * jnp.exp(jnp.where(causal, gap, -jnp.inf)) * dt[h : h + 1]
        parts.append(dot(mixing.astype(bf16), values[:, h * HEAD : (h + 1) * HEAD]))
    inner = jnp.concatenate(parts, axis=1)
    fade = over_channels(jnp.exp(cum), channels)
    carried = fade * dot(reads, inside_ref[0])
    base_ref[...] = (inner + carried + skip * values.astype(f32)) * gate
    far = jnp.exp(cum + before[...])
    lift_ref[...] = over_channels(far, channels) * gate
    before[...] += jnp.broadcast_to(cum[:, BLOCK - 1 :], before.shape)


def fades_of(notes, heads, channels):
    lane = iota((MISC, channels), 0)
    owner = iota((MISC, channels), 1) // HEAD
    pick = jnp.where((lane == owner) | (lane == owner + heads), 1.0, 0.0)
    return dot(jnp.where(iota(notes.shape, 1) < 2 * heads, notes, 0.0), pick, precision=HIGHEST)


def team_kernel(recv_ref, send_ref, local_ref, reach_ref):
    count, own, width = recv_ref.shape
    wide = width - MISC
    teams = send_ref.shape[0]
    channels = wide // teams
    heads = channels // HEAD
    notes = recv_ref[:, 0:1, wide:].astype(f32).reshape(count, MISC)
    fades = fades_of(notes, heads, channels)
    state = jnp.zeros((own, wide), f32)
    reach = jnp.ones((1, channels), f32)
    for k in range(count):
        local_ref[k] = state
        reach_ref[k : k + 1] = reach
        fade = jnp.concatenate([fades[k : k + 1]] * teams, axis=1)
        state = fade * state + recv_ref[k, :, 0:wide].astype(f32)
        reach = reach * fades[k : k + 1]
    total = state.astype(bf16)
    note = recv_ref[count - 1, :, wide:].astype(f32)
    first = (iota((channels, MISC), 0) == iota((channels, MISC), 1) * HEAD).astype(f32)
    high = reach.astype(bf16).astype(f32)
    low = reach - high
    packed = dot(jnp.concatenate([high, low, jnp.zeros((6, channels), f32)], axis=0), first, precision=HIGHEST)
    shifted = (iota((MISC, MISC), 0) + heads == iota((MISC, MISC), 1)).astype(f32)
    moved = dot(packed, shifted, precision=HIGHEST)
    lanes = iota((own, MISC), 1)
    note = jnp.where(lanes < heads, packed[0:1], jnp.where(lanes < 2 * heads, moved[1:2], note)).astype(bf16)
    for t in range(teams):
        send_ref[t, :, 0:wide] = total
        send_ref[t, :, wide:] = note


def prefix_kernel(recv_ref, local_ref, reach_ref, newdecay_ref, after_ref, send_ref, cache_ref, direct_ref):
    del after_ref
    teams, own, width = recv_ref.shape
    wide = width - MISC
    channels = wide // teams
    heads = channels // HEAD
    group = lax.axis_index("sp") // TEAM
    notes = recv_ref[:, 0:1, wide:].astype(f32).reshape(teams, MISC)
    fades = fades_of(notes, heads, channels)
    state = jnp.zeros((own, wide), f32)
    entering = state
    for t in range(teams):
        entering = jnp.where(group == t, state, entering)
        fade = jnp.concatenate([fades[t : t + 1]] * teams, axis=1)
        state = fade * state + recv_ref[t, :, 0:wide].astype(f32)
    for k in range(TEAM):
        reach = jnp.concatenate([reach_ref[k : k + 1]] * teams, axis=1)
        send_ref[k, :, 0:wide] = (local_ref[k] + reach * entering).astype(bf16)
    kept = state.astype(bf16).astype(f32)
    mine = kept[:, 0:channels]
    for g in range(1, teams):
        mine = jnp.where(group == g, kept[:, g * channels : (g + 1) * channels], mine)
    cache_ref[...] = mine.astype(bf16)
    note = recv_ref[teams - 1, :, wide:].astype(f32)
    reading = jnp.zeros((own, channels), f32)
    for g in range(teams):
        column = note[:, 2 * heads + g : 2 * heads + g + 1]
        reading = reading + column * kept[:, g * channels : (g + 1) * channels]
    partial = jnp.sum(reading, axis=0, keepdims=True) * newdecay_ref[...]
    high = partial.astype(bf16).astype(f32)
    low = partial - high
    rows = iota((own, channels), 0)
    share = jnp.where(rows == 0, high, jnp.where(rows == 1, low, 0.0)).astype(bf16)
    send_ref[:, :, wide:] = jnp.broadcast_to(share[None], (TEAM, own, channels))
    unshift = (iota((MISC, channels), 0) == iota((MISC, channels), 1) % HEAD + (MISC - HEAD)).astype(f32)
    laid = dot(note, unshift, precision=HIGHEST)
    direct_ref[...] = jnp.sum(jnp.where(rows == iota(rows.shape, 1) // HEAD, laid, 0.0), axis=0, keepdims=True)


def finish_kernel(recv_ref, base_ref, lift_ref, reads_ref, gain_ref, direct_ref, newgate_ref, out_ref, step_ref):
    rank = lax.axis_index("tp")
    place = lax.axis_index("sp")
    channels = base_ref.shape[1]
    wide = recv_ref.shape[2] - channels
    pieces = wide // channels
    own = recv_ref.shape[1]
    earlier = jnp.concatenate(
        [
            recv_ref[:, :, g * channels : (g + 1) * channels].astype(f32).reshape(TEAM * own, channels)
            for g in range(pieces)
        ],
        axis=0,
    ).astype(bf16)
    gain = gain_ref[:, pl.ds(pl.multiple_of(rank * channels, 128), channels)]
    gated = base_ref[...] + dot(reads_ref[...], earlier) * lift_ref[...]
    scale = lax.rsqrt(jnp.mean(gated * gated, axis=1, keepdims=True) + epsilon)
    out_ref[...] = (gated * scale * gain).astype(bf16)
    partial = jnp.sum(jnp.sum(recv_ref[:, :, wide:].astype(f32), axis=0), axis=0, keepdims=True)
    new = (partial + direct_ref[...]) * newgate_ref[0:1]
    scale = lax.rsqrt(jnp.mean(new * new, axis=1, keepdims=True) + epsilon)
    step = (new * scale * gain).astype(bf16)
    columns = lax.axis_size("sp")
    channel = iota((channels, 128), 0)
    take = (channel // columns == iota((channels, 128), 1)) & (channel % columns == place)
    picked = dot(jnp.broadcast_to(step, (16, channels)), take.astype(bf16))
    step_ref[...] = picked[0:1, 0 : channels // columns].astype(bf16)


def call(kernel, out_shape, grid=None, in_specs=None, out_specs=None, scratch=(), flops=0, name=None):
    return pl.pallas_call(
        kernel,
        out_shape=out_shape,
        grid_spec=pltpu.PrefetchScalarGridSpec(
            num_scalar_prefetch=0,
            grid=grid or (),
            in_specs=in_specs,
            out_specs=out_specs,
            scratch_shapes=scratch,
        ),
        compiler_params=pltpu.CompilerParams(
            vmem_limit_bytes=VMEM_LIMIT,
            dimension_semantics=("arbitrary",) * len(grid or ()),
        ),
        cost_estimate=pl.CostEstimate(flops=flops, transcendentals=0, bytes_accessed=1 << 20),
        name=name,
    )


def shaped(*shape, dtype=f32):
    return jax.ShapeDtypeStruct(shape, dtype)


def near(*shape, dtype=f32):
    return pltpu.VMEM(shape, dtype)


def held(array):
    return pltpu.with_memory_space_constraint(array, pltpu.VMEM)


def stored(array):
    return pltpu.with_memory_space_constraint(array, pltpu.HBM)


def on_device(
    tokens,
    fresh_token_input,
    value_matrix,
    write_matrix,
    read_matrix,
    gate_matrix,
    step_matrix,
    value_filter_taps,
    write_filter_taps,
    read_filter_taps,
    head_log_decay,
    step_offset_bias,
    decay_spike,
    bypass_scale,
    group_norm_scale,
):
    sequence_count = lax.axis_size("sp")
    length, depth = tokens.shape
    channels = value_matrix.shape[1]
    heads = channels // HEAD
    own = STATE // sequence_count
    teams = sequence_count // TEAM
    blocks = length // BLOCK
    width = channels + 2 * STATE
    wide = teams * channels
    vm = pl.BlockSpec(memory_space=pltpu.VMEM)
    far = pl.BlockSpec(memory_space=pltpu.HBM)
    inside_team = [[TEAM * t + i for i in range(TEAM)] for t in range(teams)]
    across_teams = [[TEAM * t + i for t in range(teams)] for i in range(TEAM)]

    halo = lax.ppermute(
        tokens[length - HALO :], "sp", [(i, i + 1) for i in range(sequence_count - 1)]
    )
    fresh = fresh_token_input.reshape(depth // 128, 128)
    spike = decay_spike.T
    rows, weights, step_raw, fresh_rows, new_step = call(
        project_kernel,
        (
            near(length, width, dtype=bf16),
            near(depth, width, dtype=bf16),
            near(heads, length),
            near(8, depth, dtype=bf16),
            near(heads, 8),
        ),
        in_specs=[far] * 6,
        out_specs=[vm] * 5,
        scratch=[
            pltpu.VMEM((length, depth), bf16),
            pltpu.VMEM((depth // 128, 128), bf16),
            pltpu.VMEM((step_matrix.shape[1], depth), bf16),
            pltpu.SemaphoreType.DMA((SPLIT, 4)),
            pltpu.SemaphoreType.DMA((2,)),
        ],
        flops=2 * length * depth * width,
        name="project",
    )(
        stored(tokens), stored(fresh), stored(value_matrix), stored(write_matrix),
        stored(read_matrix), stored(step_matrix.T),
    )

    decay_row, bias_row, skip_row = head_log_decay[None], step_offset_bias[None], bypass_scale[None]
    vw, edge, cum, dt, inside, new_decay, send = call(
        local_kernel,
        (
            near(length, channels + STATE, dtype=bf16),
            near(HALO, STATE),
            near(heads, length),
            near(heads, length),
            near(blocks, STATE, channels, dtype=bf16),
            near(1, channels),
            near(TEAM, own, wide + MISC, dtype=bf16),
        ),
        in_specs=[vm] * 13,
        out_specs=[vm] * 7,
        scratch=[pltpu.VMEM((length + HALO, channels + STATE), f32)],
        flops=2 * length * STATE * channels,
        name="local",
    )(
        held(rows), held(halo), held(weights), held(step_raw), held(fresh_rows), held(new_step), spike,
        value_filter_taps, write_filter_taps, read_filter_taps,
        decay_row, bias_row, skip_row,
    )

    received = lax.all_to_all(held(send), "sp", 0, 0, tiled=True, axis_index_groups=inside_team)

    send, local_states, reach = call(
        team_kernel,
        (
            near(teams, own, wide + MISC, dtype=bf16),
            near(TEAM, own, wide),
            near(TEAM, channels),
        ),
        in_specs=[vm],
        out_specs=[vm] * 3,
        name="team",
    )(held(received))

    received = lax.all_to_all(held(send), "sp", 0, 0, tiled=True, axis_index_groups=across_teams)

    base, lift, new_gate, reads = call(
        inner_kernel,
        (
            near(length, channels),
            near(length, channels),
            near(8, channels),
            near(length, STATE, dtype=bf16),
        ),
        grid=(blocks,),
        in_specs=[
            pl.BlockSpec((BLOCK, depth), lambda b: (b, 0)),
            pl.BlockSpec((depth, channels), lambda b: (0, 0)),
            pl.BlockSpec(fresh_rows.shape, lambda b: (0, 0)),
            pl.BlockSpec((length, width), lambda b: (0, 0)),
            pl.BlockSpec((HALO, STATE), lambda b: (0, 0)),
            pl.BlockSpec(read_filter_taps.shape, lambda b: (0, 0)),
            pl.BlockSpec((BLOCK, channels + STATE), lambda b: (b, 0)),
            pl.BlockSpec((heads, BLOCK), lambda b: (0, b)),
            pl.BlockSpec((heads, BLOCK), lambda b: (0, b)),
            pl.BlockSpec((1, STATE, channels), lambda b: (b, 0, 0)),
            pl.BlockSpec(skip_row.shape, lambda b: (0, 0)),
            pl.BlockSpec(reach.shape, lambda b: (0, 0)),
        ],
        out_specs=[
            pl.BlockSpec((BLOCK, channels), lambda b: (b, 0)),
            pl.BlockSpec((BLOCK, channels), lambda b: (b, 0)),
            pl.BlockSpec((8, channels), lambda b: (0, 0)),
            pl.BlockSpec((length, STATE), lambda b: (0, 0)),
        ],
        scratch=[pltpu.VMEM((heads, BLOCK), f32), pltpu.VMEM((length + HALO, STATE), f32)],
        flops=2 * length * depth * channels,
        name="inner",
    )(
        stored(tokens), stored(gate_matrix), held(fresh_rows), held(rows), held(edge), read_filter_taps,
        held(vw), held(cum), held(dt), held(inside), skip_row, held(reach),
    )

    send, cache_rows, direct = call(
        prefix_kernel,
        (
            near(TEAM, own, wide + channels, dtype=bf16),
            shaped(own, channels, dtype=bf16),
            near(1, channels),
        ),
        in_specs=[vm] * 5,
        out_specs=[vm] * 3,
        name="prefix",
    )(held(received), held(local_states), held(reach), held(new_decay), held(new_gate))

    received = lax.all_to_all(held(send), "sp", 0, 0, tiled=True, axis_index_groups=inside_team)

    prompt_out, step_row = call(
        finish_kernel,
        (
            shaped(length, channels, dtype=bf16),
            shaped(1, channels // sequence_count, dtype=bf16),
        ),
        in_specs=[vm] * 7,
        out_specs=[vm] * 2,
        name="finish",
    )(
        held(received), held(base), held(lift), held(reads), group_norm_scale[None],
        held(direct), held(new_gate),
    )
    return (prompt_out, cache_rows, step_row.T)


def solution(mesh):
    placed = (
        P(("grp", "sp"), None),
        P("grp"),
        P(None, "tp"),
        P(None, "tp"),
        P(None, "tp"),
        P(None, "tp"),
        P(),
        P(),
        P(),
        P(),
        P(),
        P(),
        P(("grp", "sp"), "tp"),
        P(),
        P(),
    )
    return jax.shard_map(
        on_device,
        mesh=mesh,
        in_specs=placed,
        out_specs=(P(("grp", "sp"), "tp"), P(("grp", "sp"), "tp"), P(("grp", "tp"), "sp")),
        check_vma=False,
    )
```

```python
import jax
import jax.numpy as jnp
from jax import lax
from jax.experimental import pallas as pl
from jax.experimental.pallas import tpu as pltpu
from jax.sharding import PartitionSpec as P

HEAD = 64
STATE = 128
CONV = 4
BLOCK = 128
TEAM = 4
MISC = 128
HALO = 8

epsilon = 1e-06
f32 = jnp.float32
bf16 = jnp.bfloat16
HIGHEST = lax.Precision.HIGHEST
VMEM_LIMIT = 24 * 1024 * 1024
SPLIT = 8


def dot(a, b, dims=((1,), (0,)), precision=None):
    return lax.dot_general(a, b, (dims, ((), ())), precision=precision, preferred_element_type=f32)


def silu(x):
    half = 0.5 * x
    return half * jnp.tanh(half) + half


def softplus(x):
    return jnp.maximum(x, 0.0) + jnp.log1p(jnp.exp(-jnp.abs(x)))


def iota(shape, dim):
    return lax.broadcasted_iota(jnp.int32, shape, dim)


def spread(heads, channels):
    return (iota((heads, channels), 0) == iota((heads, channels), 1) // HEAD).astype(f32)


def thirds(x):
    high = x.astype(bf16)
    rest = x - high.astype(f32)
    middle = rest.astype(bf16)
    low = (rest - middle.astype(f32)).astype(bf16)
    return jnp.concatenate([high.astype(f32), middle.astype(f32), low.astype(f32)], axis=0).astype(bf16)


def over_channels(x, channels):
    heads = x.shape[0]
    shape = (3 * heads, channels)
    mask = iota(shape, 0) % heads == iota(shape, 1) // HEAD
    return dot(thirds(x), mask.astype(bf16), ((0,), (0,)))


def summed_up(x, upper):
    heads = x.shape[0]
    parts = dot(thirds(x), upper)
    return parts[0:heads] + parts[heads : 2 * heads] + parts[2 * heads :]


def own_rows(table, rank, count):
    picked = table[0:count]
    for other in range(1, table.shape[0] // count):
        picked = jnp.where(rank == other, table[other * count : (other + 1) * count], picked)
    return picked


def head_column(ref, first, count):
    row = ref[...]
    shape = (count, row.shape[1])
    return jnp.sum(jnp.where(iota(shape, 1) == iota(shape, 0) + first, row, 0.0), axis=1, keepdims=True)


def project_kernel(
    tok_hbm, fresh_hbm, wv_hbm, ww_hbm, wr_hbm, ws_hbm,
    rows_ref, weights, step_ref, fresh_ref, newstep_ref, tok, lines, steps, sems, small,
):
    depth = tok_hbm.shape[1]
    channels = wv_hbm.shape[1]
    state = ww_hbm.shape[1]
    chunk = depth // SPLIT
    get_fresh = pltpu.make_async_copy(fresh_hbm, lines, small.at[0])
    get_steps = pltpu.make_async_copy(ws_hbm, steps, small.at[1])
    get_steps.start()
    copies = []
    for k in range(SPLIT):
        at = pl.ds(k * chunk, chunk)
        moves = [
            (tok_hbm.at[:, at], tok.at[:, at]),
            (wv_hbm.at[at], weights.at[at, pl.ds(0, channels)]),
            (ww_hbm.at[at], weights.at[at, pl.ds(channels, state)]),
            (wr_hbm.at[at], weights.at[at, pl.ds(channels + state, state)]),
        ]
        copies.append(
            [pltpu.make_async_copy(a, b, sems.at[k, i]) for i, (a, b) in enumerate(moves)]
        )
    for k in range(SPLIT):
        for copy in copies[k]:
            copy.start()
    get_fresh.start()
    rank = lax.axis_index("tp")
    heads = step_ref.shape[0]
    acc = accs = None
    get_steps.wait()
    for k in range(SPLIT):
        at = slice(k * chunk, (k + 1) * chunk)
        for copy in copies[k]:
            copy.wait()
        part = dot(tok[:, at], weights[at])
        parts = dot(steps[:, at], tok[:, at], ((1,), (1,)))
        acc = part if k == 0 else acc + part
        accs = parts if k == 0 else accs + parts
        if k == SPLIT - 1:
            get_fresh.wait()
            rows = lines[...].astype(f32)
            fresh = jnp.concatenate([rows[i : i + 1] for i in range(depth // 128)], axis=1)
            fresh_ref[...] = jnp.broadcast_to(fresh, fresh_ref.shape).astype(bf16)
            table = own_rows(steps[...].astype(f32), rank, heads)
            newstep = jnp.sum(table * fresh, axis=1, keepdims=True)
            newstep_ref[...] = jnp.broadcast_to(newstep, newstep_ref.shape)
    rows_ref[...] = acc.astype(bf16)
    step_ref[...] = own_rows(accs, rank, heads)


def local_kernel(
    rows_ref, halo_ref, weights, step_ref, fresh_ref, newstep_ref, spike_ref,
    vtap_ref, wtap_ref, rtap_ref, decay_ref, bias_ref, skip_ref,
    vw_ref, edge_ref, cum_ref, dt_ref, inside_ref, newdecay_ref, send_ref, ext,
):
    rank = lax.axis_index("tp")
    length = rows_ref.shape[0]
    heads = step_ref.shape[0]
    channels = rows_ref.shape[1] - 2 * STATE
    first = rank * heads
    few = dot(jnp.concatenate([halo_ref[...], fresh_ref[...]], axis=0), weights[...])
    few = few.astype(bf16).astype(f32)
    before = few[0:HALO]
    used = channels + STATE
    edge_ref[...] = before[:, used:]
    ext[0:HALO] = before[:, 0:used]
    ext[HALO:] = rows_ref[:, 0:used].astype(f32)
    taps = jnp.concatenate(
        [
            vtap_ref[:, pl.ds(pl.multiple_of(rank * channels, 128), channels)].astype(f32),
            wtap_ref[:, pl.ds(pl.multiple_of(rank * STATE, 128), STATE)].astype(f32),
            rtap_ref[:, pl.ds(pl.multiple_of(rank * STATE, 128), STATE)].astype(f32),
        ],
        axis=1,
    )
    off = HALO - (CONV - 1)
    summed = taps[0:1, 0:used] * ext[off : off + length]
    for k in range(1, CONV):
        summed = summed + taps[k : k + 1, 0:used] * ext[off + k : off + k + length]
    vwr = silu(summed).astype(bf16)
    vw_ref[...] = vwr
    newest = taps[CONV - 1 : CONV] * few[HALO : HALO + 1]
    ending = rows_ref[length - 16 :].astype(f32)
    for k in range(CONV - 1):
        row = 16 - (CONV - 1) + k
        newest = newest + taps[k : k + 1] * ending[row : row + 1]
    newest = silu(newest).astype(bf16).astype(f32)
    new_value = newest[:, 0:channels]
    new_write = newest[:, channels : channels + STATE]
    new_read = newest[:, channels + STATE :]
    bias = head_column(bias_ref, first, heads)
    rate = jnp.exp(head_column(decay_ref, first, heads))
    upper = (iota((BLOCK, BLOCK), 0) <= iota((BLOCK, BLOCK), 1)).astype(bf16)
    expand = spread(heads, channels)
    running = jnp.zeros((STATE, channels), f32)
    total = jnp.zeros((heads, 128), f32)
    for b in range(length // BLOCK):
        at = slice(b * BLOCK, (b + 1) * BLOCK)
        dt = softplus(step_ref[:, at] + bias)
        log_decay = spike_ref[:, at] - dt * rate
        cum = summed_up(log_decay, upper)
        dt_ref[:, at] = dt
        cum_ref[:, at] = cum
        end = jnp.broadcast_to(cum[:, BLOCK - 1 :], (heads, BLOCK))
        factor = over_channels(jnp.exp(end - cum) * dt, channels)
        scaled = (factor * vwr[at, 0:channels].astype(f32)).astype(bf16)
        states = dot(vwr[at, channels : channels + STATE], scaled, ((0,), (0,)))
        fade = jnp.sum(expand * jnp.exp(end[:, 0:1]), axis=0, keepdims=True)
        inside_ref[b] = running.astype(bf16)
        running = fade * running + states
        total = total + end
    fade = jnp.exp(total)
    high = fade.astype(bf16).astype(f32)
    low = fade - high
    shape = (STATE, MISC)
    lanes = iota(shape, 1)
    rows = iota(shape, 0)
    misc = jnp.zeros(shape, f32)
    for h in range(heads):
        misc = jnp.where(lanes == h, high[h : h + 1, 0:1], misc)
        misc = jnp.where(lanes == heads + h, low[h : h + 1, 0:1], misc)
    own = STATE // lax.axis_size("sp")
    stretch = TEAM * own
    teams = STATE // stretch
    diagonal = jnp.where(rows == lanes, jnp.broadcast_to(new_read, shape), 0.0)
    read_column = jnp.sum(diagonal, axis=1, keepdims=True)
    new_dt = softplus(newstep_ref[...][:, 0:1] + bias)
    newdecay_ref[...] = jnp.sum(expand * jnp.exp(-new_dt * rate), axis=0, keepdims=True)
    skip = head_column(skip_ref, first, heads)
    weight = new_dt * jnp.sum(new_read * new_write, axis=1, keepdims=True) + skip
    direct = jnp.sum(expand * weight, axis=0, keepdims=True) * new_value
    placed = jnp.where(iota((8, channels), 0) == iota((8, channels), 1) // HEAD, direct, 0.0)
    shift = (iota((channels, MISC), 0) % HEAD + (MISC - HEAD) == iota((channels, MISC), 1)).astype(f32)
    direct_rows = dot(placed, shift, precision=HIGHEST)[0:own]
    for g in range(teams):
        at = slice(g * stretch, (g + 1) * stretch)
        piece = running[at].reshape(TEAM, own, channels).astype(bf16)
        send_ref[:, :, g * channels : (g + 1) * channels] = piece
    note = misc[0:stretch]
    for g in range(teams):
        at = slice(g * stretch, (g + 1) * stretch)
        note = jnp.where(lanes[0:stretch] == 2 * heads + g, read_column[at], note)
    note = note.reshape(TEAM, own, MISC)
    note = jnp.where(iota(note.shape, 2) >= MISC - HEAD, direct_rows[None], note).astype(bf16)
    send_ref[:, :, teams * channels :] = note


def inner_kernel(
    tok_ref, wg_ref, fresh_ref, rows_ref, edge_ref, rtap_ref, vw_ref, cum_ref, dt_ref, inside_ref,
    skip_ref, after_ref, base_ref, lift_ref, newgate_ref, reads_ref, before, ext,
):
    del after_ref
    b = pl.program_id(0)
    rank = lax.axis_index("tp")
    heads = cum_ref.shape[0]
    channels = wg_ref.shape[1]
    length = rows_ref.shape[0]

    @pl.when(b == 0)
    def _():
        before[...] = jnp.zeros_like(before)
        gate = dot(fresh_ref[...], wg_ref[...]).astype(bf16).astype(f32)
        newgate_ref[...] = silu(gate)
        ext[0:HALO] = edge_ref[...]
        ext[HALO:] = rows_ref[:, channels + STATE :].astype(f32)
        taps = rtap_ref[:, pl.ds(pl.multiple_of(rank * STATE, 128), STATE)].astype(f32)
        off = HALO - (CONV - 1)
        summed = taps[0:1] * ext[off : off + length]
        for k in range(1, CONV):
            summed = summed + taps[k : k + 1] * ext[off + k : off + k + length]
        reads_ref[...] = silu(summed).astype(bf16)

    expand = spread(heads, channels)
    skip = jnp.sum(expand * head_column(skip_ref, rank * heads, heads), axis=0, keepdims=True)
    cum = cum_ref[...]
    dt = dt_ref[...]
    values = vw_ref[:, 0:channels]
    writes = vw_ref[:, channels:]
    reads = reads_ref[pl.ds(pl.multiple_of(b * BLOCK, BLOCK), BLOCK)]
    gate = silu(dot(tok_ref[...], wg_ref[...]).astype(bf16).astype(f32))
    scores = dot(reads, writes, ((1,), (1,)))
    causal = iota((BLOCK, BLOCK), 0) >= iota((BLOCK, BLOCK), 1)
    columns = jnp.transpose(jnp.concatenate([cum, cum], axis=0))
    parts = []
    for h in range(heads):
        gap = columns[:, h : h + 1] - cum[h : h + 1]
        mixing = scores * jnp.exp(jnp.where(causal, gap, -jnp.inf)) * dt[h : h + 1]
        parts.append(dot(mixing.astype(bf16), values[:, h * HEAD : (h + 1) * HEAD]))
    inner = jnp.concatenate(parts, axis=1)
    fade = over_channels(jnp.exp(cum), channels)
    carried = fade * dot(reads, inside_ref[0])
    base_ref[...] = (inner + carried + skip * values.astype(f32)) * gate
    far = jnp.exp(cum + before[...])
    lift_ref[...] = over_channels(far, channels) * gate
    before[...] += jnp.broadcast_to(cum[:, BLOCK - 1 :], before.shape)


def fades_of(notes, heads, channels):
    lane = iota((MISC, channels), 0)
    owner = iota((MISC, channels), 1) // HEAD
    pick = jnp.where((lane == owner) | (lane == owner + heads), 1.0, 0.0)
    return dot(jnp.where(iota(notes.shape, 1) < 2 * heads, notes, 0.0), pick, precision=HIGHEST)


def team_kernel(recv_ref, send_ref, local_ref, reach_ref):
    count, own, width = recv_ref.shape
    wide = width - MISC
    teams = send_ref.shape[0]
    channels = wide // teams
    heads = channels // HEAD
    notes = recv_ref[:, 0:1, wide:].astype(f32).reshape(count, MISC)
    fades = fades_of(notes, heads, channels)
    state = jnp.zeros((own, wide), f32)
    reach = jnp.ones((1, channels), f32)
    for k in range(count):
        local_ref[k] = state
        reach_ref[k : k + 1] = reach
        fade = jnp.concatenate([fades[k : k + 1]] * teams, axis=1)
        state = fade * state + recv_ref[k, :, 0:wide].astype(f32)
        reach = reach * fades[k : k + 1]
    total = state.astype(bf16)
    note = recv_ref[count - 1, :, wide:].astype(f32)
    first = (iota((channels, MISC), 0) == iota((channels, MISC), 1) * HEAD).astype(f32)
    high = reach.astype(bf16).astype(f32)
    low = reach - high
    packed = dot(jnp.concatenate([high, low, jnp.zeros((6, channels), f32)], axis=0), first, precision=HIGHEST)
    shifted = (iota((MISC, MISC), 0) + heads == iota((MISC, MISC), 1)).astype(f32)
    moved = dot(packed, shifted, precision=HIGHEST)
    lanes = iota((own, MISC), 1)
    note = jnp.where(lanes < heads, packed[0:1], jnp.where(lanes < 2 * heads, moved[1:2], note)).astype(bf16)
    for t in range(teams):
        send_ref[t, :, 0:wide] = total
        send_ref[t, :, wide:] = note


def prefix_kernel(recv_ref, local_ref, reach_ref, newdecay_ref, send_ref, cache_ref, direct_ref):
    teams, own, width = recv_ref.shape
    wide = width - MISC
    channels = wide // teams
    heads = channels // HEAD
    group = lax.axis_index("sp") // TEAM
    notes = recv_ref[:, 0:1, wide:].astype(f32).reshape(teams, MISC)
    fades = fades_of(notes, heads, channels)
    state = jnp.zeros((own, wide), f32)
    entering = state
    for t in range(teams):
        entering = jnp.where(group == t, state, entering)
        fade = jnp.concatenate([fades[t : t + 1]] * teams, axis=1)
        state = fade * state + recv_ref[t, :, 0:wide].astype(f32)
    for k in range(TEAM):
        reach = jnp.concatenate([reach_ref[k : k + 1]] * teams, axis=1)
        send_ref[k, :, 0:wide] = (local_ref[k] + reach * entering).astype(bf16)
    kept = state.astype(bf16).astype(f32)
    mine = kept[:, 0:channels]
    for g in range(1, teams):
        mine = jnp.where(group == g, kept[:, g * channels : (g + 1) * channels], mine)
    cache_ref[...] = mine.astype(bf16)
    note = recv_ref[teams - 1, :, wide:].astype(f32)
    reading = jnp.zeros((own, channels), f32)
    for g in range(teams):
        column = note[:, 2 * heads + g : 2 * heads + g + 1]
        reading = reading + column * kept[:, g * channels : (g + 1) * channels]
    partial = jnp.sum(reading, axis=0, keepdims=True) * newdecay_ref[...]
    high = partial.astype(bf16).astype(f32)
    low = partial - high
    rows = iota((own, channels), 0)
    share = jnp.where(rows == 0, high, jnp.where(rows == 1, low, 0.0)).astype(bf16)
    send_ref[:, :, wide:] = jnp.broadcast_to(share[None], (TEAM, own, channels))
    unshift = (iota((MISC, channels), 0) == iota((MISC, channels), 1) % HEAD + (MISC - HEAD)).astype(f32)
    laid = dot(note, unshift, precision=HIGHEST)
    direct_ref[...] = jnp.sum(jnp.where(rows == iota(rows.shape, 1) // HEAD, laid, 0.0), axis=0, keepdims=True)


def finish_kernel(recv_ref, base_ref, lift_ref, reads_ref, gain_ref, direct_ref, newgate_ref, out_ref, step_ref):
    rank = lax.axis_index("tp")
    place = lax.axis_index("sp")
    channels = base_ref.shape[1]
    wide = recv_ref.shape[2] - channels
    pieces = wide // channels
    own = recv_ref.shape[1]
    earlier = jnp.concatenate(
        [
            recv_ref[:, :, g * channels : (g + 1) * channels].astype(f32).reshape(TEAM * own, channels)
            for g in range(pieces)
        ],
        axis=0,
    ).astype(bf16)
    gain = gain_ref[:, pl.ds(pl.multiple_of(rank * channels, 128), channels)]
    gated = base_ref[...] + dot(reads_ref[...], earlier) * lift_ref[...]
    scale = lax.rsqrt(jnp.mean(gated * gated, axis=1, keepdims=True) + epsilon)
    out_ref[...] = (gated * scale * gain).astype(bf16)
    partial = jnp.sum(jnp.sum(recv_ref[:, :, wide:].astype(f32), axis=0), axis=0, keepdims=True)
    new = (partial + direct_ref[...]) * newgate_ref[0:1]
    scale = lax.rsqrt(jnp.mean(new * new, axis=1, keepdims=True) + epsilon)
    step = (new * scale * gain).astype(bf16)
    columns = lax.axis_size("sp")
    channel = iota((channels, 128), 0)
    take = (channel // columns == iota((channels, 128), 1)) & (channel % columns == place)
    picked = dot(jnp.broadcast_to(step, (16, channels)), take.astype(bf16))
    step_ref[...] = picked[0:1, 0 : channels // columns].astype(bf16)


def call(kernel, out_shape, grid=None, in_specs=None, out_specs=None, scratch=(), flops=0, name=None):
    return pl.pallas_call(
        kernel,
        out_shape=out_shape,
        grid_spec=pltpu.PrefetchScalarGridSpec(
            num_scalar_prefetch=0,
            grid=grid or (),
            in_specs=in_specs,
            out_specs=out_specs,
            scratch_shapes=scratch,
        ),
        compiler_params=pltpu.CompilerParams(
            vmem_limit_bytes=VMEM_LIMIT,
            dimension_semantics=("arbitrary",) * len(grid or ()),
        ),
        cost_estimate=pl.CostEstimate(flops=flops, transcendentals=0, bytes_accessed=1 << 20),
        name=name,
    )


def shaped(*shape, dtype=f32):
    return jax.ShapeDtypeStruct(shape, dtype)


def near(*shape, dtype=f32):
    return pltpu.VMEM(shape, dtype)


def held(array):
    return pltpu.with_memory_space_constraint(array, pltpu.VMEM)


def stored(array):
    return pltpu.with_memory_space_constraint(array, pltpu.HBM)


def on_device(
    tokens,
    fresh_token_input,
    value_matrix,
    write_matrix,
    read_matrix,
    gate_matrix,
    step_matrix,
    value_filter_taps,
    write_filter_taps,
    read_filter_taps,
    head_log_decay,
    step_offset_bias,
    decay_spike,
    bypass_scale,
    group_norm_scale,
):
    sequence_count = lax.axis_size("sp")
    length, depth = tokens.shape
    channels = value_matrix.shape[1]
    heads = channels // HEAD
    own = STATE // sequence_count
    teams = sequence_count // TEAM
    blocks = length // BLOCK
    width = channels + 2 * STATE
    wide = teams * channels
    vm = pl.BlockSpec(memory_space=pltpu.VMEM)
    far = pl.BlockSpec(memory_space=pltpu.HBM)
    inside_team = [[TEAM * t + i for i in range(TEAM)] for t in range(teams)]
    across_teams = [[TEAM * t + i for t in range(teams)] for i in range(TEAM)]

    halo = lax.ppermute(
        tokens[length - HALO :], "sp", [(i, i + 1) for i in range(sequence_count - 1)]
    )
    fresh = fresh_token_input.reshape(depth // 128, 128)
    spike = decay_spike.T
    rows, weights, step_raw, fresh_rows, new_step = call(
        project_kernel,
        (
            near(length, width, dtype=bf16),
            near(depth, width, dtype=bf16),
            near(heads, length),
            near(8, depth, dtype=bf16),
            near(heads, 8),
        ),
        in_specs=[far] * 6,
        out_specs=[vm] * 5,
        scratch=[
            pltpu.VMEM((length, depth), bf16),
            pltpu.VMEM((depth // 128, 128), bf16),
            pltpu.VMEM((step_matrix.shape[1], depth), bf16),
            pltpu.SemaphoreType.DMA((SPLIT, 4)),
            pltpu.SemaphoreType.DMA((2,)),
        ],
        flops=2 * length * depth * width,
        name="project",
    )(
        stored(tokens), stored(fresh), stored(value_matrix), stored(write_matrix),
        stored(read_matrix), stored(step_matrix.T),
    )

    decay_row, bias_row, skip_row = head_log_decay[None], step_offset_bias[None], bypass_scale[None]
    vw, edge, cum, dt, inside, new_decay, send = call(
        local_kernel,
        (
            near(length, channels + STATE, dtype=bf16),
            near(HALO, STATE),
            near(heads, length),
            near(heads, length),
            near(blocks, STATE, channels, dtype=bf16),
            near(1, channels),
            near(TEAM, own, wide + MISC, dtype=bf16),
        ),
        in_specs=[vm] * 13,
        out_specs=[vm] * 7,
        scratch=[pltpu.VMEM((length + HALO, channels + STATE), f32)],
        flops=2 * length * STATE * channels,
        name="local",
    )(
        held(rows), held(halo), held(weights), held(step_raw), held(fresh_rows), held(new_step), spike,
        value_filter_taps, write_filter_taps, read_filter_taps,
        decay_row, bias_row, skip_row,
    )

    received = lax.all_to_all(held(send), "sp", 0, 0, tiled=True, axis_index_groups=inside_team)

    send, local_states, reach = call(
        team_kernel,
        (
            near(teams, own, wide + MISC, dtype=bf16),
            near(TEAM, own, wide),
            near(TEAM, channels),
        ),
        in_specs=[vm],
        out_specs=[vm] * 3,
        name="team",
    )(held(received))

    received = lax.all_to_all(held(send), "sp", 0, 0, tiled=True, axis_index_groups=across_teams)

    send, cache_rows, direct = call(
        prefix_kernel,
        (
            near(TEAM, own, wide + channels, dtype=bf16),
            shaped(own, channels, dtype=bf16),
            near(1, channels),
        ),
        in_specs=[vm] * 4,
        out_specs=[vm] * 3,
        name="prefix",
    )(held(received), held(local_states), held(reach), held(new_decay))

    received = lax.all_to_all(held(send), "sp", 0, 0, tiled=True, axis_index_groups=inside_team)

    base, lift, new_gate, reads = call(
        inner_kernel,
        (
            near(length, channels),
            near(length, channels),
            near(8, channels),
            near(length, STATE, dtype=bf16),
        ),
        grid=(blocks,),
        in_specs=[
            pl.BlockSpec((BLOCK, depth), lambda b: (b, 0)),
            pl.BlockSpec((depth, channels), lambda b: (0, 0)),
            pl.BlockSpec(fresh_rows.shape, lambda b: (0, 0)),
            pl.BlockSpec((length, width), lambda b: (0, 0)),
            pl.BlockSpec((HALO, STATE), lambda b: (0, 0)),
            pl.BlockSpec(read_filter_taps.shape, lambda b: (0, 0)),
            pl.BlockSpec((BLOCK, channels + STATE), lambda b: (b, 0)),
            pl.BlockSpec((heads, BLOCK), lambda b: (0, b)),
            pl.BlockSpec((heads, BLOCK), lambda b: (0, b)),
            pl.BlockSpec((1, STATE, channels), lambda b: (b, 0, 0)),
            pl.BlockSpec(skip_row.shape, lambda b: (0, 0)),
            pl.BlockSpec(direct.shape, lambda b: (0, 0)),
        ],
        out_specs=[
            pl.BlockSpec((BLOCK, channels), lambda b: (b, 0)),
            pl.BlockSpec((BLOCK, channels), lambda b: (b, 0)),
            pl.BlockSpec((8, channels), lambda b: (0, 0)),
            pl.BlockSpec((length, STATE), lambda b: (0, 0)),
        ],
        scratch=[pltpu.VMEM((heads, BLOCK), f32), pltpu.VMEM((length + HALO, STATE), f32)],
        flops=2 * length * depth * channels,
        name="inner",
    )(
        stored(tokens), stored(gate_matrix), held(fresh_rows), held(rows), held(edge), read_filter_taps,
        held(vw), held(cum), held(dt), held(inside), skip_row, held(direct),
    )

    prompt_out, step_row = call(
        finish_kernel,
        (
            shaped(length, channels, dtype=bf16),
            shaped(1, channels // sequence_count, dtype=bf16),
        ),
        in_specs=[vm] * 7,
        out_specs=[vm] * 2,
        name="finish",
    )(
        held(received), held(base), held(lift), held(reads), group_norm_scale[None],
        held(direct), held(new_gate),
    )
    return (prompt_out, cache_rows, step_row.T)


def solution(mesh):
    placed = (
        P(("grp", "sp"), None),
        P("grp"),
        P(None, "tp"),
        P(None, "tp"),
        P(None, "tp"),
        P(None, "tp"),
        P(),
        P(),
        P(),
        P(),
        P(),
        P(),
        P(("grp", "sp"), "tp"),
        P(),
        P(),
    )
    return jax.shard_map(
        on_device,
        mesh=mesh,
        in_specs=placed,
        out_specs=(P(("grp", "sp"), "tp"), P(("grp", "sp"), "tp"), P(("grp", "tp"), "sp")),
        check_vma=False,
    )
```

```python
import jax
import jax.numpy as jnp
from jax import lax
from jax.experimental import pallas as pl
from jax.experimental.pallas import tpu as pltpu
from jax.sharding import PartitionSpec as P

HEAD = 64
STATE = 128
CONV = 4
BLOCK = 128
TEAM = 4
MISC = 128
HALO = 8

epsilon = 1e-06
f32 = jnp.float32
bf16 = jnp.bfloat16
HIGHEST = lax.Precision.HIGHEST
VMEM_LIMIT = 24 * 1024 * 1024
SPLIT = 4


def dot(a, b, dims=((1,), (0,)), precision=None):
    return lax.dot_general(a, b, (dims, ((), ())), precision=precision, preferred_element_type=f32)


def silu(x):
    half = 0.5 * x
    return half * jnp.tanh(half) + half


def softplus(x):
    return jnp.maximum(x, 0.0) + jnp.log1p(jnp.exp(-jnp.abs(x)))


def iota(shape, dim):
    return lax.broadcasted_iota(jnp.int32, shape, dim)


def spread(heads, channels):
    return (iota((heads, channels), 0) == iota((heads, channels), 1) // HEAD).astype(f32)


def thirds(x):
    high = x.astype(bf16)
    rest = x - high.astype(f32)
    middle = rest.astype(bf16)
    low = (rest - middle.astype(f32)).astype(bf16)
    return jnp.concatenate([high.astype(f32), middle.astype(f32), low.astype(f32)], axis=0).astype(bf16)


def over_channels(x, channels):
    heads = x.shape[0]
    shape = (3 * heads, channels)
    mask = iota(shape, 0) % heads == iota(shape, 1) // HEAD
    return dot(thirds(x), mask.astype(bf16), ((0,), (0,)))


def summed_up(x, upper):
    heads = x.shape[0]
    parts = dot(thirds(x), upper)
    return parts[0:heads] + parts[heads : 2 * heads] + parts[2 * heads :]


def own_rows(table, rank, count):
    picked = table[0:count]
    for other in range(1, table.shape[0] // count):
        picked = jnp.where(rank == other, table[other * count : (other + 1) * count], picked)
    return picked


def head_column(ref, first, count):
    row = ref[...]
    shape = (count, row.shape[1])
    return jnp.sum(jnp.where(iota(shape, 1) == iota(shape, 0) + first, row, 0.0), axis=1, keepdims=True)


def project_kernel(
    tok_hbm, fresh_hbm, wv_hbm, ww_hbm, wr_hbm, ws_hbm,
    rows_ref, weights, step_ref, fresh_ref, newstep_ref, tok, lines, steps, sems, small,
):
    depth = tok_hbm.shape[1]
    channels = wv_hbm.shape[1]
    state = ww_hbm.shape[1]
    chunk = depth // SPLIT
    get_fresh = pltpu.make_async_copy(fresh_hbm, lines, small.at[0])
    get_steps = pltpu.make_async_copy(ws_hbm, steps, small.at[1])
    get_steps.start()
    copies = []
    for k in range(SPLIT):
        at = pl.ds(k * chunk, chunk)
        moves = [
            (tok_hbm.at[:, at], tok.at[:, at]),
            (wv_hbm.at[at], weights.at[at, pl.ds(0, channels)]),
            (ww_hbm.at[at], weights.at[at, pl.ds(channels, state)]),
            (wr_hbm.at[at], weights.at[at, pl.ds(channels + state, state)]),
        ]
        copies.append(
            [pltpu.make_async_copy(a, b, sems.at[k, i]) for i, (a, b) in enumerate(moves)]
        )
    for k in range(SPLIT):
        for copy in copies[k]:
            copy.start()
    get_fresh.start()
    rank = lax.axis_index("tp")
    heads = step_ref.shape[0]
    acc = accs = None
    get_steps.wait()
    for k in range(SPLIT):
        at = slice(k * chunk, (k + 1) * chunk)
        for copy in copies[k]:
            copy.wait()
        part = dot(tok[:, at], weights[at])
        parts = dot(steps[:, at], tok[:, at], ((1,), (1,)))
        acc = part if k == 0 else acc + part
        accs = parts if k == 0 else accs + parts
        if k == SPLIT - 1:
            get_fresh.wait()
            rows = lines[...].astype(f32)
            fresh = jnp.concatenate([rows[i : i + 1] for i in range(depth // 128)], axis=1)
            fresh_ref[...] = jnp.broadcast_to(fresh, fresh_ref.shape).astype(bf16)
            table = own_rows(steps[...].astype(f32), rank, heads)
            newstep = jnp.sum(table * fresh, axis=1, keepdims=True)
            newstep_ref[...] = jnp.broadcast_to(newstep, newstep_ref.shape)
    rows_ref[...] = acc.astype(bf16)
    step_ref[...] = own_rows(accs, rank, heads)


def local_kernel(
    rows_ref, halo_ref, weights, step_ref, fresh_ref, newstep_ref, spike_ref,
    vtap_ref, wtap_ref, rtap_ref, decay_ref, bias_ref, skip_ref,
    vw_ref, edge_ref, cum_ref, dt_ref, inside_ref, newdecay_ref, send_ref, ext,
):
    rank = lax.axis_index("tp")
    length = rows_ref.shape[0]
    heads = step_ref.shape[0]
    channels = rows_ref.shape[1] - 2 * STATE
    first = rank * heads
    few = dot(jnp.concatenate([halo_ref[...], fresh_ref[...]], axis=0), weights[...])
    few = few.astype(bf16).astype(f32)
    before = few[0:HALO]
    used = channels + STATE
    edge_ref[...] = before[:, used:]
    ext[0:HALO] = before[:, 0:used]
    ext[HALO:] = rows_ref[:, 0:used].astype(f32)
    taps = jnp.concatenate(
        [
            vtap_ref[:, pl.ds(pl.multiple_of(rank * channels, 128), channels)].astype(f32),
            wtap_ref[:, pl.ds(pl.multiple_of(rank * STATE, 128), STATE)].astype(f32),
            rtap_ref[:, pl.ds(pl.multiple_of(rank * STATE, 128), STATE)].astype(f32),
        ],
        axis=1,
    )
    off = HALO - (CONV - 1)
    summed = taps[0:1, 0:used] * ext[off : off + length]
    for k in range(1, CONV):
        summed = summed + taps[k : k + 1, 0:used] * ext[off + k : off + k + length]
    vwr = silu(summed).astype(bf16)
    vw_ref[...] = vwr
    newest = taps[CONV - 1 : CONV] * few[HALO : HALO + 1]
    ending = rows_ref[length - 16 :].astype(f32)
    for k in range(CONV - 1):
        row = 16 - (CONV - 1) + k
        newest = newest + taps[k : k + 1] * ending[row : row + 1]
    newest = silu(newest).astype(bf16).astype(f32)
    new_value = newest[:, 0:channels]
    new_write = newest[:, channels : channels + STATE]
    new_read = newest[:, channels + STATE :]
    bias = head_column(bias_ref, first, heads)
    rate = jnp.exp(head_column(decay_ref, first, heads))
    upper = (iota((BLOCK, BLOCK), 0) <= iota((BLOCK, BLOCK), 1)).astype(bf16)
    expand = spread(heads, channels)
    running = jnp.zeros((STATE, channels), f32)
    total = jnp.zeros((heads, 128), f32)
    for b in range(length // BLOCK):
        at = slice(b * BLOCK, (b + 1) * BLOCK)
        dt = softplus(step_ref[:, at] + bias)
        log_decay = spike_ref[:, at] - dt * rate
        cum = summed_up(log_decay, upper)
        dt_ref[:, at] = dt
        cum_ref[:, at] = cum
        end = jnp.broadcast_to(cum[:, BLOCK - 1 :], (heads, BLOCK))
        factor = over_channels(jnp.exp(end - cum) * dt, channels)
        scaled = (factor * vwr[at, 0:channels].astype(f32)).astype(bf16)
        states = dot(vwr[at, channels : channels + STATE], scaled, ((0,), (0,)))
        fade = jnp.sum(expand * jnp.exp(end[:, 0:1]), axis=0, keepdims=True)
        inside_ref[b] = running.astype(bf16)
        running = fade * running + states
        total = total + end
    fade = jnp.exp(total)
    high = fade.astype(bf16).astype(f32)
    low = fade - high
    shape = (STATE, MISC)
    lanes = iota(shape, 1)
    rows = iota(shape, 0)
    misc = jnp.zeros(shape, f32)
    for h in range(heads):
        misc = jnp.where(lanes == h, high[h : h + 1, 0:1], misc)
        misc = jnp.where(lanes == heads + h, low[h : h + 1, 0:1], misc)
    own = STATE // lax.axis_size("sp")
    stretch = TEAM * own
    teams = STATE // stretch
    diagonal = jnp.where(rows == lanes, jnp.broadcast_to(new_read, shape), 0.0)
    read_column = jnp.sum(diagonal, axis=1, keepdims=True)
    new_dt = softplus(newstep_ref[...][:, 0:1] + bias)
    newdecay_ref[...] = jnp.sum(expand * jnp.exp(-new_dt * rate), axis=0, keepdims=True)
    skip = head_column(skip_ref, first, heads)
    weight = new_dt * jnp.sum(new_read * new_write, axis=1, keepdims=True) + skip
    direct = jnp.sum(expand * weight, axis=0, keepdims=True) * new_value
    placed = jnp.where(iota((8, channels), 0) == iota((8, channels), 1) // HEAD, direct, 0.0)
    shift = (iota((channels, MISC), 0) % HEAD + (MISC - HEAD) == iota((channels, MISC), 1)).astype(f32)
    direct_rows = dot(placed, shift, precision=HIGHEST)[0:own]
    for g in range(teams):
        at = slice(g * stretch, (g + 1) * stretch)
        piece = running[at].reshape(TEAM, own, channels).astype(bf16)
        send_ref[:, :, g * channels : (g + 1) * channels] = piece
    note = misc[0:stretch]
    for g in range(teams):
        at = slice(g * stretch, (g + 1) * stretch)
        note = jnp.where(lanes[0:stretch] == 2 * heads + g, read_column[at], note)
    note = note.reshape(TEAM, own, MISC)
    note = jnp.where(iota(note.shape, 2) >= MISC - HEAD, direct_rows[None], note).astype(bf16)
    send_ref[:, :, teams * channels :] = note


def inner_kernel(
    tok_ref, wg_ref, fresh_ref, rows_ref, edge_ref, rtap_ref, vw_ref, cum_ref, dt_ref, inside_ref,
    skip_ref, after_ref, base_ref, lift_ref, newgate_ref, reads_ref, before, ext,
):
    del after_ref
    b = pl.program_id(0)
    rank = lax.axis_index("tp")
    heads = cum_ref.shape[0]
    channels = wg_ref.shape[1]
    length = rows_ref.shape[0]

    @pl.when(b == 0)
    def _():
        before[...] = jnp.zeros_like(before)
        gate = dot(fresh_ref[...], wg_ref[...]).astype(bf16).astype(f32)
        newgate_ref[...] = silu(gate)
        ext[0:HALO] = edge_ref[...]
        ext[HALO:] = rows_ref[:, channels + STATE :].astype(f32)
        taps = rtap_ref[:, pl.ds(pl.multiple_of(rank * STATE, 128), STATE)].astype(f32)
        off = HALO - (CONV - 1)
        summed = taps[0:1] * ext[off : off + length]
        for k in range(1, CONV):
            summed = summed + taps[k : k + 1] * ext[off + k : off + k + length]
        reads_ref[...] = silu(summed).astype(bf16)

    expand = spread(heads, channels)
    skip = jnp.sum(expand * head_column(skip_ref, rank * heads, heads), axis=0, keepdims=True)
    cum = cum_ref[...]
    dt = dt_ref[...]
    values = vw_ref[:, 0:channels]
    writes = vw_ref[:, channels:]
    reads = reads_ref[pl.ds(pl.multiple_of(b * BLOCK, BLOCK), BLOCK)]
    gate = silu(dot(tok_ref[...], wg_ref[...]).astype(bf16).astype(f32))
    scores = dot(reads, writes, ((1,), (1,)))
    causal = iota((BLOCK, BLOCK), 0) >= iota((BLOCK, BLOCK), 1)
    columns = jnp.transpose(jnp.concatenate([cum, cum], axis=0))
    parts = []
    for h in range(heads):
        gap = columns[:, h : h + 1] - cum[h : h + 1]
        mixing = scores * jnp.exp(jnp.where(causal, gap, -jnp.inf)) * dt[h : h + 1]
        parts.append(dot(mixing.astype(bf16), values[:, h * HEAD : (h + 1) * HEAD]))
    inner = jnp.concatenate(parts, axis=1)
    fade = over_channels(jnp.exp(cum), channels)
    carried = fade * dot(reads, inside_ref[0])
    base_ref[...] = (inner + carried + skip * values.astype(f32)) * gate
    far = jnp.exp(cum + before[...])
    lift_ref[...] = over_channels(far, channels) * gate
    before[...] += jnp.broadcast_to(cum[:, BLOCK - 1 :], before.shape)


def places(teams):
    return [*reversed(range(teams))]


def fades_of(notes, heads, channels):
    lane = iota((MISC, channels), 0)
    owner = iota((MISC, channels), 1) // HEAD
    pick = jnp.where((lane == owner) | (lane == owner + heads), 1.0, 0.0)
    return dot(jnp.where(iota(notes.shape, 1) < 2 * heads, notes, 0.0), pick, precision=HIGHEST)


def team_kernel(recv_ref, send_ref, local_ref, reach_ref):
    count, own, width = recv_ref.shape
    wide = width - MISC
    teams = send_ref.shape[0]
    channels = wide // teams
    heads = channels // HEAD
    notes = recv_ref[:, 0:1, wide:].astype(f32).reshape(count, MISC)
    fades = fades_of(notes, heads, channels)
    state = jnp.zeros((own, wide), f32)
    reach = jnp.ones((1, channels), f32)
    for k in range(count):
        local_ref[k] = state
        reach_ref[k : k + 1] = reach
        fade = jnp.concatenate([fades[k : k + 1]] * teams, axis=1)
        state = fade * state + recv_ref[k, :, 0:wide].astype(f32)
        reach = reach * fades[k : k + 1]
    total = state.astype(bf16)
    note = recv_ref[count - 1, :, wide:].astype(f32)
    first = (iota((channels, MISC), 0) == iota((channels, MISC), 1) * HEAD).astype(f32)
    high = reach.astype(bf16).astype(f32)
    low = reach - high
    packed = dot(jnp.concatenate([high, low, jnp.zeros((6, channels), f32)], axis=0), first, precision=HIGHEST)
    shifted = (iota((MISC, MISC), 0) + heads == iota((MISC, MISC), 1)).astype(f32)
    moved = dot(packed, shifted, precision=HIGHEST)
    lanes = iota((own, MISC), 1)
    note = jnp.where(lanes < heads, packed[0:1], jnp.where(lanes < 2 * heads, moved[1:2], note)).astype(bf16)
    for t in range(teams):
        send_ref[t, :, 0:wide] = total
        send_ref[t, :, wide:] = note


def prefix_kernel(recv_ref, local_ref, reach_ref, newdecay_ref, send_ref, cache_ref, direct_ref):
    teams, own, width = recv_ref.shape
    wide = width - MISC
    channels = wide // teams
    heads = channels // HEAD
    group = lax.axis_index("sp") // TEAM
    notes = recv_ref[:, 0:1, wide:].astype(f32).reshape(teams, MISC)
    fades = fades_of(notes, heads, channels)
    state = jnp.zeros((own, wide), f32)
    entering = state
    place = {t: p for p, t in enumerate(places(teams))}
    for t in range(teams):
        at = place[t]
        entering = jnp.where(group == t, state, entering)
        fade = jnp.concatenate([fades[at : at + 1]] * teams, axis=1)
        state = fade * state + recv_ref[at, :, 0:wide].astype(f32)
    for k in range(TEAM):
        reach = jnp.concatenate([reach_ref[k : k + 1]] * teams, axis=1)
        send_ref[k, :, 0:wide] = (local_ref[k] + reach * entering).astype(bf16)
    kept = state.astype(bf16).astype(f32)
    mine = kept[:, 0:channels]
    for g in range(1, teams):
        mine = jnp.where(group == g, kept[:, g * channels : (g + 1) * channels], mine)
    cache_ref[...] = mine.astype(bf16)
    note = recv_ref[place[teams - 1], :, wide:].astype(f32)
    reading = jnp.zeros((own, channels), f32)
    for g in range(teams):
        column = note[:, 2 * heads + g : 2 * heads + g + 1]
        reading = reading + column * kept[:, g * channels : (g + 1) * channels]
    partial = jnp.sum(reading, axis=0, keepdims=True) * newdecay_ref[...]
    high = partial.astype(bf16).astype(f32)
    low = partial - high
    rows = iota((own, channels), 0)
    share = jnp.where(rows == 0, high, jnp.where(rows == 1, low, 0.0)).astype(bf16)
    send_ref[:, :, wide:] = jnp.broadcast_to(share[None], (TEAM, own, channels))
    unshift = (iota((MISC, channels), 0) == iota((MISC, channels), 1) % HEAD + (MISC - HEAD)).astype(f32)
    laid = dot(note, unshift, precision=HIGHEST)
    direct_ref[...] = jnp.sum(jnp.where(rows == iota(rows.shape, 1) // HEAD, laid, 0.0), axis=0, keepdims=True)


def finish_kernel(recv_ref, base_ref, lift_ref, reads_ref, gain_ref, direct_ref, newgate_ref, out_ref, step_ref):
    rank = lax.axis_index("tp")
    place = lax.axis_index("sp")
    channels = base_ref.shape[1]
    wide = recv_ref.shape[2] - channels
    pieces = wide // channels
    own = recv_ref.shape[1]
    earlier = jnp.concatenate(
        [
            recv_ref[:, :, g * channels : (g + 1) * channels].astype(f32).reshape(TEAM * own, channels)
            for g in range(pieces)
        ],
        axis=0,
    ).astype(bf16)
    gain = gain_ref[:, pl.ds(pl.multiple_of(rank * channels, 128), channels)]
    gated = base_ref[...] + dot(reads_ref[...], earlier) * lift_ref[...]
    scale = lax.rsqrt(jnp.mean(gated * gated, axis=1, keepdims=True) + epsilon)
    out_ref[...] = (gated * scale * gain).astype(bf16)
    partial = jnp.sum(jnp.sum(recv_ref[:, :, wide:].astype(f32), axis=0), axis=0, keepdims=True)
    new = (partial + direct_ref[...]) * newgate_ref[0:1]
    scale = lax.rsqrt(jnp.mean(new * new, axis=1, keepdims=True) + epsilon)
    step = (new * scale * gain).astype(bf16)
    columns = lax.axis_size("sp")
    channel = iota((channels, 128), 0)
    take = (channel // columns == iota((channels, 128), 1)) & (channel % columns == place)
    picked = dot(jnp.broadcast_to(step, (16, channels)), take.astype(bf16))
    step_ref[...] = picked[0:1, 0 : channels // columns].astype(bf16)


def call(kernel, out_shape, grid=None, in_specs=None, out_specs=None, scratch=(), flops=0, name=None):
    return pl.pallas_call(
        kernel,
        out_shape=out_shape,
        grid_spec=pltpu.PrefetchScalarGridSpec(
            num_scalar_prefetch=0,
            grid=grid or (),
            in_specs=in_specs,
            out_specs=out_specs,
            scratch_shapes=scratch,
        ),
        compiler_params=pltpu.CompilerParams(
            vmem_limit_bytes=VMEM_LIMIT,
            dimension_semantics=("arbitrary",) * len(grid or ()),
        ),
        cost_estimate=pl.CostEstimate(flops=flops, transcendentals=0, bytes_accessed=1 << 20),
        name=name,
    )


def shaped(*shape, dtype=f32):
    return jax.ShapeDtypeStruct(shape, dtype)


def near(*shape, dtype=f32):
    return pltpu.VMEM(shape, dtype)


def held(array):
    return pltpu.with_memory_space_constraint(array, pltpu.VMEM)


def stored(array):
    return pltpu.with_memory_space_constraint(array, pltpu.HBM)


def on_device(
    tokens,
    fresh_token_input,
    value_matrix,
    write_matrix,
    read_matrix,
    gate_matrix,
    step_matrix,
    value_filter_taps,
    write_filter_taps,
    read_filter_taps,
    head_log_decay,
    step_offset_bias,
    decay_spike,
    bypass_scale,
    group_norm_scale,
):
    sequence_count = lax.axis_size("sp")
    length, depth = tokens.shape
    channels = value_matrix.shape[1]
    heads = channels // HEAD
    own = STATE // sequence_count
    teams = sequence_count // TEAM
    blocks = length // BLOCK
    width = channels + 2 * STATE
    wide = teams * channels
    vm = pl.BlockSpec(memory_space=pltpu.VMEM)
    far = pl.BlockSpec(memory_space=pltpu.HBM)
    inside_team = [[TEAM * t + i for i in range(TEAM)] for t in range(teams)]
    across_teams = [[TEAM * t + i for t in places(teams)] for i in range(TEAM)]

    halo = lax.ppermute(
        tokens[length - HALO :], "sp", [(i, i + 1) for i in range(sequence_count - 1)]
    )
    fresh = fresh_token_input.reshape(depth // 128, 128)
    spike = decay_spike.T
    rows, weights, step_raw, fresh_rows, new_step = call(
        project_kernel,
        (
            near(length, width, dtype=bf16),
            near(depth, width, dtype=bf16),
            near(heads, length),
            near(8, depth, dtype=bf16),
            near(heads, 8),
        ),
        in_specs=[far] * 6,
        out_specs=[vm] * 5,
        scratch=[
            pltpu.VMEM((length, depth), bf16),
            pltpu.VMEM((depth // 128, 128), bf16),
            pltpu.VMEM((step_matrix.shape[1], depth), bf16),
            pltpu.SemaphoreType.DMA((SPLIT, 4)),
            pltpu.SemaphoreType.DMA((2,)),
        ],
        flops=2 * length * depth * width,
        name="project",
    )(
        stored(tokens), stored(fresh), stored(value_matrix), stored(write_matrix),
        stored(read_matrix), stored(step_matrix.T),
    )

    decay_row, bias_row, skip_row = head_log_decay[None], step_offset_bias[None], bypass_scale[None]
    vw, edge, cum, dt, inside, new_decay, send = call(
        local_kernel,
        (
            near(length, channels + STATE, dtype=bf16),
            near(HALO, STATE),
            near(heads, length),
            near(heads, length),
            near(blocks, STATE, channels, dtype=bf16),
            near(1, channels),
            near(TEAM, own, wide + MISC, dtype=bf16),
        ),
        in_specs=[vm] * 13,
        out_specs=[vm] * 7,
        scratch=[pltpu.VMEM((length + HALO, channels + STATE), f32)],
        flops=2 * length * STATE * channels,
        name="local",
    )(
        held(rows), held(halo), held(weights), held(step_raw), held(fresh_rows), held(new_step), spike,
        value_filter_taps, write_filter_taps, read_filter_taps,
        decay_row, bias_row, skip_row,
    )

    received = lax.all_to_all(held(send), "sp", 0, 0, tiled=True, axis_index_groups=inside_team)

    send, local_states, reach = call(
        team_kernel,
        (
            near(teams, own, wide + MISC, dtype=bf16),
            near(TEAM, own, wide),
            near(TEAM, channels),
        ),
        in_specs=[vm],
        out_specs=[vm] * 3,
        name="team",
    )(held(received))

    received = lax.all_to_all(held(send), "sp", 0, 0, tiled=True, axis_index_groups=across_teams)

    send, cache_rows, direct = call(
        prefix_kernel,
        (
            near(TEAM, own, wide + channels, dtype=bf16),
            shaped(own, channels, dtype=bf16),
            near(1, channels),
        ),
        in_specs=[vm] * 4,
        out_specs=[vm] * 3,
        name="prefix",
    )(held(received), held(local_states), held(reach), held(new_decay))

    received = lax.all_to_all(held(send), "sp", 0, 0, tiled=True, axis_index_groups=inside_team)

    base, lift, new_gate, reads = call(
        inner_kernel,
        (
            near(length, channels),
            near(length, channels),
            near(8, channels),
            near(length, STATE, dtype=bf16),
        ),
        grid=(blocks,),
        in_specs=[
            pl.BlockSpec((BLOCK, depth), lambda b: (b, 0)),
            pl.BlockSpec((depth, channels), lambda b: (0, 0)),
            pl.BlockSpec(fresh_rows.shape, lambda b: (0, 0)),
            pl.BlockSpec((length, width), lambda b: (0, 0)),
            pl.BlockSpec((HALO, STATE), lambda b: (0, 0)),
            pl.BlockSpec(read_filter_taps.shape, lambda b: (0, 0)),
            pl.BlockSpec((BLOCK, channels + STATE), lambda b: (b, 0)),
            pl.BlockSpec((heads, BLOCK), lambda b: (0, b)),
            pl.BlockSpec((heads, BLOCK), lambda b: (0, b)),
            pl.BlockSpec((1, STATE, channels), lambda b: (b, 0, 0)),
            pl.BlockSpec(skip_row.shape, lambda b: (0, 0)),
            pl.BlockSpec(direct.shape, lambda b: (0, 0)),
        ],
        out_specs=[
            pl.BlockSpec((BLOCK, channels), lambda b: (b, 0)),
            pl.BlockSpec((BLOCK, channels), lambda b: (b, 0)),
            pl.BlockSpec((8, channels), lambda b: (0, 0)),
            pl.BlockSpec((length, STATE), lambda b: (0, 0)),
        ],
        scratch=[pltpu.VMEM((heads, BLOCK), f32), pltpu.VMEM((length + HALO, STATE), f32)],
        flops=2 * length * depth * channels,
        name="inner",
    )(
        stored(tokens), stored(gate_matrix), held(fresh_rows), held(rows), held(edge), read_filter_taps,
        held(vw), held(cum), held(dt), held(inside), skip_row, held(direct),
    )

    prompt_out, step_row = call(
        finish_kernel,
        (
            shaped(length, channels, dtype=bf16),
            shaped(1, channels // sequence_count, dtype=bf16),
        ),
        in_specs=[vm] * 7,
        out_specs=[vm] * 2,
        name="finish",
    )(
        held(received), held(base), held(lift), held(reads), group_norm_scale[None],
        held(direct), held(new_gate),
    )
    return (prompt_out, cache_rows, step_row.T)


def solution(mesh):
    placed = (
        P(("grp", "sp"), None),
        P("grp"),
        P(None, "tp"),
        P(None, "tp"),
        P(None, "tp"),
        P(None, "tp"),
        P(),
        P(),
        P(),
        P(),
        P(),
        P(),
        P(("grp", "sp"), "tp"),
        P(),
        P(),
    )
    return jax.shard_map(
        on_device,
        mesh=mesh,
        in_specs=placed,
        out_specs=(P(("grp", "sp"), "tp"), P(("grp", "sp"), "tp"), P(("grp", "tp"), "sp")),
        check_vma=False,
    )
```

```python
import jax
import jax.numpy as jnp
from jax import lax
from jax.experimental import pallas as pl
from jax.experimental.pallas import tpu as pltpu
from jax.sharding import PartitionSpec as P

HEAD = 64
STATE = 128
CONV = 4
BLOCK = 128
TEAM = 4
MISC = 128
HALO = 8

epsilon = 1e-06
f32 = jnp.float32
bf16 = jnp.bfloat16
HIGHEST = lax.Precision.HIGHEST
VMEM_LIMIT = 24 * 1024 * 1024
SPLIT = 4


def dot(a, b, dims=((1,), (0,)), precision=None):
    return lax.dot_general(a, b, (dims, ((), ())), precision=precision, preferred_element_type=f32)


def silu(x):
    half = 0.5 * x
    return half * jnp.tanh(half) + half


def softplus(x):
    return jnp.maximum(x, 0.0) + jnp.log1p(jnp.exp(-jnp.abs(x)))


def iota(shape, dim):
    return lax.broadcasted_iota(jnp.int32, shape, dim)


def spread(heads, channels):
    return (iota((heads, channels), 0) == iota((heads, channels), 1) // HEAD).astype(f32)


def thirds(x):
    high = x.astype(bf16)
    rest = x - high.astype(f32)
    middle = rest.astype(bf16)
    low = (rest - middle.astype(f32)).astype(bf16)
    return jnp.concatenate([high.astype(f32), middle.astype(f32), low.astype(f32)], axis=0).astype(bf16)


def over_channels(x, channels):
    heads = x.shape[0]
    shape = (3 * heads, channels)
    mask = iota(shape, 0) % heads == iota(shape, 1) // HEAD
    return dot(thirds(x), mask.astype(bf16), ((0,), (0,)))


def summed_up(x, upper):
    heads = x.shape[0]
    parts = dot(thirds(x), upper)
    return parts[0:heads] + parts[heads : 2 * heads] + parts[2 * heads :]


def own_rows(table, rank, count):
    picked = table[0:count]
    for other in range(1, table.shape[0] // count):
        picked = jnp.where(rank == other, table[other * count : (other + 1) * count], picked)
    return picked


def head_column(ref, first, count):
    row = ref[...]
    shape = (count, row.shape[1])
    return jnp.sum(jnp.where(iota(shape, 1) == iota(shape, 0) + first, row, 0.0), axis=1, keepdims=True)


def project_kernel(
    tok_hbm, fresh_hbm, wv_hbm, ww_hbm, wr_hbm, ws_hbm,
    rows_ref, weights, step_ref, fresh_ref, newstep_ref, tok, lines, steps, sems, small,
):
    depth = tok_hbm.shape[1]
    channels = wv_hbm.shape[1]
    state = ww_hbm.shape[1]
    chunk = depth // SPLIT
    get_fresh = pltpu.make_async_copy(fresh_hbm, lines, small.at[0])
    get_steps = pltpu.make_async_copy(ws_hbm, steps, small.at[1])
    get_steps.start()
    copies = []
    for k in range(SPLIT):
        at = pl.ds(k * chunk, chunk)
        moves = [
            (tok_hbm.at[:, at], tok.at[:, at]),
            (wv_hbm.at[at], weights.at[at, pl.ds(0, channels)]),
            (ww_hbm.at[at], weights.at[at, pl.ds(channels, state)]),
            (wr_hbm.at[at], weights.at[at, pl.ds(channels + state, state)]),
        ]
        copies.append(
            [pltpu.make_async_copy(a, b, sems.at[k, i]) for i, (a, b) in enumerate(moves)]
        )
    for k in range(SPLIT):
        for copy in copies[k]:
            copy.start()
    get_fresh.start()
    rank = lax.axis_index("tp")
    heads = step_ref.shape[0]
    acc = accs = None
    get_steps.wait()
    for k in range(SPLIT):
        at = slice(k * chunk, (k + 1) * chunk)
        for copy in copies[k]:
            copy.wait()
        part = dot(tok[:, at], weights[at])
        parts = dot(steps[:, at], tok[:, at], ((1,), (1,)))
        acc = part if k == 0 else acc + part
        accs = parts if k == 0 else accs + parts
        if k == SPLIT - 1:
            get_fresh.wait()
            rows = lines[...].astype(f32)
            fresh = jnp.concatenate([rows[i : i + 1] for i in range(depth // 128)], axis=1)
            fresh_ref[...] = jnp.broadcast_to(fresh, fresh_ref.shape).astype(bf16)
            table = own_rows(steps[...].astype(f32), rank, heads)
            newstep = jnp.sum(table * fresh, axis=1, keepdims=True)
            newstep_ref[...] = jnp.broadcast_to(newstep, newstep_ref.shape)
    rows_ref[...] = acc.astype(bf16)
    step_ref[...] = own_rows(accs, rank, heads)


def local_kernel(
    rows_ref, halo_ref, weights, step_ref, fresh_ref, newstep_ref, spike_ref,
    vtap_ref, wtap_ref, rtap_ref, decay_ref, bias_ref, skip_ref,
    vw_ref, edge_ref, cum_ref, dt_ref, inside_ref, newdecay_ref, send_ref, ext,
):
    rank = lax.axis_index("tp")
    length = rows_ref.shape[0]
    heads = step_ref.shape[0]
    channels = rows_ref.shape[1] - 2 * STATE
    first = rank * heads
    few = dot(jnp.concatenate([halo_ref[...], fresh_ref[...]], axis=0), weights[...])
    few = few.astype(bf16).astype(f32)
    before = few[0:HALO]
    used = channels + STATE
    edge_ref[...] = before[:, used:]
    ext[0:HALO] = before[:, 0:used]
    ext[HALO:] = rows_ref[:, 0:used].astype(f32)
    taps = jnp.concatenate(
        [
            vtap_ref[:, pl.ds(pl.multiple_of(rank * channels, 128), channels)].astype(f32),
            wtap_ref[:, pl.ds(pl.multiple_of(rank * STATE, 128), STATE)].astype(f32),
            rtap_ref[:, pl.ds(pl.multiple_of(rank * STATE, 128), STATE)].astype(f32),
        ],
        axis=1,
    )
    off = HALO - (CONV - 1)
    summed = taps[0:1, 0:used] * ext[off : off + length]
    for k in range(1, CONV):
        summed = summed + taps[k : k + 1, 0:used] * ext[off + k : off + k + length]
    vwr = silu(summed).astype(bf16)
    vw_ref[...] = vwr
    newest = taps[CONV - 1 : CONV] * few[HALO : HALO + 1]
    ending = rows_ref[length - 16 :].astype(f32)
    for k in range(CONV - 1):
        row = 16 - (CONV - 1) + k
        newest = newest + taps[k : k + 1] * ending[row : row + 1]
    newest = silu(newest).astype(bf16).astype(f32)
    new_value = newest[:, 0:channels]
    new_write = newest[:, channels : channels + STATE]
    new_read = newest[:, channels + STATE :]
    bias = head_column(bias_ref, first, heads)
    rate = jnp.exp(head_column(decay_ref, first, heads))
    upper = (iota((BLOCK, BLOCK), 0) <= iota((BLOCK, BLOCK), 1)).astype(bf16)
    expand = spread(heads, channels)
    running = jnp.zeros((STATE, channels), f32)
    total = jnp.zeros((heads, 128), f32)
    for b in range(length // BLOCK):
        at = slice(b * BLOCK, (b + 1) * BLOCK)
        dt = softplus(step_ref[:, at] + bias)
        log_decay = spike_ref[:, at] - dt * rate
        cum = summed_up(log_decay, upper)
        dt_ref[:, at] = dt
        cum_ref[:, at] = cum
        end = jnp.broadcast_to(cum[:, BLOCK - 1 :], (heads, BLOCK))
        factor = over_channels(jnp.exp(end - cum) * dt, channels)
        scaled = (factor * vwr[at, 0:channels].astype(f32)).astype(bf16)
        states = dot(vwr[at, channels : channels + STATE], scaled, ((0,), (0,)))
        fade = jnp.sum(expand * jnp.exp(end[:, 0:1]), axis=0, keepdims=True)
        inside_ref[b] = running.astype(bf16)
        running = fade * running + states
        total = total + end
    fade = jnp.exp(total)
    high = fade.astype(bf16).astype(f32)
    low = fade - high
    shape = (STATE, MISC)
    lanes = iota(shape, 1)
    rows = iota(shape, 0)
    misc = jnp.zeros(shape, f32)
    for h in range(heads):
        misc = jnp.where(lanes == h, high[h : h + 1, 0:1], misc)
        misc = jnp.where(lanes == heads + h, low[h : h + 1, 0:1], misc)
    own = STATE // lax.axis_size("sp")
    stretch = TEAM * own
    teams = STATE // stretch
    diagonal = jnp.where(rows == lanes, jnp.broadcast_to(new_read, shape), 0.0)
    read_column = jnp.sum(diagonal, axis=1, keepdims=True)
    new_dt = softplus(newstep_ref[...][:, 0:1] + bias)
    newdecay_ref[...] = jnp.sum(expand * jnp.exp(-new_dt * rate), axis=0, keepdims=True)
    skip = head_column(skip_ref, first, heads)
    weight = new_dt * jnp.sum(new_read * new_write, axis=1, keepdims=True) + skip
    direct = jnp.sum(expand * weight, axis=0, keepdims=True) * new_value
    placed = jnp.where(iota((8, channels), 0) == iota((8, channels), 1) // HEAD, direct, 0.0)
    shift = (iota((channels, MISC), 0) % HEAD + (MISC - HEAD) == iota((channels, MISC), 1)).astype(f32)
    direct_rows = dot(placed, shift, precision=HIGHEST)[0:own]
    for g in range(teams):
        at = slice(g * stretch, (g + 1) * stretch)
        piece = running[at].reshape(TEAM, own, channels).astype(bf16)
        for p, member in enumerate(places(TEAM)):
            send_ref[p, :, g * channels : (g + 1) * channels] = piece[member]
    note = misc[0:stretch]
    for g in range(teams):
        at = slice(g * stretch, (g + 1) * stretch)
        note = jnp.where(lanes[0:stretch] == 2 * heads + g, read_column[at], note)
    note = note.reshape(TEAM, own, MISC)
    note = jnp.where(iota(note.shape, 2) >= MISC - HEAD, direct_rows[None], note).astype(bf16)
    for p, member in enumerate(places(TEAM)):
        send_ref[p, :, teams * channels :] = note[member]


def inner_kernel(
    tok_ref, wg_ref, fresh_ref, rows_ref, edge_ref, rtap_ref, vw_ref, cum_ref, dt_ref, inside_ref,
    skip_ref, after_ref, base_ref, lift_ref, newgate_ref, reads_ref, before, ext,
):
    del after_ref
    b = pl.program_id(0)
    rank = lax.axis_index("tp")
    heads = cum_ref.shape[0]
    channels = wg_ref.shape[1]
    length = rows_ref.shape[0]

    @pl.when(b == 0)
    def _():
        before[...] = jnp.zeros_like(before)
        gate = dot(fresh_ref[...], wg_ref[...]).astype(bf16).astype(f32)
        newgate_ref[...] = silu(gate)
        ext[0:HALO] = edge_ref[...]
        ext[HALO:] = rows_ref[:, channels + STATE :].astype(f32)
        taps = rtap_ref[:, pl.ds(pl.multiple_of(rank * STATE, 128), STATE)].astype(f32)
        off = HALO - (CONV - 1)
        summed = taps[0:1] * ext[off : off + length]
        for k in range(1, CONV):
            summed = summed + taps[k : k + 1] * ext[off + k : off + k + length]
        reads_ref[...] = silu(summed).astype(bf16)

    expand = spread(heads, channels)
    skip = jnp.sum(expand * head_column(skip_ref, rank * heads, heads), axis=0, keepdims=True)
    cum = cum_ref[...]
    dt = dt_ref[...]
    values = vw_ref[:, 0:channels]
    writes = vw_ref[:, channels:]
    reads = reads_ref[pl.ds(pl.multiple_of(b * BLOCK, BLOCK), BLOCK)]
    gate = silu(dot(tok_ref[...], wg_ref[...]).astype(bf16).astype(f32))
    scores = dot(reads, writes, ((1,), (1,)))
    causal = iota((BLOCK, BLOCK), 0) >= iota((BLOCK, BLOCK), 1)
    columns = jnp.transpose(jnp.concatenate([cum, cum], axis=0))
    parts = []
    for h in range(heads):
        gap = columns[:, h : h + 1] - cum[h : h + 1]
        mixing = scores * jnp.exp(jnp.where(causal, gap, -jnp.inf)) * dt[h : h + 1]
        parts.append(dot(mixing.astype(bf16), values[:, h * HEAD : (h + 1) * HEAD]))
    inner = jnp.concatenate(parts, axis=1)
    fade = over_channels(jnp.exp(cum), channels)
    carried = fade * dot(reads, inside_ref[0])
    base_ref[...] = (inner + carried + skip * values.astype(f32)) * gate
    far = jnp.exp(cum + before[...])
    lift_ref[...] = over_channels(far, channels) * gate
    before[...] += jnp.broadcast_to(cum[:, BLOCK - 1 :], before.shape)


def places(count):
    return [*reversed(range(count))]


def fades_of(notes, heads, channels):
    lane = iota((MISC, channels), 0)
    owner = iota((MISC, channels), 1) // HEAD
    pick = jnp.where((lane == owner) | (lane == owner + heads), 1.0, 0.0)
    return dot(jnp.where(iota(notes.shape, 1) < 2 * heads, notes, 0.0), pick, precision=HIGHEST)


def team_kernel(recv_ref, send_ref, local_ref, reach_ref):
    count, own, width = recv_ref.shape
    wide = width - MISC
    teams = send_ref.shape[0]
    channels = wide // teams
    heads = channels // HEAD
    notes = recv_ref[:, 0:1, wide:].astype(f32).reshape(count, MISC)
    fades = fades_of(notes, heads, channels)
    state = jnp.zeros((own, wide), f32)
    reach = jnp.ones((1, channels), f32)
    place = {member: p for p, member in enumerate(places(count))}
    for k in range(count):
        local_ref[k] = state
        reach_ref[k : k + 1] = reach
        at = place[k]
        fade = jnp.concatenate([fades[at : at + 1]] * teams, axis=1)
        state = fade * state + recv_ref[at, :, 0:wide].astype(f32)
        reach = reach * fades[at : at + 1]
    total = state.astype(bf16)
    note = recv_ref[place[count - 1], :, wide:].astype(f32)
    first = (iota((channels, MISC), 0) == iota((channels, MISC), 1) * HEAD).astype(f32)
    high = reach.astype(bf16).astype(f32)
    low = reach - high
    packed = dot(jnp.concatenate([high, low, jnp.zeros((6, channels), f32)], axis=0), first, precision=HIGHEST)
    shifted = (iota((MISC, MISC), 0) + heads == iota((MISC, MISC), 1)).astype(f32)
    moved = dot(packed, shifted, precision=HIGHEST)
    lanes = iota((own, MISC), 1)
    note = jnp.where(lanes < heads, packed[0:1], jnp.where(lanes < 2 * heads, moved[1:2], note)).astype(bf16)
    for t in range(teams):
        send_ref[t, :, 0:wide] = total
        send_ref[t, :, wide:] = note


def prefix_kernel(recv_ref, local_ref, reach_ref, newdecay_ref, send_ref, cache_ref, direct_ref):
    teams, own, width = recv_ref.shape
    wide = width - MISC
    channels = wide // teams
    heads = channels // HEAD
    group = lax.axis_index("sp") // TEAM
    notes = recv_ref[:, 0:1, wide:].astype(f32).reshape(teams, MISC)
    fades = fades_of(notes, heads, channels)
    state = jnp.zeros((own, wide), f32)
    entering = state
    place = {t: p for p, t in enumerate(places(teams))}
    for t in range(teams):
        at = place[t]
        entering = jnp.where(group == t, state, entering)
        fade = jnp.concatenate([fades[at : at + 1]] * teams, axis=1)
        state = fade * state + recv_ref[at, :, 0:wide].astype(f32)
    for p, k in enumerate(places(TEAM)):
        reach = jnp.concatenate([reach_ref[k : k + 1]] * teams, axis=1)
        send_ref[p, :, 0:wide] = (local_ref[k] + reach * entering).astype(bf16)
    kept = state.astype(bf16).astype(f32)
    mine = kept[:, 0:channels]
    for g in range(1, teams):
        mine = jnp.where(group == g, kept[:, g * channels : (g + 1) * channels], mine)
    cache_ref[...] = mine.astype(bf16)
    note = recv_ref[place[teams - 1], :, wide:].astype(f32)
    reading = jnp.zeros((own, channels), f32)
    for g in range(teams):
        column = note[:, 2 * heads + g : 2 * heads + g + 1]
        reading = reading + column * kept[:, g * channels : (g + 1) * channels]
    partial = jnp.sum(reading, axis=0, keepdims=True) * newdecay_ref[...]
    high = partial.astype(bf16).astype(f32)
    low = partial - high
    rows = iota((own, channels), 0)
    share = jnp.where(rows == 0, high, jnp.where(rows == 1, low, 0.0)).astype(bf16)
    send_ref[:, :, wide:] = jnp.broadcast_to(share[None], (TEAM, own, channels))
    unshift = (iota((MISC, channels), 0) == iota((MISC, channels), 1) % HEAD + (MISC - HEAD)).astype(f32)
    laid = dot(note, unshift, precision=HIGHEST)
    direct_ref[...] = jnp.sum(jnp.where(rows == iota(rows.shape, 1) // HEAD, laid, 0.0), axis=0, keepdims=True)


def finish_kernel(recv_ref, base_ref, lift_ref, reads_ref, gain_ref, direct_ref, newgate_ref, out_ref, step_ref):
    rank = lax.axis_index("tp")
    place = lax.axis_index("sp")
    channels = base_ref.shape[1]
    wide = recv_ref.shape[2] - channels
    pieces = wide // channels
    own = recv_ref.shape[1]
    spot = {member: p for p, member in enumerate(places(TEAM))}
    earlier = jnp.concatenate(
        [
            recv_ref[spot[i], :, g * channels : (g + 1) * channels].astype(f32)
            for g in range(pieces)
            for i in range(TEAM)
        ],
        axis=0,
    ).astype(bf16)
    gain = gain_ref[:, pl.ds(pl.multiple_of(rank * channels, 128), channels)]
    gated = base_ref[...] + dot(reads_ref[...], earlier) * lift_ref[...]
    scale = lax.rsqrt(jnp.mean(gated * gated, axis=1, keepdims=True) + epsilon)
    out_ref[...] = (gated * scale * gain).astype(bf16)
    partial = jnp.sum(jnp.sum(recv_ref[:, :, wide:].astype(f32), axis=0), axis=0, keepdims=True)
    new = (partial + direct_ref[...]) * newgate_ref[0:1]
    scale = lax.rsqrt(jnp.mean(new * new, axis=1, keepdims=True) + epsilon)
    step = (new * scale * gain).astype(bf16)
    columns = lax.axis_size("sp")
    channel = iota((channels, 128), 0)
    take = (channel // columns == iota((channels, 128), 1)) & (channel % columns == place)
    picked = dot(jnp.broadcast_to(step, (16, channels)), take.astype(bf16))
    step_ref[...] = picked[0:1, 0 : channels // columns].astype(bf16)


def call(kernel, out_shape, grid=None, in_specs=None, out_specs=None, scratch=(), flops=0, name=None):
    return pl.pallas_call(
        kernel,
        out_shape=out_shape,
        grid_spec=pltpu.PrefetchScalarGridSpec(
            num_scalar_prefetch=0,
            grid=grid or (),
            in_specs=in_specs,
            out_specs=out_specs,
            scratch_shapes=scratch,
        ),
        compiler_params=pltpu.CompilerParams(
            vmem_limit_bytes=VMEM_LIMIT,
            dimension_semantics=("arbitrary",) * len(grid or ()),
        ),
        cost_estimate=pl.CostEstimate(flops=flops, transcendentals=0, bytes_accessed=1 << 20),
        name=name,
    )


def shaped(*shape, dtype=f32):
    return jax.ShapeDtypeStruct(shape, dtype)


def near(*shape, dtype=f32):
    return pltpu.VMEM(shape, dtype)


def held(array):
    return pltpu.with_memory_space_constraint(array, pltpu.VMEM)


def stored(array):
    return pltpu.with_memory_space_constraint(array, pltpu.HBM)


def on_device(
    tokens,
    fresh_token_input,
    value_matrix,
    write_matrix,
    read_matrix,
    gate_matrix,
    step_matrix,
    value_filter_taps,
    write_filter_taps,
    read_filter_taps,
    head_log_decay,
    step_offset_bias,
    decay_spike,
    bypass_scale,
    group_norm_scale,
):
    sequence_count = lax.axis_size("sp")
    length, depth = tokens.shape
    channels = value_matrix.shape[1]
    heads = channels // HEAD
    own = STATE // sequence_count
    teams = sequence_count // TEAM
    blocks = length // BLOCK
    width = channels + 2 * STATE
    wide = teams * channels
    vm = pl.BlockSpec(memory_space=pltpu.VMEM)
    far = pl.BlockSpec(memory_space=pltpu.HBM)
    inside_team = [[TEAM * t + i for i in places(TEAM)] for t in range(teams)]
    across_teams = [[TEAM * t + i for t in places(teams)] for i in range(TEAM)]

    halo = lax.ppermute(
        tokens[length - HALO :], "sp", [(i, i + 1) for i in range(sequence_count - 1)]
    )
    fresh = fresh_token_input.reshape(depth // 128, 128)
    spike = decay_spike.T
    rows, weights, step_raw, fresh_rows, new_step = call(
        project_kernel,
        (
            near(length, width, dtype=bf16),
            near(depth, width, dtype=bf16),
            near(heads, length),
            near(8, depth, dtype=bf16),
            near(heads, 8),
        ),
        in_specs=[far] * 6,
        out_specs=[vm] * 5,
        scratch=[
            pltpu.VMEM((length, depth), bf16),
            pltpu.VMEM((depth // 128, 128), bf16),
            pltpu.VMEM((step_matrix.shape[1], depth), bf16),
            pltpu.SemaphoreType.DMA((SPLIT, 4)),
            pltpu.SemaphoreType.DMA((2,)),
        ],
        flops=2 * length * depth * width,
        name="project",
    )(
        stored(tokens), stored(fresh), stored(value_matrix), stored(write_matrix),
        stored(read_matrix), stored(step_matrix.T),
    )

    decay_row, bias_row, skip_row = head_log_decay[None], step_offset_bias[None], bypass_scale[None]
    vw, edge, cum, dt, inside, new_decay, send = call(
        local_kernel,
        (
            near(length, channels + STATE, dtype=bf16),
            near(HALO, STATE),
            near(heads, length),
            near(heads, length),
            near(blocks, STATE, channels, dtype=bf16),
            near(1, channels),
            near(TEAM, own, wide + MISC, dtype=bf16),
        ),
        in_specs=[vm] * 13,
        out_specs=[vm] * 7,
        scratch=[pltpu.VMEM((length + HALO, channels + STATE), f32)],
        flops=2 * length * STATE * channels,
        name="local",
    )(
        held(rows), held(halo), held(weights), held(step_raw), held(fresh_rows), held(new_step), spike,
        value_filter_taps, write_filter_taps, read_filter_taps,
        decay_row, bias_row, skip_row,
    )

    received = lax.all_to_all(held(send), "sp", 0, 0, tiled=True, axis_index_groups=inside_team)

    send, local_states, reach = call(
        team_kernel,
        (
            near(teams, own, wide + MISC, dtype=bf16),
            near(TEAM, own, wide),
            near(TEAM, channels),
        ),
        in_specs=[vm],
        out_specs=[vm] * 3,
        name="team",
    )(held(received))

    received = lax.all_to_all(held(send), "sp", 0, 0, tiled=True, axis_index_groups=across_teams)

    send, cache_rows, direct = call(
        prefix_kernel,
        (
            near(TEAM, own, wide + channels, dtype=bf16),
            shaped(own, channels, dtype=bf16),
            near(1, channels),
        ),
        in_specs=[vm] * 4,
        out_specs=[vm] * 3,
        name="prefix",
    )(held(received), held(local_states), held(reach), held(new_decay))

    received = lax.all_to_all(held(send), "sp", 0, 0, tiled=True, axis_index_groups=inside_team)

    base, lift, new_gate, reads = call(
        inner_kernel,
        (
            near(length, channels),
            near(length, channels),
            near(8, channels),
            near(length, STATE, dtype=bf16),
        ),
        grid=(blocks,),
        in_specs=[
            pl.BlockSpec((BLOCK, depth), lambda b: (b, 0)),
            pl.BlockSpec((depth, channels), lambda b: (0, 0)),
            pl.BlockSpec(fresh_rows.shape, lambda b: (0, 0)),
            pl.BlockSpec((length, width), lambda b: (0, 0)),
            pl.BlockSpec((HALO, STATE), lambda b: (0, 0)),
            pl.BlockSpec(read_filter_taps.shape, lambda b: (0, 0)),
            pl.BlockSpec((BLOCK, channels + STATE), lambda b: (b, 0)),
            pl.BlockSpec((heads, BLOCK), lambda b: (0, b)),
            pl.BlockSpec((heads, BLOCK), lambda b: (0, b)),
            pl.BlockSpec((1, STATE, channels), lambda b: (b, 0, 0)),
            pl.BlockSpec(skip_row.shape, lambda b: (0, 0)),
            pl.BlockSpec(direct.shape, lambda b: (0, 0)),
        ],
        out_specs=[
            pl.BlockSpec((BLOCK, channels), lambda b: (b, 0)),
            pl.BlockSpec((BLOCK, channels), lambda b: (b, 0)),
            pl.BlockSpec((8, channels), lambda b: (0, 0)),
            pl.BlockSpec((length, STATE), lambda b: (0, 0)),
        ],
        scratch=[pltpu.VMEM((heads, BLOCK), f32), pltpu.VMEM((length + HALO, STATE), f32)],
        flops=2 * length * depth * channels,
        name="inner",
    )(
        stored(tokens), stored(gate_matrix), held(fresh_rows), held(rows), held(edge), read_filter_taps,
        held(vw), held(cum), held(dt), held(inside), skip_row, held(direct),
    )

    prompt_out, step_row = call(
        finish_kernel,
        (
            shaped(length, channels, dtype=bf16),
            shaped(1, channels // sequence_count, dtype=bf16),
        ),
        in_specs=[vm] * 7,
        out_specs=[vm] * 2,
        name="finish",
    )(
        held(received), held(base), held(lift), held(reads), group_norm_scale[None],
        held(direct), held(new_gate),
    )
    return (prompt_out, cache_rows, step_row.T)


def solution(mesh):
    placed = (
        P(("grp", "sp"), None),
        P("grp"),
        P(None, "tp"),
        P(None, "tp"),
        P(None, "tp"),
        P(None, "tp"),
        P(),
        P(),
        P(),
        P(),
        P(),
        P(),
        P(("grp", "sp"), "tp"),
        P(),
        P(),
    )
    return jax.shard_map(
        on_device,
        mesh=mesh,
        in_specs=placed,
        out_specs=(P(("grp", "sp"), "tp"), P(("grp", "sp"), "tp"), P(("grp", "tp"), "sp")),
        check_vma=False,
    )
```

```python
import jax
import jax.numpy as jnp
from jax import lax
from jax.experimental import pallas as pl
from jax.experimental.pallas import tpu as pltpu
from jax.sharding import PartitionSpec as P

HEAD = 64
STATE = 128
CONV = 4
BLOCK = 128
TEAM = 4
MISC = 128
HALO = 8

epsilon = 1e-06
f32 = jnp.float32
bf16 = jnp.bfloat16
HIGHEST = lax.Precision.HIGHEST
VMEM_LIMIT = 24 * 1024 * 1024
SPLIT = 4


def dot(a, b, dims=((1,), (0,)), precision=None):
    return lax.dot_general(a, b, (dims, ((), ())), precision=precision, preferred_element_type=f32)


def silu(x):
    half = 0.5 * x
    return half * jnp.tanh(half) + half


def softplus(x):
    return jnp.maximum(x, 0.0) + jnp.log1p(jnp.exp(-jnp.abs(x)))


def iota(shape, dim):
    return lax.broadcasted_iota(jnp.int32, shape, dim)


def spread(heads, channels):
    return (iota((heads, channels), 0) == iota((heads, channels), 1) // HEAD).astype(f32)


def thirds(x):
    high = x.astype(bf16)
    rest = x - high.astype(f32)
    middle = rest.astype(bf16)
    low = (rest - middle.astype(f32)).astype(bf16)
    return jnp.concatenate([high.astype(f32), middle.astype(f32), low.astype(f32)], axis=0).astype(bf16)


def over_channels(x, channels):
    heads = x.shape[0]
    shape = (3 * heads, channels)
    mask = iota(shape, 0) % heads == iota(shape, 1) // HEAD
    return dot(thirds(x), mask.astype(bf16), ((0,), (0,)))


def summed_up(x, upper):
    heads = x.shape[0]
    parts = dot(thirds(x), upper)
    return parts[0:heads] + parts[heads : 2 * heads] + parts[2 * heads :]


def own_rows(table, rank, count):
    picked = table[0:count]
    for other in range(1, table.shape[0] // count):
        picked = jnp.where(rank == other, table[other * count : (other + 1) * count], picked)
    return picked


def head_column(ref, first, count):
    row = ref[...]
    shape = (count, row.shape[1])
    return jnp.sum(jnp.where(iota(shape, 1) == iota(shape, 0) + first, row, 0.0), axis=1, keepdims=True)


def tail_kernel(tok_hbm, tail_ref, sem):
    rows = tok_hbm.at[pl.ds(tok_hbm.shape[0] - HALO, HALO)]
    copy = pltpu.make_async_copy(rows, tail_ref, sem)
    copy.start()
    copy.wait()


def project_kernel(
    tok_hbm, fresh_hbm, wv_hbm, ww_hbm, wr_hbm, ws_hbm,
    rows_ref, weights, step_ref, fresh_ref, newstep_ref, tok, lines, steps, sems, small,
):
    depth = tok_hbm.shape[1]
    channels = wv_hbm.shape[1]
    state = ww_hbm.shape[1]
    chunk = depth // SPLIT
    get_fresh = pltpu.make_async_copy(fresh_hbm, lines, small.at[0])
    get_steps = pltpu.make_async_copy(ws_hbm, steps, small.at[1])
    get_steps.start()
    copies = []
    for k in range(SPLIT):
        at = pl.ds(k * chunk, chunk)
        moves = [
            (tok_hbm.at[:, at], tok.at[:, at]),
            (wv_hbm.at[at], weights.at[at, pl.ds(0, channels)]),
            (ww_hbm.at[at], weights.at[at, pl.ds(channels, state)]),
            (wr_hbm.at[at], weights.at[at, pl.ds(channels + state, state)]),
        ]
        copies.append(
            [pltpu.make_async_copy(a, b, sems.at[k, i]) for i, (a, b) in enumerate(moves)]
        )
    for k in range(SPLIT):
        for copy in copies[k]:
            copy.start()
    get_fresh.start()
    rank = lax.axis_index("tp")
    heads = step_ref.shape[0]
    acc = accs = None
    get_steps.wait()
    for k in range(SPLIT):
        at = slice(k * chunk, (k + 1) * chunk)
        for copy in copies[k]:
            copy.wait()
        part = dot(tok[:, at], weights[at])
        parts = dot(steps[:, at], tok[:, at], ((1,), (1,)))
        acc = part if k == 0 else acc + part
        accs = parts if k == 0 else accs + parts
        if k == SPLIT - 1:
            get_fresh.wait()
            rows = lines[...].astype(f32)
            fresh = jnp.concatenate([rows[i : i + 1] for i in range(depth // 128)], axis=1)
            fresh_ref[...] = jnp.broadcast_to(fresh, fresh_ref.shape).astype(bf16)
            table = own_rows(steps[...].astype(f32), rank, heads)
            newstep = jnp.sum(table * fresh, axis=1, keepdims=True)
            newstep_ref[...] = jnp.broadcast_to(newstep, newstep_ref.shape)
    rows_ref[...] = acc.astype(bf16)
    step_ref[...] = own_rows(accs, rank, heads)


def local_kernel(
    rows_ref, halo_ref, weights, step_ref, fresh_ref, newstep_ref, spike_ref,
    vtap_ref, wtap_ref, rtap_ref, decay_ref, bias_ref, skip_ref,
    vw_ref, edge_ref, cum_ref, dt_ref, inside_ref, newdecay_ref, send_ref, ext,
):
    rank = lax.axis_index("tp")
    length = rows_ref.shape[0]
    heads = step_ref.shape[0]
    channels = rows_ref.shape[1] - 2 * STATE
    first = rank * heads
    few = dot(jnp.concatenate([halo_ref[...], fresh_ref[...]], axis=0), weights[...])
    few = few.astype(bf16).astype(f32)
    before = few[0:HALO]
    used = channels + STATE
    edge_ref[...] = before[:, used:]
    ext[0:HALO] = before[:, 0:used]
    ext[HALO:] = rows_ref[:, 0:used].astype(f32)
    taps = jnp.concatenate(
        [
            vtap_ref[:, pl.ds(pl.multiple_of(rank * channels, 128), channels)].astype(f32),
            wtap_ref[:, pl.ds(pl.multiple_of(rank * STATE, 128), STATE)].astype(f32),
            rtap_ref[:, pl.ds(pl.multiple_of(rank * STATE, 128), STATE)].astype(f32),
        ],
        axis=1,
    )
    off = HALO - (CONV - 1)
    summed = taps[0:1, 0:used] * ext[off : off + length]
    for k in range(1, CONV):
        summed = summed + taps[k : k + 1, 0:used] * ext[off + k : off + k + length]
    vwr = silu(summed).astype(bf16)
    vw_ref[...] = vwr
    newest = taps[CONV - 1 : CONV] * few[HALO : HALO + 1]
    ending = rows_ref[length - 16 :].astype(f32)
    for k in range(CONV - 1):
        row = 16 - (CONV - 1) + k
        newest = newest + taps[k : k + 1] * ending[row : row + 1]
    newest = silu(newest).astype(bf16).astype(f32)
    new_value = newest[:, 0:channels]
    new_write = newest[:, channels : channels + STATE]
    new_read = newest[:, channels + STATE :]
    bias = head_column(bias_ref, first, heads)
    rate = jnp.exp(head_column(decay_ref, first, heads))
    upper = (iota((BLOCK, BLOCK), 0) <= iota((BLOCK, BLOCK), 1)).astype(bf16)
    expand = spread(heads, channels)
    running = jnp.zeros((STATE, channels), f32)
    total = jnp.zeros((heads, 128), f32)
    for b in range(length // BLOCK):
        at = slice(b * BLOCK, (b + 1) * BLOCK)
        dt = softplus(step_ref[:, at] + bias)
        log_decay = spike_ref[:, at] - dt * rate
        cum = summed_up(log_decay, upper)
        dt_ref[:, at] = dt
        cum_ref[:, at] = cum
        end = jnp.broadcast_to(cum[:, BLOCK - 1 :], (heads, BLOCK))
        factor = over_channels(jnp.exp(end - cum) * dt, channels)
        scaled = (factor * vwr[at, 0:channels].astype(f32)).astype(bf16)
        states = dot(vwr[at, channels : channels + STATE], scaled, ((0,), (0,)))
        fade = jnp.sum(expand * jnp.exp(end[:, 0:1]), axis=0, keepdims=True)
        inside_ref[b] = running.astype(bf16)
        running = fade * running + states
        total = total + end
    fade = jnp.exp(total)
    high = fade.astype(bf16).astype(f32)
    low = fade - high
    shape = (STATE, MISC)
    lanes = iota(shape, 1)
    rows = iota(shape, 0)
    misc = jnp.zeros(shape, f32)
    for h in range(heads):
        misc = jnp.where(lanes == h, high[h : h + 1, 0:1], misc)
        misc = jnp.where(lanes == heads + h, low[h : h + 1, 0:1], misc)
    own = STATE // lax.axis_size("sp")
    stretch = TEAM * own
    teams = STATE // stretch
    diagonal = jnp.where(rows == lanes, jnp.broadcast_to(new_read, shape), 0.0)
    read_column = jnp.sum(diagonal, axis=1, keepdims=True)
    new_dt = softplus(newstep_ref[...][:, 0:1] + bias)
    newdecay_ref[...] = jnp.sum(expand * jnp.exp(-new_dt * rate), axis=0, keepdims=True)
    skip = head_column(skip_ref, first, heads)
    weight = new_dt * jnp.sum(new_read * new_write, axis=1, keepdims=True) + skip
    direct = jnp.sum(expand * weight, axis=0, keepdims=True) * new_value
    placed = jnp.where(iota((8, channels), 0) == iota((8, channels), 1) // HEAD, direct, 0.0)
    shift = (iota((channels, MISC), 0) % HEAD + (MISC - HEAD) == iota((channels, MISC), 1)).astype(f32)
    direct_rows = dot(placed, shift, precision=HIGHEST)[0:own]
    for g in range(teams):
        at = slice(g * stretch, (g + 1) * stretch)
        piece = running[at].reshape(TEAM, own, channels).astype(bf16)
        for p, member in enumerate(places(TEAM)):
            send_ref[p, :, g * channels : (g + 1) * channels] = piece[member]
    note = misc[0:stretch]
    for g in range(teams):
        at = slice(g * stretch, (g + 1) * stretch)
        note = jnp.where(lanes[0:stretch] == 2 * heads + g, read_column[at], note)
    note = note.reshape(TEAM, own, MISC)
    note = jnp.where(iota(note.shape, 2) >= MISC - HEAD, direct_rows[None], note).astype(bf16)
    for p, member in enumerate(places(TEAM)):
        send_ref[p, :, teams * channels :] = note[member]


def inner_kernel(
    tok_ref, wg_ref, fresh_ref, rows_ref, edge_ref, rtap_ref, vw_ref, cum_ref, dt_ref, inside_ref,
    skip_ref, after_ref, base_ref, lift_ref, newgate_ref, reads_ref, before, ext,
):
    del after_ref
    b = pl.program_id(0)
    rank = lax.axis_index("tp")
    heads = cum_ref.shape[0]
    channels = wg_ref.shape[1]
    length = rows_ref.shape[0]

    @pl.when(b == 0)
    def _():
        before[...] = jnp.zeros_like(before)
        gate = dot(fresh_ref[...], wg_ref[...]).astype(bf16).astype(f32)
        newgate_ref[...] = silu(gate)
        ext[0:HALO] = edge_ref[...]
        ext[HALO:] = rows_ref[:, channels + STATE :].astype(f32)
        taps = rtap_ref[:, pl.ds(pl.multiple_of(rank * STATE, 128), STATE)].astype(f32)
        off = HALO - (CONV - 1)
        summed = taps[0:1] * ext[off : off + length]
        for k in range(1, CONV):
            summed = summed + taps[k : k + 1] * ext[off + k : off + k + length]
        reads_ref[...] = silu(summed).astype(bf16)

    expand = spread(heads, channels)
    skip = jnp.sum(expand * head_column(skip_ref, rank * heads, heads), axis=0, keepdims=True)
    cum = cum_ref[...]
    dt = dt_ref[...]
    values = vw_ref[:, 0:channels]
    writes = vw_ref[:, channels:]
    reads = reads_ref[pl.ds(pl.multiple_of(b * BLOCK, BLOCK), BLOCK)]
    gate = silu(dot(tok_ref[...], wg_ref[...]).astype(bf16).astype(f32))
    scores = dot(reads, writes, ((1,), (1,)))
    causal = iota((BLOCK, BLOCK), 0) >= iota((BLOCK, BLOCK), 1)
    columns = jnp.transpose(jnp.concatenate([cum, cum], axis=0))
    parts = []
    for h in range(heads):
        gap = columns[:, h : h + 1] - cum[h : h + 1]
        mixing = scores * jnp.exp(jnp.where(causal, gap, -jnp.inf)) * dt[h : h + 1]
        parts.append(dot(mixing.astype(bf16), values[:, h * HEAD : (h + 1) * HEAD]))
    inner = jnp.concatenate(parts, axis=1)
    fade = over_channels(jnp.exp(cum), channels)
    carried = fade * dot(reads, inside_ref[0])
    base_ref[...] = (inner + carried + skip * values.astype(f32)) * gate
    far = jnp.exp(cum + before[...])
    lift_ref[...] = over_channels(far, channels) * gate
    before[...] += jnp.broadcast_to(cum[:, BLOCK - 1 :], before.shape)


def places(count):
    return [*reversed(range(count))]


def fades_of(notes, heads, channels):
    lane = iota((MISC, channels), 0)
    owner = iota((MISC, channels), 1) // HEAD
    pick = jnp.where((lane == owner) | (lane == owner + heads), 1.0, 0.0)
    return dot(jnp.where(iota(notes.shape, 1) < 2 * heads, notes, 0.0), pick, precision=HIGHEST)


def team_kernel(recv_ref, send_ref, local_ref, reach_ref):
    count, own, width = recv_ref.shape
    wide = width - MISC
    teams = send_ref.shape[0]
    channels = wide // teams
    heads = channels // HEAD
    notes = recv_ref[:, 0:1, wide:].astype(f32).reshape(count, MISC)
    fades = fades_of(notes, heads, channels)
    state = jnp.zeros((own, wide), f32)
    reach = jnp.ones((1, channels), f32)
    place = {member: p for p, member in enumerate(places(count))}
    for k in range(count):
        local_ref[k] = state
        reach_ref[k : k + 1] = reach
        at = place[k]
        fade = jnp.concatenate([fades[at : at + 1]] * teams, axis=1)
        state = fade * state + recv_ref[at, :, 0:wide].astype(f32)
        reach = reach * fades[at : at + 1]
    total = state.astype(bf16)
    note = recv_ref[place[count - 1], :, wide:].astype(f32)
    first = (iota((channels, MISC), 0) == iota((channels, MISC), 1) * HEAD).astype(f32)
    high = reach.astype(bf16).astype(f32)
    low = reach - high
    packed = dot(jnp.concatenate([high, low, jnp.zeros((6, channels), f32)], axis=0), first, precision=HIGHEST)
    shifted = (iota((MISC, MISC), 0) + heads == iota((MISC, MISC), 1)).astype(f32)
    moved = dot(packed, shifted, precision=HIGHEST)
    lanes = iota((own, MISC), 1)
    note = jnp.where(lanes < heads, packed[0:1], jnp.where(lanes < 2 * heads, moved[1:2], note)).astype(bf16)
    for t in range(teams):
        send_ref[t, :, 0:wide] = total
        send_ref[t, :, wide:] = note


def prefix_kernel(recv_ref, local_ref, reach_ref, newdecay_ref, send_ref, cache_ref, direct_ref):
    teams, own, width = recv_ref.shape
    wide = width - MISC
    channels = wide // teams
    heads = channels // HEAD
    group = lax.axis_index("sp") // TEAM
    notes = recv_ref[:, 0:1, wide:].astype(f32).reshape(teams, MISC)
    fades = fades_of(notes, heads, channels)
    state = jnp.zeros((own, wide), f32)
    entering = state
    place = {t: p for p, t in enumerate(places(teams))}
    for t in range(teams):
        at = place[t]
        entering = jnp.where(group == t, state, entering)
        fade = jnp.concatenate([fades[at : at + 1]] * teams, axis=1)
        state = fade * state + recv_ref[at, :, 0:wide].astype(f32)
    for p, k in enumerate(places(TEAM)):
        reach = jnp.concatenate([reach_ref[k : k + 1]] * teams, axis=1)
        send_ref[p, :, 0:wide] = (local_ref[k] + reach * entering).astype(bf16)
    kept = state.astype(bf16).astype(f32)
    mine = kept[:, 0:channels]
    for g in range(1, teams):
        mine = jnp.where(group == g, kept[:, g * channels : (g + 1) * channels], mine)
    cache_ref[...] = mine.astype(bf16)
    note = recv_ref[place[teams - 1], :, wide:].astype(f32)
    reading = jnp.zeros((own, channels), f32)
    for g in range(teams):
        column = note[:, 2 * heads + g : 2 * heads + g + 1]
        reading = reading + column * kept[:, g * channels : (g + 1) * channels]
    partial = jnp.sum(reading, axis=0, keepdims=True) * newdecay_ref[...]
    high = partial.astype(bf16).astype(f32)
    low = partial - high
    rows = iota((own, channels), 0)
    share = jnp.where(rows == 0, high, jnp.where(rows == 1, low, 0.0)).astype(bf16)
    send_ref[:, :, wide:] = jnp.broadcast_to(share[None], (TEAM, own, channels))
    unshift = (iota((MISC, channels), 0) == iota((MISC, channels), 1) % HEAD + (MISC - HEAD)).astype(f32)
    laid = dot(note, unshift, precision=HIGHEST)
    direct_ref[...] = jnp.sum(jnp.where(rows == iota(rows.shape, 1) // HEAD, laid, 0.0), axis=0, keepdims=True)


def finish_kernel(recv_ref, base_ref, lift_ref, reads_ref, gain_ref, direct_ref, newgate_ref, out_ref, step_ref):
    rank = lax.axis_index("tp")
    place = lax.axis_index("sp")
    channels = base_ref.shape[1]
    wide = recv_ref.shape[2] - channels
    pieces = wide // channels
    own = recv_ref.shape[1]
    spot = {member: p for p, member in enumerate(places(TEAM))}
    earlier = jnp.concatenate(
        [
            recv_ref[spot[i], :, g * channels : (g + 1) * channels].astype(f32)
            for g in range(pieces)
            for i in range(TEAM)
        ],
        axis=0,
    ).astype(bf16)
    gain = gain_ref[:, pl.ds(pl.multiple_of(rank * channels, 128), channels)]
    gated = base_ref[...] + dot(reads_ref[...], earlier) * lift_ref[...]
    scale = lax.rsqrt(jnp.mean(gated * gated, axis=1, keepdims=True) + epsilon)
    out_ref[...] = (gated * scale * gain).astype(bf16)
    partial = jnp.sum(jnp.sum(recv_ref[:, :, wide:].astype(f32), axis=0), axis=0, keepdims=True)
    new = (partial + direct_ref[...]) * newgate_ref[0:1]
    scale = lax.rsqrt(jnp.mean(new * new, axis=1, keepdims=True) + epsilon)
    step = (new * scale * gain).astype(bf16)
    columns = lax.axis_size("sp")
    channel = iota((channels, 128), 0)
    take = (channel // columns == iota((channels, 128), 1)) & (channel % columns == place)
    picked = dot(jnp.broadcast_to(step, (16, channels)), take.astype(bf16))
    step_ref[...] = picked[0:1, 0 : channels // columns].astype(bf16)


def call(kernel, out_shape, grid=None, in_specs=None, out_specs=None, scratch=(), flops=0, name=None):
    return pl.pallas_call(
        kernel,
        out_shape=out_shape,
        grid_spec=pltpu.PrefetchScalarGridSpec(
            num_scalar_prefetch=0,
            grid=grid or (),
            in_specs=in_specs,
            out_specs=out_specs,
            scratch_shapes=scratch,
        ),
        compiler_params=pltpu.CompilerParams(
            vmem_limit_bytes=VMEM_LIMIT,
            dimension_semantics=("arbitrary",) * len(grid or ()),
        ),
        cost_estimate=pl.CostEstimate(flops=flops, transcendentals=0, bytes_accessed=1 << 20),
        name=name,
    )


def shaped(*shape, dtype=f32):
    return jax.ShapeDtypeStruct(shape, dtype)


def near(*shape, dtype=f32):
    return pltpu.VMEM(shape, dtype)


def held(array):
    return pltpu.with_memory_space_constraint(array, pltpu.VMEM)


def stored(array):
    return pltpu.with_memory_space_constraint(array, pltpu.HBM)


def on_device(
    tokens,
    fresh_token_input,
    value_matrix,
    write_matrix,
    read_matrix,
    gate_matrix,
    step_matrix,
    value_filter_taps,
    write_filter_taps,
    read_filter_taps,
    head_log_decay,
    step_offset_bias,
    decay_spike,
    bypass_scale,
    group_norm_scale,
):
    sequence_count = lax.axis_size("sp")
    length, depth = tokens.shape
    channels = value_matrix.shape[1]
    heads = channels // HEAD
    own = STATE // sequence_count
    teams = sequence_count // TEAM
    blocks = length // BLOCK
    width = channels + 2 * STATE
    wide = teams * channels
    vm = pl.BlockSpec(memory_space=pltpu.VMEM)
    far = pl.BlockSpec(memory_space=pltpu.HBM)
    inside_team = [[TEAM * t + i for i in places(TEAM)] for t in range(teams)]
    across_teams = [[TEAM * t + i for t in places(teams)] for i in range(TEAM)]

    tail = call(
        tail_kernel,
        near(HALO, depth, dtype=bf16),
        in_specs=[far],
        out_specs=vm,
        scratch=[pltpu.SemaphoreType.DMA],
        name="tail",
    )(stored(tokens))
    halo = lax.ppermute(held(tail), "sp", [(i, i + 1) for i in range(sequence_count - 1)])
    fresh = fresh_token_input.reshape(depth // 128, 128)
    spike = decay_spike.T
    rows, weights, step_raw, fresh_rows, new_step = call(
        project_kernel,
        (
            near(length, width, dtype=bf16),
            near(depth, width, dtype=bf16),
            near(heads, length),
            near(8, depth, dtype=bf16),
            near(heads, 8),
        ),
        in_specs=[far] * 6,
        out_specs=[vm] * 5,
        scratch=[
            pltpu.VMEM((length, depth), bf16),
            pltpu.VMEM((depth // 128, 128), bf16),
            pltpu.VMEM((step_matrix.shape[1], depth), bf16),
            pltpu.SemaphoreType.DMA((SPLIT, 4)),
            pltpu.SemaphoreType.DMA((2,)),
        ],
        flops=2 * length * depth * width,
        name="project",
    )(
        stored(tokens), stored(fresh), stored(value_matrix), stored(write_matrix),
        stored(read_matrix), stored(step_matrix.T),
    )

    decay_row, bias_row, skip_row = head_log_decay[None], step_offset_bias[None], bypass_scale[None]
    vw, edge, cum, dt, inside, new_decay, send = call(
        local_kernel,
        (
            near(length, channels + STATE, dtype=bf16),
            near(HALO, STATE),
            near(heads, length),
            near(heads, length),
            near(blocks, STATE, channels, dtype=bf16),
            near(1, channels),
            near(TEAM, own, wide + MISC, dtype=bf16),
        ),
        in_specs=[vm] * 13,
        out_specs=[vm] * 7,
        scratch=[pltpu.VMEM((length + HALO, channels + STATE), f32)],
        flops=2 * length * STATE * channels,
        name="local",
    )(
        held(rows), held(halo), held(weights), held(step_raw), held(fresh_rows), held(new_step), spike,
        value_filter_taps, write_filter_taps, read_filter_taps,
        decay_row, bias_row, skip_row,
    )

    received = lax.all_to_all(held(send), "sp", 0, 0, tiled=True, axis_index_groups=inside_team)

    send, local_states, reach = call(
        team_kernel,
        (
            near(teams, own, wide + MISC, dtype=bf16),
            near(TEAM, own, wide),
            near(TEAM, channels),
        ),
        in_specs=[vm],
        out_specs=[vm] * 3,
        name="team",
    )(held(received))

    received = lax.all_to_all(held(send), "sp", 0, 0, tiled=True, axis_index_groups=across_teams)

    send, cache_rows, direct = call(
        prefix_kernel,
        (
            near(TEAM, own, wide + channels, dtype=bf16),
            shaped(own, channels, dtype=bf16),
            near(1, channels),
        ),
        in_specs=[vm] * 4,
        out_specs=[vm] * 3,
        name="prefix",
    )(held(received), held(local_states), held(reach), held(new_decay))

    received = lax.all_to_all(held(send), "sp", 0, 0, tiled=True, axis_index_groups=inside_team)

    base, lift, new_gate, reads = call(
        inner_kernel,
        (
            near(length, channels),
            near(length, channels),
            near(8, channels),
            near(length, STATE, dtype=bf16),
        ),
        grid=(blocks,),
        in_specs=[
            pl.BlockSpec((BLOCK, depth), lambda b: (b, 0)),
            pl.BlockSpec((depth, channels), lambda b: (0, 0)),
            pl.BlockSpec(fresh_rows.shape, lambda b: (0, 0)),
            pl.BlockSpec((length, width), lambda b: (0, 0)),
            pl.BlockSpec((HALO, STATE), lambda b: (0, 0)),
            pl.BlockSpec(read_filter_taps.shape, lambda b: (0, 0)),
            pl.BlockSpec((BLOCK, channels + STATE), lambda b: (b, 0)),
            pl.BlockSpec((heads, BLOCK), lambda b: (0, b)),
            pl.BlockSpec((heads, BLOCK), lambda b: (0, b)),
            pl.BlockSpec((1, STATE, channels), lambda b: (b, 0, 0)),
            pl.BlockSpec(skip_row.shape, lambda b: (0, 0)),
            pl.BlockSpec(direct.shape, lambda b: (0, 0)),
        ],
        out_specs=[
            pl.BlockSpec((BLOCK, channels), lambda b: (b, 0)),
            pl.BlockSpec((BLOCK, channels), lambda b: (b, 0)),
            pl.BlockSpec((8, channels), lambda b: (0, 0)),
            pl.BlockSpec((length, STATE), lambda b: (0, 0)),
        ],
        scratch=[pltpu.VMEM((heads, BLOCK), f32), pltpu.VMEM((length + HALO, STATE), f32)],
        flops=2 * length * depth * channels,
        name="inner",
    )(
        stored(tokens), stored(gate_matrix), held(fresh_rows), held(rows), held(edge), read_filter_taps,
        held(vw), held(cum), held(dt), held(inside), skip_row, held(direct),
    )

    prompt_out, step_row = call(
        finish_kernel,
        (
            shaped(length, channels, dtype=bf16),
            shaped(1, channels // sequence_count, dtype=bf16),
        ),
        in_specs=[vm] * 7,
        out_specs=[vm] * 2,
        name="finish",
    )(
        held(received), held(base), held(lift), held(reads), group_norm_scale[None],
        held(direct), held(new_gate),
    )
    return (prompt_out, cache_rows, step_row.T)


def solution(mesh):
    placed = (
        P(("grp", "sp"), None),
        P("grp"),
        P(None, "tp"),
        P(None, "tp"),
        P(None, "tp"),
        P(None, "tp"),
        P(),
        P(),
        P(),
        P(),
        P(),
        P(),
        P(("grp", "sp"), "tp"),
        P(),
        P(),
    )
    return jax.shard_map(
        on_device,
        mesh=mesh,
        in_specs=placed,
        out_specs=(P(("grp", "sp"), "tp"), P(("grp", "sp"), "tp"), P(("grp", "tp"), "sp")),
        check_vma=False,
    )
```
